256 devices in a mesh: sp: 32 (over z, y), tp: 8 (over x, core).
Axes of the slice: x: 4, y: 4, z: 8, core: 2. Of those that a mesh axis runs over, the one named last changes fastest.
Arguments:
- hidden: bfloat16 [4096, 2048], P('sp'), may hold values from -6 to 6
- value_weight: bfloat16 [2048, 4096], P(None, 'tp'), may hold values from -0.125 to 0.125
- key_vecs: bfloat16 [4096, 8, 128], P('sp', 'tp'), may hold values from -0.29882812 to 0.29882812
- queries: bfloat16 [4096, 8, 128], P('sp', 'tp'), may hold values from -0.29882812 to 0.29882812
- decay_pre: float32 [4096, 64], P('sp', 'tp'), may hold values from -4 to 4
- decay_rate: float32 [64], P('tp'), may hold values from 1.4648437e-05 to 0.0009033203
- cotangent: bfloat16 [4096, 64, 64], P('sp', 'tp'), may hold values from -1.1953125 to 1.1953125
Outputs:
- grad_keys: bfloat16 [4096, 8, 128], P('sp', 'tp')
- grad_queries: bfloat16 [4096, 8, 128], P('sp', 'tp')
- grad_decay: float32 [4096, 64], P('sp', 'tp')
- grad_hidden: bfloat16 [4096, 2048], P(('sp', 'tp'))
- grad_weight: float32 [2048, 4096], P('sp', 'tp')
The draws below stay inside these ranges and needn't reach their ends.
All inputs are finite; a program needn't handle non-finite values.
Results may differ from the reference program's by a relative error of at most 0.003.
Values sent between devices are 32-bit elements.
A program may use at most 64 MiB of HBM per device.

```python
import math
import jax
import jax.numpy as jnp
from jax import lax

D = 2048
HEADS = 64
HEAD_DIM = 64
GROUPS = 8
STATE = 128
TOK_DEV = 128
INNER = 4096
TOKENS = 4096


def shard_levels(rng, shape, pieces, smallest, top_value):
    level = 1.0
    for axis_at, shards_of in pieces:
        heights = jax.random.uniform(jax.random.fold_in(jax.random.fold_in(rng, 6), axis_at), (shards_of,), jnp.float32, smallest / len(pieces), top_value / len(pieces))
        level = level * jnp.repeat(jnp.exp(heights), shape[axis_at] // shards_of).reshape((-1,) + (1,) * (len(shape) - 1 - axis_at))
    return level


def bell_draw(rng, dims, scale, limit, shards=(), kind=jnp.bfloat16):
    entries = scale * jax.random.normal(rng, dims, jnp.float32)
    if shards:
        entries = entries * shard_levels(rng, dims, shards, -0.22, 0.18)
    return jnp.clip(entries, -limit, limit).astype(kind)


def setup_inputs(seed: int = 0) -> dict:
    splits = jax.random.split(jax.random.key(seed), 8)
    return {
        "hidden": bell_draw(splits[0], (TOKENS, D), 1.0, 6.0, ((0, 32),)),
        "value_weight": bell_draw(splits[1], (D, INNER), D ** -0.5, 0.125, ((1, 8),)),
        "key_vecs": bell_draw(splits[2], (TOKENS, GROUPS, STATE), 0.05, 0.29882812, ((0, 32), (1, 8))),
        "queries": bell_draw(splits[3], (TOKENS, GROUPS, STATE), 0.05, 0.29882812, ((0, 32), (1, 8))),
        "decay_pre": bell_draw(splits[4], (TOKENS, HEADS), 1.0, 4.0, ((0, 32), (1, 8)), jnp.float32),
        "decay_rate": jnp.clip(jnp.exp(math.log(0.0009033203) - 4.1217436 * jax.random.uniform(splits[5], (HEADS,), jnp.float32) ** shard_levels(splits[5], (HEADS,), ((0, 8),), -0.2, 0.2)), 1.4648437172581907e-05, 0.0009033203),
        "cotangent": bell_draw(splits[6], (TOKENS, HEADS, HEAD_DIM), 0.2, 1.1953125, ((0, 32), (1, 8))),
    }


highest = lax.Precision.HIGHEST

def local_mixer(values_f, keys_f, queries_f, decay_pre, decay_rate, state_in):
    heads_here = values_f.shape[1]
    per_group = heads_here // keys_f.shape[1]
    key_heads = jnp.repeat(keys_f, per_group, axis=1)
    query_heads = jnp.repeat(queries_f, per_group, axis=1)
    log_decay = -decay_rate[None, :] * jax.nn.softplus(decay_pre)
    cumulative = jnp.cumsum(log_decay, axis=0)
    length = values_f.shape[0]
    causal = jnp.tril(jnp.ones((length, length), dtype=bool))[None]
    across = cumulative.T[:, :, None] - cumulative.T[:, None, :]
    damping = jnp.where(causal, jnp.exp(jnp.where(causal, across, 0.0)), 0.0)
    scores = jnp.einsum('thn,shn->hts', query_heads, key_heads, precision=highest)
    outputs = jnp.einsum('hts,shp->thp', scores * damping, values_f, precision=highest)
    carried = jnp.einsum('thn,hpn->thp', query_heads, state_in, precision=highest)
    outputs = outputs + jnp.exp(cumulative)[:, :, None] * carried
    to_end = jnp.exp(cumulative[-1][None, :] - cumulative)
    state_out = jnp.exp(cumulative[-1])[:, None, None] * state_in + jnp.einsum('sh,shp,shn->hpn', to_end, values_f, key_heads, precision=highest)
    return (outputs, state_out)

def reference(hidden, value_weight, key_vecs, queries, decay_pre, decay_rate, cotangent):
    values = jnp.dot(hidden, value_weight, preferred_element_type=jnp.float32).astype(jnp.bfloat16)
    tokens_all = hidden.shape[0]
    block_count = tokens_all // TOK_DEV
    head_count = decay_rate.shape[0]

    def to_blocks(tensor):
        return tensor.reshape((block_count, TOK_DEV) + tensor.shape[1:])

    def whole_seq(values_in, keys_in, queries_in, pre_in):

        def advance(state_now, inputs):
            block_out, state_next = local_mixer(inputs[0], inputs[1], inputs[2], inputs[3], decay_rate, state_now)
            return (state_next, block_out)
        start_state = jnp.zeros((head_count, HEAD_DIM, STATE), jnp.float32)
        final_state, block_outs = lax.scan(advance, start_state, (to_blocks(values_in), to_blocks(keys_in), to_blocks(queries_in), to_blocks(pre_in)))
        return block_outs.reshape((tokens_all,) + block_outs.shape[2:])
    values_f = values.reshape(tokens_all, head_count, HEAD_DIM).astype(jnp.float32)
    primal, pullback = jax.vjp(whole_seq, values_f, key_vecs.astype(jnp.float32), queries.astype(jnp.float32), decay_pre)
    grad_values, grad_keys, grad_queries, grad_decay = pullback(cotangent.astype(jnp.float32))
    grad_flat = grad_values.reshape(tokens_all, -1).astype(jnp.bfloat16)
    grad_hidden = lax.dot_general(grad_flat, value_weight, (((1,), (1,)), ((), ())), preferred_element_type=jnp.float32).astype(jnp.bfloat16)
    grad_weight = lax.dot_general(hidden, grad_flat, (((0,), (0,)), ((), ())), preferred_element_type=jnp.float32)
    return (grad_keys.astype(jnp.bfloat16), grad_queries.astype(jnp.bfloat16), grad_decay, grad_hidden, grad_weight)
```

```python
import jax
import jax.numpy as jnp
from jax import lax
from jax.experimental import pallas as pl
from jax.experimental.pallas import tpu as pltpu
from jax.sharding import Mesh
from jax.sharding import PartitionSpec as P

F32, BF16 = jnp.float32, jnp.bfloat16
MESH = pl.DeviceIdType.MESH
SP, TP = ("z", "y"), ("x", "c")
NZ, NY, NX = 8, 4, 4
TOK, STATE, PAIRS, HEADS = 128, 128, 4, 8
ROWS = STATE // NZ


def dot(a, b, dims=((1,), (0,))):
    return lax.dot_general(a, b, (dims, ((), ())), preferred_element_type=F32)


def halves(a):
    high = a.astype(BF16)
    return high, (a - high.astype(F32)).astype(BF16)


def dot_fine_right(a, b, dims=((1,), (0,))):
    high, low = halves(b)
    return dot(a, high, dims) + dot(a, low, dims)


def dot_fine_left(a, b, dims=((1,), (0,))):
    high, low = halves(a)
    return dot(high, b, dims) + dot(low, b, dims)


def dot_fine(a, b, dims=((1,), (0,))):
    a_high, a_low = halves(a)
    b_high, b_low = halves(b)
    return dot(a_high, b_high, dims) + dot(a_high, b_low, dims) + dot(a_low, b_high, dims)


def cols(pair):
    return slice(128 * pair, 128 * pair + 128)


def kernel(
    hid, w, k_in, q_in, pre, rate, cot,
    gk_out, gq_out, gd_out, gh_out, gw_out,
    ys_b, yr_b, ys_f, yr_f, zs_b, zr_b, zs_f, zr_f,
    zbs_b, zbr_b, zbs_f, zbr_f, ybs_b, ybr_b, ybs_f, ybr_f,
    hid_t, hid_r, hid_all, ag_s, ag_r, part, ring_s, ring_r,
    gh_s, gh_r, gx_s, gx_r, gv_in, vals, row_sum,
    y_sem, z_sem, ag_sem, ring_sem, d_sem, x_sem,
):
    z, y = lax.axis_index("z"), lax.axis_index("y")
    x, c = lax.axis_index("x"), lax.axis_index("c")
    lane = lax.broadcasted_iota(jnp.int32, (128, 128), 1)
    first_head = lane[0:1, :] < 64
    sent = []

    def peer_y(o):
        return lax.rem(y + o, NY)

    def peer_z(o):
        return lax.rem(z + o, NZ)

    def peer_x(o):
        return lax.rem(x + o, NX)

    def copy(src, dst, s_sem, r_sem, **where):
        return pltpu.make_async_remote_copy(
            src_ref=src, dst_ref=dst, send_sem=s_sem, recv_sem=r_sem, device_id=where, device_id_type=MESH
        )

    def send(src, dst, s_sem, r_sem, **where):
        made = copy(src, dst, s_sem, r_sem, **where)
        made.start()
        sent.append(made)

    def arrived(dst, r_sem):
        copy(dst, dst, r_sem, r_sem, c=1 - c).wait_recv()

    barrier = pltpu.get_barrier_semaphore()
    for o in range(1, NY):
        pl.semaphore_signal(barrier, inc=1, device_id={"y": peer_y(o)}, device_id_type=MESH)
    for o in range(1, NZ):
        pl.semaphore_signal(barrier, inc=1, device_id={"z": peer_z(o)}, device_id_type=MESH)
    for o in range(1, NX):
        pl.semaphore_signal(barrier, inc=1, device_id={"x": peer_x(o)}, device_id_type=MESH)
    pl.semaphore_signal(barrier, inc=1, device_id={"c": 1 - c}, device_id_type=MESH)

    pre_v = pre[...]
    soft = jnp.maximum(pre_v, 0.0) + jnp.log1p(jnp.exp(-jnp.abs(pre_v)))
    cum = -rate[...] * soft
    lane8 = lane[0:8, :]
    for shift in (1, 2, 4, 8, 16, 32, 64):
        cum = cum + jnp.where(lane8 >= shift, pltpu.roll(cum, shift, 1), 0.0)
    total = jnp.broadcast_to(cum[:, 127:128], (8, 128))
    factor = jnp.exp(total)
    cum_t = cum.T
    from_start_t = jnp.exp(cum).T
    to_end_t = jnp.exp(total - cum).T

    def spread(columns, pair):
        return jnp.where(first_head, columns[:, 2 * pair : 2 * pair + 1], columns[:, 2 * pair + 1 : 2 * pair + 2])

    def factor_row(pair):
        return jnp.where(first_head, factor[2 * pair : 2 * pair + 1, :], factor[2 * pair + 1 : 2 * pair + 2, :])

    q, k = q_in[...], k_in[...]
    q_t = q.astype(F32).T.astype(BF16)
    k_t = k.astype(F32).T.astype(BF16)

    for pair in range(PAIRS):
        scaled = spread(from_start_t, pair) * cot[:, cols(pair)].astype(F32)
        ys_b[pair, 0:128, :] = dot_fine_right(q_t, scaled)
        ys_b[pair, 128:136, :] = jnp.broadcast_to(factor_row(pair), (8, 128))
    yr_b[y] = ys_b[y]
    pl.semaphore_wait(barrier, NY + NZ + NX - 2)

    def send_y(kind, src, dst):
        for o in range(1, NY):
            send(src.at[peer_y(o)], dst.at[y], y_sem.at[0, kind, peer_y(o)], y_sem.at[1, kind, y], y=peer_y(o))

    def wait_y(kind, dst):
        for o in range(1, NY):
            arrived(dst.at[peer_y(o)], y_sem.at[1, kind, peer_y(o)])

    def send_z(kind, src, dst):
        for o in range(1, NZ):
            send(src.at[peer_z(o)], dst.at[z], z_sem.at[0, kind, peer_z(o)], z_sem.at[1, kind, z], z=peer_z(o))

    def wait_z(kind, dst):
        for o in range(1, NZ):
            arrived(dst.at[peer_z(o)], z_sem.at[1, kind, peer_z(o)])

    send_y(0, ys_b, yr_b)

    for half in range(2):
        span = slice(256 * half, 256 * half + 256)
        vals[:, span] = dot(hid[...], w[:, span]).astype(BF16)
    for pair in range(PAIRS):
        scaled = spread(to_end_t, pair) * vals[:, cols(pair)].astype(F32)
        ys_f[pair, 0:128, :] = dot_fine_right(k_t, scaled)
        ys_f[pair, 128:136, :] = jnp.broadcast_to(factor_row(pair), (8, 128))
    yr_f[y] = ys_f[y]
    send_y(1, ys_f, yr_f)

    def scan_plane(got, kept, z_send, reverse):
        state, gain = None, None
        order = range(NY - 1, -1, -1) if reverse else range(NY)
        for block in order:
            value, here = got[block, 0:128, :], got[block, 128:129, :]
            if state is None:
                kept[block] = jnp.zeros((128, 128), F32)
                state, gain = value, here
            else:
                kept[block] = state
                state, gain = here * state + value, gain * here
        for row in range(NZ):
            z_send[row, 0:ROWS, :] = state[row * ROWS : row * ROWS + ROWS, :]
            z_send[row, ROWS : ROWS + 8, :] = jnp.broadcast_to(gain, (8, 128))

    def scan_z(got, back, reverse):
        state = None
        for plane in range(NZ - 1, -1, -1) if reverse else range(NZ):
            value, here = got[plane, 0:ROWS, :], got[plane, ROWS : ROWS + 1, :]
            if state is None:
                back[plane] = jnp.zeros((ROWS, 128), F32)
                state = value
            else:
                back[plane] = state
                state = here * state + value

    def finish_plane(got, kept, plane_in, reverse):
        incoming = plane_in[...].reshape(STATE, 128)
        gain = None
        for block in range(NY - 1, -1, -1) if reverse else range(NY):
            kept[block] = kept[block] + (incoming if gain is None else gain * incoming)
            here = got[block, 128:129, :]
            gain = here if gain is None else gain * here

    wait_y(0, yr_b)
    scan_plane(yr_b, ybs_b, zs_b, True)
    zr_b[z] = zs_b[z]
    send_z(0, zs_b, zr_b)

    for block in range(16):
        turned = hid[:, cols(block)].astype(F32).T
        hid_t[block // 2, 2 * (block % 2) : 2 * (block % 2) + 2] = turned.reshape(2, 64, 128)
    for o in range(1, NY):
        send(hid_t.at[:, peer_y(o)], hid_r.at[y], y_sem.at[0, 2, peer_y(o)], y_sem.at[1, 2, y], y=peer_y(o))
    hid_r[y] = hid_t[:, y]

    wait_y(1, yr_f)
    scan_plane(yr_f, ybs_f, zs_f, False)
    zr_f[z] = zs_f[z]
    send_z(1, zs_f, zr_f)

    wait_z(0, zr_b)
    scan_z(zr_b, zbs_b, True)
    zbr_b[z] = zbs_b[z]
    send_z(2, zbs_b, zbr_b)

    score = dot(k, q, ((1,), (1,)))
    causal = lax.broadcasted_iota(jnp.int32, (128, 128), 0) <= lane
    blend = jnp.zeros((128, 128), F32)
    for pair in range(PAIRS):
        cot_pair, val_pair = cot[:, cols(pair)], vals[:, cols(pair)]
        inner = jnp.zeros((128, 128), F32)
        for side in range(2):
            head = 2 * pair + side
            mine = first_head if side == 0 else jnp.logical_not(first_head)
            across = jnp.where(causal, cum[head : head + 1, :] - cum_t[:, head : head + 1], 0.0)
            damping = jnp.where(causal, jnp.exp(across), 0.0)
            weight = score * damping
            cot_head = jnp.where(mine, cot_pair.astype(F32), 0.0).astype(BF16)
            inner = inner + dot_fine_left(weight, cot_head)
            moved = dot(val_pair, cot_head, ((1,), (1,)))
            blend = blend + moved * damping
            row_sum[head : head + 1, :] = jnp.sum(moved * weight, axis=0, keepdims=True)
        gv_in[pair] = inner

    wait_z(2, zbr_b)
    finish_plane(yr_b, ybs_b, zbr_b, True)
    ybr_b[y] = ybs_b[y]
    send_y(3, ybs_b, ybr_b)

    wait_z(1, zr_f)
    scan_z(zr_f, zbs_f, False)
    zbr_f[z] = zbs_f[z]
    send_z(3, zbs_f, zbr_f)

    blend_t = blend.T
    gk = dot_fine_left(blend, q)
    gq = dot_fine_left(blend_t, k)

    wait_y(3, ybr_b)
    for pair in range(PAIRS):
        pull = ybr_b[pair]
        from_state = spread(to_end_t, pair) * dot_fine_right(k, pull)
        gv_out_pair = gv_in[pair] + from_state
        ag_s[pair] = gv_out_pair.astype(BF16).astype(F32)
        for o in range(1, NY):
            send(ag_s.at[pair], ag_r.at[pair, y], ag_sem.at[0, pair, peer_y(o)], ag_sem.at[1, pair, y], y=peer_y(o))
        ag_r[pair, y] = ag_s[pair]
        gv_in[pair] = gv_out_pair
    grad_v = jnp.concatenate([ag_s[pair].astype(BF16) for pair in range(PAIRS)], axis=1)

    for part_now in range(4):
        span = slice(512 * part_now, 512 * part_now + 512)
        gh_s[:, :, :, span] = dot(grad_v, w[span, :], ((1,), (1,))).reshape(NX, 2, 16, 512)
    send(gh_s.at[:, 1 - c], gh_r, d_sem.at[0], d_sem.at[1], c=1 - c)

    wait_z(3, zbr_f)
    finish_plane(yr_f, ybs_f, zbr_f, False)
    ybr_f[y] = ybs_f[y]
    send_y(4, ybs_f, ybr_f)

    wait_y(2, hid_r)
    for block in range(NY):
        hid_all[:, cols(block)] = hid_r[block].reshape(512, 128).astype(BF16)

    def steps(pair, way):
        return 4 if (pair + way) % 2 == 0 else 3

    def ring_target(pair, way, step):
        n = steps(pair, way)
        return peer_z(n - step) if way == 0 else peer_z(NZ - n + step)

    def ring_send(src, pair, way, step):
        send(
            src, ring_r.at[way, pair, step], ring_sem.at[0, way, pair, step], ring_sem.at[1, way, pair, step],
            z=peer_z(1) if way == 0 else peer_z(NZ - 1),
        )

    def ring_step(pair, way, step):
        arrived(ring_r.at[way, pair, step - 1], ring_sem.at[1, way, pair, step - 1])
        if step < steps(pair, way):
            ring_s[way, pair, step] = ring_r[way, pair, step - 1] + part[pair, ring_target(pair, way, step)]
            ring_send(ring_s.at[way, pair, step], pair, way, step)

    for pair in range(PAIRS):
        for o in range(1, NY):
            arrived(ag_r.at[pair, peer_y(o)], ag_sem.at[1, pair, peer_y(o)])
        gathered = ag_r[pair].reshape(512, 128).astype(BF16)
        part[pair] = dot(hid_all[...], gathered).reshape(NZ, 64, 128)
        for way in range(2):
            ring_send(part.at[pair, ring_target(pair, way, 0)], pair, way, 0)
        if pair == 0:
            arrived(gh_r, d_sem.at[1])
            gx_s[...] = gh_s[:, c] + gh_r[...]
            for o in range(1, NX):
                send(gx_s.at[peer_x(o)], gx_r.at[x], x_sem.at[0, peer_x(o)], x_sem.at[1, x], x=peer_x(o))
            gx_r[x] = gx_s[x]

    for step in range(1, 4):
        for pair in range(PAIRS):
            for way in range(2):
                if step <= steps(pair, way):
                    ring_step(pair, way, step)
        if step == 1:
            wait_y(4, ybr_f)
            gap = jnp.zeros((8, 128), F32)
            shared = jnp.zeros((8, 128), F32)
            head_row = lax.broadcasted_iota(jnp.int32, (8, 128), 0)
            for pair in range(PAIRS):
                carry, pull = ybr_f[pair], ybr_b[pair]
                cot_f = cot[:, cols(pair)].astype(F32)
                val_f = vals[:, cols(pair)].astype(F32)
                cot_scaled = spread(from_start_t, pair) * cot_f
                val_scaled = spread(to_end_t, pair) * val_f
                gq = gq + dot_fine(cot_scaled, carry, ((1,), (1,)))
                gk = gk + dot_fine(val_scaled, pull, ((1,), (1,)))
                out_carried = dot_fine_right(q, carry)
                from_state = dot_fine_right(k, pull)
                owner = head_row == 2 * pair + (lane8 >= 64).astype(jnp.int32)
                chooser = jnp.where(owner, 1.0, 0.0)
                change = cot_scaled * out_carried - val_f * gv_in[pair]
                gap = gap + lax.dot_general(
                    chooser, change, (((1,), (1,)), ((), ())),
                    precision=lax.Precision.HIGHEST, preferred_element_type=F32,
                )
                whole = jnp.sum(val_scaled * from_state, axis=0, keepdims=True)
                whole = whole + factor_row(pair) * jnp.sum(carry * pull, axis=0, keepdims=True)
                shared = shared + jnp.sum(chooser * whole, axis=1, keepdims=True)
            gap = gap + row_sum[...]
            for shift in (1, 2, 4, 8, 16, 32, 64):
                gap = gap + jnp.where(lane8 < 128 - shift, pltpu.roll(gap, 128 - shift, 1), 0.0)
            gd_out[...] = (gap + shared) * (-rate[...] / (1.0 + jnp.exp(-pre_v)))
            gk_out[...] = gk.astype(BF16)
            gq_out[...] = gq.astype(BF16)
        if step == 2:
            for o in range(1, NX):
                arrived(gx_r.at[peer_x(o)], x_sem.at[1, peer_x(o)])
            gh_out[...] = (gx_r[0] + gx_r[1] + gx_r[2] + gx_r[3]).astype(BF16)

    for pair in range(PAIRS):
        for way in range(2):
            if steps(pair, way) == 4:
                ring_step(pair, way, 4)
        last = [steps(pair, way) - 1 for way in range(2)]
        gw_out[:, cols(pair)] = part[pair, z] + ring_r[0, pair, last[0]] + ring_r[1, pair, last[1]]

    for made in sent:
        made.wait_send()


def local(hidden, value_weight, key_vecs, queries, decay_pre, decay_rate, cotangent):
    vmem = pl.BlockSpec(memory_space=pltpu.VMEM)
    dma = pltpu.SemaphoreType.DMA
    f32 = lambda *shape: pltpu.VMEM(shape, F32)
    y_box, z_box = (NY, STATE + 8, 128), (NZ, ROWS + 8, 128)
    z_back, y_back = (NZ, ROWS, 128), (NY, STATE, 128)
    outs = pl.pallas_call(
        kernel,
        out_shape=(
            jax.ShapeDtypeStruct((TOK, STATE), BF16),
            jax.ShapeDtypeStruct((TOK, STATE), BF16),
            jax.ShapeDtypeStruct((HEADS, TOK), F32),
            jax.ShapeDtypeStruct((16, 2048), BF16),
            jax.ShapeDtypeStruct((64, 512), F32),
        ),
        in_specs=[vmem] * 7,
        out_specs=[vmem] * 5,
        scratch_shapes=[
            *[f32(*y_box)] * 4,
            *[f32(*z_box)] * 4,
            *[f32(*z_back)] * 4,
            *[f32(*y_back)] * 4,
            f32(NZ, NY, 64, TOK),
            f32(NY, NZ, 64, TOK),
            pltpu.VMEM((512, 512), BF16),
            f32(PAIRS, TOK, 128),
            f32(PAIRS, NY, TOK, 128),
            f32(PAIRS, NZ, 64, 128),
            f32(2, PAIRS, 4, 64, 128),
            f32(2, PAIRS, 4, 64, 128),
            f32(NX, 2, 16, 2048),
            f32(NX, 16, 2048),
            f32(NX, 16, 2048),
            f32(NX, 16, 2048),
            f32(PAIRS, TOK, 128),
            pltpu.VMEM((TOK, 512), BF16),
            f32(HEADS, TOK),
            dma((2, 5, NY)),
            dma((2, 4, NZ)),
            dma((2, PAIRS, NY)),
            dma((2, 2, PAIRS, 4)),
            dma((2,)),
            dma((2, NX)),
        ],
        compiler_params=pltpu.CompilerParams(
            collective_id=0, has_side_effects=True, vmem_limit_bytes=48 * 1024 * 1024
        ),
        name="mixer_backward",
    )(
        hidden,
        value_weight,
        key_vecs.reshape(TOK, STATE),
        queries.reshape(TOK, STATE),
        decay_pre.T,
        jnp.broadcast_to(decay_rate[:, None], (HEADS, TOK)),
        cotangent.reshape(TOK, 512),
    )
    gk, gq, gd, gh, gw = outs
    return gk.reshape(TOK, 1, STATE), gq.reshape(TOK, 1, STATE), gd.T, gh, gw


def solution(mesh):
    split = Mesh(mesh.devices.reshape(NZ, NY, NX, 2), ("z", "y", "x", "c"))
    placed = (
        P(SP, None),
        P(None, TP),
        P(SP, TP, None),
        P(SP, TP, None),
        P(SP, TP),
        P(TP),
        P(SP, TP, None),
    )
    return jax.shard_map(
        local,
        mesh=split,
        in_specs=placed,
        out_specs=(P(SP, TP, None), P(SP, TP, None), P(SP, TP), P(SP + TP, None), P(SP, TP)),
        check_vma=False,
    )
```

```python
import contextlib

import jax
import jax.numpy as jnp
from jax import lax
from jax.experimental import pallas as pl
from jax.experimental.pallas import tpu as pltpu
from jax.sharding import Mesh
from jax.sharding import PartitionSpec as P

F32, BF16 = jnp.float32, jnp.bfloat16
MESH = pl.DeviceIdType.MESH
SP, TP = ("z", "y"), ("x", "c")
NZ, NY, NX = 8, 4, 4
TOK, STATE, PAIRS, HEADS = 128, 128, 4, 8
ROWS = STATE // NZ
VMEM_LIMIT = 65 * 1024 * 1000


def dot(a, b, dims=((1,), (0,))):
    return lax.dot_general(a, b, (dims, ((), ())), preferred_element_type=F32)


def halves(a):
    high = a.astype(BF16)
    return high, (a - high.astype(F32)).astype(BF16)


def dot_fine_right(a, b, dims=((1,), (0,))):
    high, low = halves(b)
    return dot(a, high, dims) + dot(a, low, dims)


def dot_fine_left(a, b, dims=((1,), (0,))):
    high, low = halves(a)
    return dot(high, b, dims) + dot(low, b, dims)


def dot_fine(a, b, dims=((1,), (0,))):
    a_high, a_low = halves(a)
    b_high, b_low = halves(b)
    return dot(a_high, b_high, dims) + dot(a_high, b_low, dims) + dot(a_low, b_high, dims)


def cols(pair):
    return slice(128 * pair, 128 * pair + 128)


def kernel(
    hid_at, w_at, k_at, q_at, pre_at, rate_at, cot_at,
    gk_at, gq_at, gd_at, gh_at, gw_at,
    ys_b, yr_b, ys_f, yr_f, zs_b, zr_b, zs_f, zr_f,
    zbs_b, zbr_b, zbs_f, zbr_f, ybs_b, ybr_b, ybs_f, ybr_f,
    hid_t, hid_p, hid_x, hid_c, hid_all, gv_s, gv_r, part, ring_s, ring_r,
    gh_s, gh_r, gx_s, gx_r, zg_s, zg_r, k_s, k_r, cum_s, cum_r, fade, gv_own, vals, row_sum,
    gk_out, gq_out, gd_out, gh_out, gw_out,
    hid, w, k_in, q_in, pre, rate_in, cot_t, cot,
    y_sem, z_sem, ag_sem, ring_sem, d_sem, x_sem, in_sem, h_sem, out_sem, zg_sem,
):
    z, y = lax.axis_index("z"), lax.axis_index("y")
    x, c = lax.axis_index("x"), lax.axis_index("c")
    lane = lax.broadcasted_iota(jnp.int32, (128, 128), 1)
    first_head = lane[0:1, :] < 64
    sent, stored = [], []
    stack = contextlib.ExitStack()

    def phase(name):
        stack.close()
        stack.enter_context(jax.named_scope(name))

    def put(src, dst, at):
        made = pltpu.make_async_copy(src, dst, out_sem.at[at])
        made.start()
        stored.append(made)

    def peer_y(o):
        return lax.rem(y + o, NY)

    def peer_z(o):
        return lax.rem(z + o, NZ)

    def peer_x(o):
        return lax.rem(x + o, NX)

    def copy(src, dst, s_sem, r_sem, **where):
        return pltpu.make_async_remote_copy(
            src_ref=src, dst_ref=dst, send_sem=s_sem, recv_sem=r_sem, device_id=where, device_id_type=MESH
        )

    def send(src, dst, s_sem, r_sem, **where):
        made = copy(src, dst, s_sem, r_sem, **where)
        made.start()
        sent.append(made)

    def arrived(dst, r_sem):
        copy(dst, dst, r_sem, r_sem, c=1 - c).wait_recv()

    def send_y(kind, src, dst):
        for o in range(1, NY):
            send(src.at[peer_y(o)], dst.at[y], y_sem.at[0, kind, peer_y(o)], y_sem.at[1, kind, y], y=peer_y(o))

    def share_y(kind, src, dst):
        for o in range(1, NY):
            send(src, dst.at[y], y_sem.at[0, kind, peer_y(o)], y_sem.at[1, kind, y], y=peer_y(o))

    def wait_y(kind, dst):
        for o in range(1, NY):
            arrived(dst.at[peer_y(o)], y_sem.at[1, kind, peer_y(o)])

    def send_z(kind, src, dst):
        for o in range(1, NZ):
            send(src.at[peer_z(o)], dst.at[z], z_sem.at[0, kind, peer_z(o)], z_sem.at[1, kind, z], z=peer_z(o))

    def wait_z(kind, dst):
        for o in range(1, NZ):
            arrived(dst.at[peer_z(o)], z_sem.at[1, kind, peer_z(o)])

    phase("enter")
    loads = [
        pltpu.make_async_copy(src, dst, in_sem.at[i])
        for i, (src, dst) in enumerate(
            [(pre_at, pre), (rate_at, rate_in), (cot_at, cot_t), (q_at, q_in), (k_at, k_in), (hid_at, hid), (w_at, w)]
        )
    ]
    for made in loads:
        made.start()

    barrier = pltpu.get_barrier_semaphore()
    for o in range(1, NY):
        pl.semaphore_signal(barrier, inc=1, device_id={"y": peer_y(o)}, device_id_type=MESH)
    for o in range(1, NZ):
        pl.semaphore_signal(barrier, inc=1, device_id={"z": peer_z(o)}, device_id_type=MESH)
    for o in range(1, NX):
        pl.semaphore_signal(barrier, inc=1, device_id={"x": peer_x(o)}, device_id_type=MESH)
    pl.semaphore_signal(barrier, inc=1, device_id={"c": 1 - c}, device_id_type=MESH)

    phase("decay")
    loads[0].wait()
    loads[1].wait()
    pre_v = pre[...]
    square = lax.broadcasted_iota(jnp.int32, (8, 8), 0) == lax.broadcasted_iota(jnp.int32, (8, 8), 1)
    rate = jnp.sum(jnp.where(square, jnp.broadcast_to(rate_in[...], (8, 8)), 0.0), axis=1, keepdims=True)
    soft = jnp.maximum(pre_v, 0.0) + jnp.log1p(jnp.exp(-jnp.abs(pre_v)))
    cum = -rate * soft
    lane8 = lane[0:8, :]
    for shift in (1, 2, 4, 8, 16, 32, 64):
        cum = cum + jnp.where(lane8 >= shift, pltpu.roll(cum, shift, 1), 0.0)
    cum_s[...] = cum
    cum_r[y] = cum
    total = jnp.broadcast_to(cum[:, 127:128], (8, 128))
    factor = jnp.exp(total)
    cum_t = cum.T
    from_start = jnp.exp(cum)
    from_start_t = from_start.T
    to_end_t = jnp.exp(total - cum).T

    def spread(columns, pair):
        return jnp.where(first_head, columns[:, 2 * pair : 2 * pair + 1], columns[:, 2 * pair + 1 : 2 * pair + 2])

    def row_of(gains, pair):
        return jnp.where(first_head, gains[2 * pair : 2 * pair + 1, :], gains[2 * pair + 1 : 2 * pair + 2, :])

    phase("pull")
    loads[2].wait()
    loads[3].wait()
    q = q_in[...]
    q_t = q.astype(F32).T.astype(BF16)
    upper = lax.broadcasted_iota(jnp.int32, (128, 128), 0) < 64
    for pair in range(PAIRS):
        growth = jnp.where(upper, from_start[2 * pair : 2 * pair + 1, :], from_start[2 * pair + 1 : 2 * pair + 2, :])
        scaled = growth * cot_t[cols(pair), :].astype(F32)
        ys_b[pair, 0:128, :] = dot_fine_right(q_t, scaled, ((1,), (1,)))
        ys_b[pair, 128:136, :] = jnp.broadcast_to(row_of(factor, pair), (8, 128))
    yr_b[y] = ys_b[y]
    loads[4].wait()
    k = k_in[...]
    k_s[...] = k.astype(F32)
    k_r[y] = k_s[...]

    phase("barrier")
    pl.semaphore_wait(barrier, NY + NZ + NX - 2)
    send_y(0, ys_b, yr_b)

    phase("hidden")
    loads[5].wait()
    for block in range(16):
        turned = hid[:, cols(block)].astype(F32).T
        hid_t[block // 2, 2 * (block % 2) : 2 * (block % 2) + 2] = turned.reshape(2, 64, 128)
    seat = 2 * x + c
    for o in range(1, NY):
        send(hid_t.at[seat, peer_y(o)], hid_p.at[y], y_sem.at[0, 2, peer_y(o)], y_sem.at[1, 2, y], y=peer_y(o))
    hid_p[y] = hid_t[seat, y]
    share_y(5, k_s, k_r)
    share_y(6, cum_s, cum_r)

    phase("values")
    loads[6].wait()
    k_t = k_s[...].T.astype(BF16)
    for half in range(2):
        span = slice(256 * half, 256 * half + 256)
        vals[:, span] = dot(hid[...], w[:, span]).astype(BF16)
    for pair in range(PAIRS):
        scaled = spread(to_end_t, pair) * vals[:, cols(pair)].astype(F32)
        ys_f[pair, 0:128, :] = dot_fine_right(k_t, scaled)
        ys_f[pair, 128:136, :] = jnp.broadcast_to(row_of(factor, pair), (8, 128))
    yr_f[y] = ys_f[y]

    phase("block")
    for pair in range(PAIRS):
        cot[:, cols(pair)] = cot_t[cols(pair), :].astype(F32).T.astype(BF16)
    score = dot(k, q, ((1,), (1,)))
    causal = lax.broadcasted_iota(jnp.int32, (128, 128), 0) <= lane
    blend = jnp.zeros((128, 128), F32)
    for pair in range(PAIRS):
        cot_pair, val_pair = cot[:, cols(pair)], vals[:, cols(pair)]
        inner = jnp.zeros((128, 128), F32)
        for side in range(2):
            head = 2 * pair + side
            mine = first_head if side == 0 else jnp.logical_not(first_head)
            across = jnp.where(causal, cum[head : head + 1, :] - cum_t[:, head : head + 1], 0.0)
            damping = jnp.where(causal, jnp.exp(across), 0.0)
            weight = score * damping
            cot_head = jnp.where(mine, cot_pair.astype(F32), 0.0).astype(BF16)
            inner = inner + dot_fine_left(weight, cot_head)
            moved = dot(val_pair, cot_head, ((1,), (1,)))
            blend = blend + moved * damping
            row_sum[head : head + 1, :] = jnp.sum(moved * weight, axis=0, keepdims=True)
        gv_s[pair] = inner

    def scan_plane(got, kept, z_send, reverse):
        state, gain = None, None
        order = range(NY - 1, -1, -1) if reverse else range(NY)
        for block in order:
            value, here = got[block, 0:128, :], got[block, 128:129, :]
            if state is None:
                kept[block] = jnp.zeros((128, 128), F32)
                state, gain = value, here
            else:
                kept[block] = state
                state, gain = here * state + value, gain * here
        for row in range(NZ):
            z_send[row, 0:ROWS, :] = state[row * ROWS : row * ROWS + ROWS, :]
            z_send[row, ROWS : ROWS + 8, :] = jnp.broadcast_to(gain, (8, 128))

    def scan_z(got, back, reverse):
        state = None
        for plane in range(NZ - 1, -1, -1) if reverse else range(NZ):
            value, here = got[plane, 0:ROWS, :], got[plane, ROWS : ROWS + 1, :]
            if state is None:
                back[plane] = jnp.zeros((ROWS, 128), F32)
                state = value
            else:
                back[plane] = state
                state = here * state + value

    def finish_plane(got, kept, plane_in, reverse):
        incoming = plane_in[...].reshape(STATE, 128)
        gain = None
        for block in range(NY - 1, -1, -1) if reverse else range(NY):
            kept[block] = kept[block] + (incoming if gain is None else gain * incoming)
            here = got[block, 128:129, :]
            gain = here if gain is None else gain * here

    phase("scan_y_b")
    wait_y(0, yr_b)
    scan_plane(yr_b, ybs_b, zs_b, True)
    zr_b[z] = zs_b[z]
    send_z(0, zs_b, zr_b)
    ybr_b[y] = ybs_b[y]
    send_y(3, ybs_b, ybr_b)
    send_y(1, ys_f, yr_f)

    phase("hidden_x")
    wait_y(2, hid_p)
    for o in range(1, NX):
        send(hid_p, hid_x.at[x], h_sem.at[0, peer_x(o)], h_sem.at[1, x], x=peer_x(o))
    hid_x[x] = hid_p[...]

    phase("scan_z_b")
    wait_z(0, zr_b)
    scan_z(zr_b, zbs_b, True)
    zbr_b[z] = zbs_b[z]
    send_z(2, zbs_b, zbr_b)

    phase("wait_suffix")
    wait_y(3, ybr_b)
    phase("gv_plane")
    for pair in range(PAIRS):
        gv_s[pair] = gv_s[pair] + spread(to_end_t, pair) * dot_fine_right(k, ybr_b[pair])
    for slot in range(PAIRS):
        for o in range(1, NY):
            send(
                gv_s.at[peer_y(o + slot)], gv_r.at[slot, y], ag_sem.at[0, slot, peer_y(o)], ag_sem.at[1, slot, y],
                y=peer_y(o),
            )
        gv_r[slot, y] = gv_s[peer_y(slot)]

    phase("scan_y_f")
    wait_y(1, yr_f)
    scan_plane(yr_f, ybs_f, zs_f, False)
    zr_f[z] = zs_f[z]
    send_z(1, zs_f, zr_f)

    phase("hidden_c")
    for o in range(1, NX):
        arrived(hid_x.at[peer_x(o)], h_sem.at[1, peer_x(o)])
    send(hid_x, hid_c, d_sem.at[0, 1], d_sem.at[1, 1], c=1 - c)

    phase("fade")
    wait_y(5, k_r)
    wait_y(6, cum_r)
    tail = jnp.zeros((8, 1), F32)
    tail_own = jnp.zeros((8, 1), F32)
    for block in range(NY - 1, -1, -1):
        here = cum_r[block]
        tail_own = jnp.where(y == block, tail, tail_own)
        tail = tail + here[:, 127:128]
        fade_t = jnp.exp(tail - here).T
        for pair in range(PAIRS):
            fade[block, pair] = spread(fade_t, pair)
    gain_own = jnp.exp(jnp.broadcast_to(tail_own, (8, 128)))
    k_all = k_r[...].reshape(512, 128).astype(BF16)
    arrived(hid_c, d_sem.at[1, 1])
    for across_x in range(NX):
        for block in range(NY):
            hid_all[across_x, c, :, cols(block)] = hid_x[across_x, block].astype(BF16)
            hid_all[across_x, 1 - c, :, cols(block)] = hid_c[across_x, block].astype(BF16)

    phase("wait_zg")
    wait_z(2, zbr_b)
    zg_s[...] = zbr_b[...].reshape(STATE, 128)
    zg_r[0] = zg_s[...]
    for o in range(1, NY):
        send(zg_s, zg_r.at[NY - o], zg_sem.at[0, NY - o], zg_sem.at[1, NY - o], y=peer_y(o))

    def steps(slot, way):
        return 4 if (slot + way) % 2 == 0 else 3

    def ring_target(slot, way, step):
        n = steps(slot, way)
        return peer_z(n - step) if way == 0 else peer_z(NZ - n + step)

    def ring_send(src, slot, way, step):
        send(
            src, ring_r.at[way, slot, step], ring_sem.at[0, way, slot, step], ring_sem.at[1, way, slot, step],
            z=peer_z(1) if way == 0 else peer_z(NZ - 1),
        )

    def ring_step(slot, way, step):
        if not 1 <= step <= steps(slot, way):
            return
        arrived(ring_r.at[way, slot, step - 1], ring_sem.at[1, way, slot, step - 1])
        if step < steps(slot, way):
            ring_s[way, slot, step] = ring_r[way, slot, step - 1] + part[slot, ring_target(slot, way, step)]
            ring_send(ring_s.at[way, slot, step], slot, way, step)

    def weight_slot(slot):
        pair = peer_y(slot)
        if slot > 0:
            arrived(zg_r.at[slot], zg_sem.at[1, slot])
        for o in range(1, NY):
            arrived(gv_r.at[slot, peer_y(o)], ag_sem.at[1, slot, peer_y(o)])
        phase(f"weight{slot}")
        fresh = dot_fine_right(k_all, zg_r[slot])
        for block in range(NY):
            gv_r[slot, block] = gv_r[slot, block] + fade[block, pair] * fresh[128 * block : 128 * block + 128, :]
        gv_own[pair] = gv_r[slot, y]
        gathered = gv_r[slot].reshape(512, 128).astype(BF16)
        part[slot] = dot(hid_all[...].reshape(512, 512), gathered).reshape(NZ, 64, 128)
        for way in range(2):
            ring_send(part.at[slot, ring_target(slot, way, 0)], slot, way, 0)

    phase("wait_ag0")
    weight_slot(0)

    phase("scan_z_f")
    wait_z(1, zr_f)
    scan_z(zr_f, zbs_f, False)
    zbr_f[z] = zbs_f[z]
    send_z(3, zbs_f, zbr_f)

    phase("ring0_1")
    for way in range(2):
        ring_step(0, way, 1)

    phase("back_y_f")
    wait_z(3, zbr_f)
    finish_plane(yr_f, ybs_f, zbr_f, False)
    ybr_f[y] = ybs_f[y]
    send_y(4, ybs_f, ybr_f)

    phase("ring0_2")
    for way in range(2):
        ring_step(0, way, 2)

    for slot in range(1, PAIRS):
        phase(f"wait_ag{slot}")
        weight_slot(slot)

    phase("grad_h")
    grad_v = jnp.concatenate([gv_own[pair].astype(BF16) for pair in range(PAIRS)], axis=1)
    for part_now in range(4):
        span = slice(512 * part_now, 512 * part_now + 512)
        gh_s[:, :, :, span] = dot(grad_v, w[span, :], ((1,), (1,))).reshape(NX, 2, 16, 512)
    send(gh_s.at[:, 1 - c], gh_r, d_sem.at[0, 0], d_sem.at[1, 0], c=1 - c)

    def ring_turn(step):
        phase(f"ring{step}")
        for slot in range(PAIRS):
            for way in range(2):
                ring_step(slot, way, step + 2 if slot == 0 else step)

    ring_turn(1)
    phase("chip_pair")
    arrived(gh_r, d_sem.at[1, 0])
    gx_s[...] = gh_s[:, c] + gh_r[...]
    for o in range(1, NX):
        send(gx_s.at[peer_x(o)], gx_r.at[x], x_sem.at[0, peer_x(o)], x_sem.at[1, x], x=peer_x(o))
    gx_r[x] = gx_s[x]
    ring_turn(2)

    phase("grad_kq")
    wait_y(4, ybr_f)
    gk = dot_fine_left(blend, q)
    gq = dot_fine_left(blend.T, k)
    gap = jnp.zeros((8, 128), F32)
    shared = jnp.zeros((8, 128), F32)
    head_row = lax.broadcasted_iota(jnp.int32, (8, 128), 0)
    for pair in range(PAIRS):
        carry = ybr_f[pair]
        pull = ybr_b[pair] + row_of(gain_own, pair) * zg_r[lax.rem(pair + NY - y, NY)]
        cot_f = cot[:, cols(pair)].astype(F32)
        val_f = vals[:, cols(pair)].astype(F32)
        cot_scaled = spread(from_start_t, pair) * cot_f
        val_scaled = spread(to_end_t, pair) * val_f
        gq = gq + dot_fine(cot_scaled, carry, ((1,), (1,)))
        gk = gk + dot_fine(val_scaled, pull, ((1,), (1,)))
        out_carried = dot_fine_right(q, carry)
        from_state = dot_fine_right(k, pull)
        owner = head_row == 2 * pair + (lane8 >= 64).astype(jnp.int32)
        chooser = jnp.where(owner, 1.0, 0.0)
        change = cot_scaled * out_carried - val_f * gv_own[pair]
        gap = gap + lax.dot_general(
            chooser, change, (((1,), (1,)), ((), ())),
            precision=lax.Precision.HIGHEST, preferred_element_type=F32,
        )
        whole = jnp.sum(val_scaled * from_state, axis=0, keepdims=True)
        whole = whole + row_of(factor, pair) * jnp.sum(carry * pull, axis=0, keepdims=True)
        shared = shared + jnp.sum(chooser * whole, axis=1, keepdims=True)
    gap = gap + row_sum[...]
    for shift in (1, 2, 4, 8, 16, 32, 64):
        gap = gap + jnp.where(lane8 < 128 - shift, pltpu.roll(gap, 128 - shift, 1), 0.0)
    gd_out[...] = (gap + shared) * (-rate / (1.0 + jnp.exp(-pre_v)))
    gk_out[...] = gk.astype(BF16)
    gq_out[...] = gq.astype(BF16)
    put(gk_out, gk_at, 0)
    put(gq_out, gq_at, 1)
    put(gd_out, gd_at, 2)

    ring_turn(3)
    phase("out_h")
    for o in range(1, NX):
        arrived(gx_r.at[peer_x(o)], x_sem.at[1, peer_x(o)])
    gh_out[...] = (gx_r[0] + gx_r[1] + gx_r[2] + gx_r[3]).astype(BF16)
    put(gh_out, gh_at, 3)

    ring_turn(4)
    for slot in range(PAIRS):
        last = [steps(slot, way) - 1 for way in range(2)]
        gw_out[slot] = part[slot, z] + ring_r[0, slot, last[0]] + ring_r[1, slot, last[1]]
        put(gw_out.at[slot], gw_at.at[:, pl.ds(pl.multiple_of(128 * peer_y(slot), 128), 128)], 4 + slot)

    phase("drain")
    for made in sent:
        made.wait_send()
    for made in stored:
        made.wait()
    stack.close()


def store_all(*refs):
    sems = refs[15]
    taken = [pltpu.make_async_copy(refs[i], refs[10 + i], sems.at[0, i]) for i in range(5)]
    given = [pltpu.make_async_copy(refs[10 + i], refs[5 + i], sems.at[1, i]) for i in range(5)]
    for made in taken:
        made.start()
    for take, give in zip(taken, given):
        take.wait()
        give.start()
    for made in given:
        made.wait()


def local(hidden, value_weight, key_vecs, queries, decay_pre, decay_rate, cotangent):
    dma = pltpu.SemaphoreType.DMA
    f32 = lambda *shape: pltpu.VMEM(shape, F32)
    y_box, z_box = (NY, STATE + 8, 128), (NZ, ROWS + 8, 128)
    z_back, y_back = (NZ, ROWS, 128), (NY, STATE, 128)
    outs = pl.pallas_call(
        kernel,
        out_shape=(
            jax.ShapeDtypeStruct((TOK, STATE), BF16),
            jax.ShapeDtypeStruct((TOK, STATE), BF16),
            jax.ShapeDtypeStruct((HEADS, TOK), F32),
            jax.ShapeDtypeStruct((16, 2048), BF16),
            jax.ShapeDtypeStruct((64, 512), F32),
        ),
        in_specs=[pl.BlockSpec(memory_space=pl.ANY)] * 7,
        out_specs=[pl.BlockSpec(memory_space=pl.ANY)] * 5,
        scratch_shapes=[
            *[f32(*y_box)] * 4,
            *[f32(*z_box)] * 4,
            *[f32(*z_back)] * 4,
            *[f32(*y_back)] * 4,
            f32(NZ, NY, 64, TOK),
            f32(NY, 64, TOK),
            f32(NX, NY, 64, TOK),
            f32(NX, NY, 64, TOK),
            pltpu.VMEM((NX, 2, 64, 512), BF16),
            f32(PAIRS, TOK, 128),
            f32(PAIRS, NY, TOK, 128),
            f32(PAIRS, NZ, 64, 128),
            f32(2, PAIRS, 4, 64, 128),
            f32(2, PAIRS, 4, 64, 128),
            f32(NX, 2, 16, 2048),
            f32(NX, 16, 2048),
            f32(NX, 16, 2048),
            f32(NX, 16, 2048),
            f32(STATE, 128),
            f32(NY, STATE, 128),
            f32(TOK, STATE),
            f32(NY, TOK, STATE),
            f32(HEADS, TOK),
            f32(NY, HEADS, TOK),
            f32(NY, PAIRS, TOK, 128),
            f32(PAIRS, TOK, 128),
            pltpu.VMEM((TOK, 512), BF16),
            f32(HEADS, TOK),
            pltpu.VMEM((TOK, STATE), BF16),
            pltpu.VMEM((TOK, STATE), BF16),
            f32(HEADS, TOK),
            pltpu.VMEM((16, 2048), BF16),
            f32(PAIRS, 64, 128),
            pltpu.VMEM((TOK, 2048), BF16),
            pltpu.VMEM((2048, 512), BF16),
            pltpu.VMEM((TOK, STATE), BF16),
            pltpu.VMEM((TOK, STATE), BF16),
            f32(HEADS, TOK),
            f32(1, HEADS),
            pltpu.VMEM((512, TOK), BF16),
            pltpu.VMEM((TOK, 512), BF16),
            dma((2, 7, NY)),
            dma((2, 4, NZ)),
            dma((2, PAIRS, NY)),
            dma((2, 2, PAIRS, 4)),
            dma((2, 2)),
            dma((2, NX)),
            dma((7,)),
            dma((2, NX)),
            dma((8,)),
            dma((2, NY)),
        ],
        compiler_params=pltpu.CompilerParams(
            collective_id=0, has_side_effects=True, vmem_limit_bytes=VMEM_LIMIT
        ),
        name="mixer_backward",
    )(
        hidden,
        value_weight,
        key_vecs.reshape(TOK, STATE),
        queries.reshape(TOK, STATE),
        decay_pre.T,
        decay_rate[None, :],
        cotangent.reshape(TOK, 512).T,
    )
    gk, gq, gd, gh, gw = pl.pallas_call(
        store_all,
        out_shape=tuple(jax.ShapeDtypeStruct(o.shape, o.dtype) for o in outs),
        in_specs=[pl.BlockSpec(memory_space=pl.ANY)] * 5,
        out_specs=[pl.BlockSpec(memory_space=pl.ANY)] * 5,
        scratch_shapes=[*[pltpu.VMEM(o.shape, o.dtype) for o in outs], dma((2, 5))],
        compiler_params=pltpu.CompilerParams(vmem_limit_bytes=VMEM_LIMIT),
        name="store_all",
    )(*outs)
    return gk.reshape(TOK, 1, STATE), gq.reshape(TOK, 1, STATE), gd.T, gh, gw


def solution(mesh):
    split = Mesh(mesh.devices.reshape(NZ, NY, NX, 2), ("z", "y", "x", "c"))
    placed = (
        P(SP, None),
        P(None, TP),
        P(SP, TP, None),
        P(SP, TP, None),
        P(SP, TP),
        P(TP),
        P(SP, TP, None),
    )
    return jax.shard_map(
        local,
        mesh=split,
        in_specs=placed,
        out_specs=(P(SP, TP, None), P(SP, TP, None), P(SP, TP), P(SP + TP, None), P(SP, TP)),
        check_vma=False,
    )
```

```python
import contextlib

import jax
import jax.numpy as jnp
from jax import lax
from jax.experimental import pallas as pl
from jax.experimental.pallas import tpu as pltpu
from jax.sharding import Mesh
from jax.sharding import PartitionSpec as P

F32, BF16 = jnp.float32, jnp.bfloat16
MESH = pl.DeviceIdType.MESH
SP, TP = ("z", "y"), ("x", "c")
NZ, NY, NX = 8, 4, 4
TOK, STATE, PAIRS, HEADS = 128, 128, 4, 8
ROWS = STATE // NZ
VMEM_LIMIT = 48 * 1024 * 1024


def dot(a, b, dims=((1,), (0,))):
    return lax.dot_general(a, b, (dims, ((), ())), preferred_element_type=F32)


def halves(a):
    high = a.astype(BF16)
    return high, (a - high.astype(F32)).astype(BF16)


def dot_fine_right(a, b, dims=((1,), (0,))):
    high, low = halves(b)
    return dot(a, high, dims) + dot(a, low, dims)


def dot_fine_left(a, b, dims=((1,), (0,))):
    high, low = halves(a)
    return dot(high, b, dims) + dot(low, b, dims)


def dot_fine(a, b, dims=((1,), (0,))):
    a_high, a_low = halves(a)
    b_high, b_low = halves(b)
    return dot(a_high, b_high, dims) + dot(a_high, b_low, dims) + dot(a_low, b_high, dims)


def cols(pair):
    return slice(128 * pair, 128 * pair + 128)


def kernel(
    hid_at, w_at, k_at, q_at, pre_at, rate_at, cot_at,
    gk_out, gq_out, gd_out, gh_out, gw_out,
    ys_b, yr_b, ys_f, yr_f, zs_b, zr_b, zs_f, zr_f,
    zbs_b, zbr_b, zbs_f, zbr_f, ybs_b, ybr_b, ybs_f, ybr_f,
    hid_t, hid_p, hid_x, hid_c, hid_all, gv_s, gv_r, part, ring_s, ring_r,
    gh_s, gh_r, gx_s, gx_r, zg_s, zg_r, k_s, k_r, cum_s, cum_r, fade, gv_own, vals, row_sum,
    hid, w, k_in, q_in, pre, rate_in, cot_t, cot,
    y_sem, z_sem, ag_sem, ring_sem, d_sem, x_sem, in_sem, h_sem, zg_sem,
):
    z, y = lax.axis_index("z"), lax.axis_index("y")
    x, c = lax.axis_index("x"), lax.axis_index("c")
    lane = lax.broadcasted_iota(jnp.int32, (128, 128), 1)
    first_head = lane[0:1, :] < 64
    sent = []
    stack = contextlib.ExitStack()

    def phase(name):
        stack.close()
        stack.enter_context(jax.named_scope(name))

    def peer_y(o):
        return lax.rem(y + o, NY)

    def peer_z(o):
        return lax.rem(z + o, NZ)

    def peer_x(o):
        return lax.rem(x + o, NX)

    def copy(src, dst, s_sem, r_sem, **where):
        return pltpu.make_async_remote_copy(
            src_ref=src, dst_ref=dst, send_sem=s_sem, recv_sem=r_sem, device_id=where, device_id_type=MESH
        )

    def send(src, dst, s_sem, r_sem, **where):
        copy(src, dst, s_sem, r_sem, **where).start()

    def arrived(dst, r_sem):
        copy(dst, dst, r_sem, r_sem, c=1 - c).wait_recv()

    def drain_later(like, s_sem):
        sent.append(copy(like, like, s_sem, s_sem, c=1 - c))

    def send_y(kind, src, dst):
        for o in range(1, NY):
            send(src.at[peer_y(o)], dst.at[y], y_sem.at[0, kind], y_sem.at[1, kind], y=peer_y(o))
        drain_later(dst.at[0 : NY - 1], y_sem.at[0, kind])

    def share_y(kind, src, dst):
        for o in range(1, NY):
            send(src, dst.at[y], y_sem.at[0, kind], y_sem.at[1, kind], y=peer_y(o))
        drain_later(dst.at[0 : NY - 1], y_sem.at[0, kind])

    def wait_y(kind, dst):
        arrived(dst.at[0 : NY - 1], y_sem.at[1, kind])

    def send_z(kind, src, dst):
        for o in range(1, NZ):
            send(src.at[peer_z(o)], dst.at[z], z_sem.at[0, kind], z_sem.at[1, kind], z=peer_z(o))
        drain_later(dst.at[0 : NZ - 1], z_sem.at[0, kind])

    def wait_z(kind, dst):
        arrived(dst.at[0 : NZ - 1], z_sem.at[1, kind])

    phase("enter")
    loads = [
        pltpu.make_async_copy(src, dst, in_sem.at[i])
        for i, (src, dst) in enumerate(
            [(pre_at, pre), (rate_at, rate_in), (cot_at, cot_t), (q_at, q_in), (k_at, k_in), (hid_at, hid), (w_at, w)]
        )
    ]
    for made in loads:
        made.start()

    barrier = pltpu.get_barrier_semaphore()
    for o in range(1, NY):
        pl.semaphore_signal(barrier, inc=1, device_id={"y": peer_y(o)}, device_id_type=MESH)
    for o in range(1, NZ):
        pl.semaphore_signal(barrier, inc=1, device_id={"z": peer_z(o)}, device_id_type=MESH)
    for o in range(1, NX):
        pl.semaphore_signal(barrier, inc=1, device_id={"x": peer_x(o)}, device_id_type=MESH)
    pl.semaphore_signal(barrier, inc=1, device_id={"c": 1 - c}, device_id_type=MESH)

    phase("decay")
    loads[0].wait()
    loads[1].wait()
    pre_v = pre[...]
    square = lax.broadcasted_iota(jnp.int32, (8, 8), 0) == lax.broadcasted_iota(jnp.int32, (8, 8), 1)
    rate = jnp.sum(jnp.where(square, jnp.broadcast_to(rate_in[...], (8, 8)), 0.0), axis=1, keepdims=True)
    soft = jnp.maximum(pre_v, 0.0) + jnp.log1p(jnp.exp(-jnp.abs(pre_v)))
    cum = -rate * soft
    lane8 = lane[0:8, :]
    for shift in (1, 2, 4, 8, 16, 32, 64):
        cum = cum + jnp.where(lane8 >= shift, pltpu.roll(cum, shift, 1), 0.0)
    cum_s[...] = cum
    cum_r[y] = cum
    total = jnp.broadcast_to(cum[:, 127:128], (8, 128))
    factor = jnp.exp(total)
    cum_t = cum.T
    from_start = jnp.exp(cum)
    from_start_t = from_start.T
    to_end_t = jnp.exp(total - cum).T

    def spread(columns, pair):
        return jnp.where(first_head, columns[:, 2 * pair : 2 * pair + 1], columns[:, 2 * pair + 1 : 2 * pair + 2])

    def row_of(gains, pair):
        return jnp.where(first_head, gains[2 * pair : 2 * pair + 1, :], gains[2 * pair + 1 : 2 * pair + 2, :])

    phase("pull")
    loads[2].wait()
    loads[3].wait()
    q = q_in[...]
    q_t = q.astype(F32).T.astype(BF16)
    upper = lax.broadcasted_iota(jnp.int32, (128, 128), 0) < 64
    for pair in range(PAIRS):
        growth = jnp.where(upper, from_start[2 * pair : 2 * pair + 1, :], from_start[2 * pair + 1 : 2 * pair + 2, :])
        scaled = growth * cot_t[cols(pair), :].astype(F32)
        ys_b[pair, 0:128, :] = dot_fine_right(q_t, scaled, ((1,), (1,)))
        ys_b[pair, 128:136, :] = jnp.broadcast_to(row_of(factor, pair), (8, 128))
    yr_b[y] = ys_b[y]
    loads[4].wait()
    k = k_in[...]
    k_s[...] = k.astype(F32)
    k_r[y] = k_s[...]

    phase("barrier")
    pl.semaphore_wait(barrier, NY + NZ + NX - 2)
    send_y(0, ys_b, yr_b)

    phase("hidden")
    loads[5].wait()
    for block in range(16):
        turned = hid[:, cols(block)].astype(F32).T
        hid_t[block // 2, 2 * (block % 2) : 2 * (block % 2) + 2] = turned.reshape(2, 64, 128)
    seat = 2 * x + c
    for o in range(1, NY):
        send(hid_t.at[seat, peer_y(o)], hid_p.at[y], y_sem.at[0, 2], y_sem.at[1, 2], y=peer_y(o))
    drain_later(hid_p.at[0 : NY - 1], y_sem.at[0, 2])
    hid_p[y] = hid_t[seat, y]
    share_y(5, k_s, k_r)
    share_y(6, cum_s, cum_r)

    phase("values")
    loads[6].wait()
    k_t = k_s[...].T.astype(BF16)
    for half in range(2):
        span = slice(256 * half, 256 * half + 256)
        vals[:, span] = dot(hid[...], w[:, span]).astype(BF16)
    for pair in range(PAIRS):
        scaled = spread(to_end_t, pair) * vals[:, cols(pair)].astype(F32)
        ys_f[pair, 0:128, :] = dot_fine_right(k_t, scaled)
        ys_f[pair, 128:136, :] = jnp.broadcast_to(row_of(factor, pair), (8, 128))
    yr_f[y] = ys_f[y]

    phase("block")
    for pair in range(PAIRS):
        cot[:, cols(pair)] = cot_t[cols(pair), :].astype(F32).T.astype(BF16)
    score = dot(k, q, ((1,), (1,)))
    causal = lax.broadcasted_iota(jnp.int32, (128, 128), 0) <= lane
    blend = jnp.zeros((128, 128), F32)
    for pair in range(PAIRS):
        cot_pair, val_pair = cot[:, cols(pair)], vals[:, cols(pair)]
        inner = jnp.zeros((128, 128), F32)
        for side in range(2):
            head = 2 * pair + side
            mine = first_head if side == 0 else jnp.logical_not(first_head)
            across = jnp.where(causal, cum[head : head + 1, :] - cum_t[:, head : head + 1], 0.0)
            damping = jnp.where(causal, jnp.exp(across), 0.0)
            weight = score * damping
            cot_head = jnp.where(mine, cot_pair.astype(F32), 0.0).astype(BF16)
            inner = inner + dot_fine_left(weight, cot_head)
            moved = dot(val_pair, cot_head, ((1,), (1,)))
            blend = blend + moved * damping
            row_sum[head : head + 1, :] = jnp.sum(moved * weight, axis=0, keepdims=True)
        gv_s[pair] = inner

    def scan_plane(got, kept, z_send, reverse):
        state, gain = None, None
        order = range(NY - 1, -1, -1) if reverse else range(NY)
        for block in order:
            value, here = got[block, 0:128, :], got[block, 128:129, :]
            if state is None:
                kept[block] = jnp.zeros((128, 128), F32)
                state, gain = value, here
            else:
                kept[block] = state
                state, gain = here * state + value, gain * here
        for row in range(NZ):
            z_send[row, 0:ROWS, :] = state[row * ROWS : row * ROWS + ROWS, :]
            z_send[row, ROWS : ROWS + 8, :] = jnp.broadcast_to(gain, (8, 128))

    def scan_z(got, back, reverse):
        state = None
        for plane in range(NZ - 1, -1, -1) if reverse else range(NZ):
            value, here = got[plane, 0:ROWS, :], got[plane, ROWS : ROWS + 1, :]
            if state is None:
                back[plane] = jnp.zeros((ROWS, 128), F32)
                state = value
            else:
                back[plane] = state
                state = here * state + value

    def finish_plane(got, kept, plane_in, reverse):
        incoming = plane_in[...].reshape(STATE, 128)
        gain = None
        for block in range(NY - 1, -1, -1) if reverse else range(NY):
            kept[block] = kept[block] + (incoming if gain is None else gain * incoming)
            here = got[block, 128:129, :]
            gain = here if gain is None else gain * here

    phase("scan_y_b")
    wait_y(0, yr_b)
    scan_plane(yr_b, ybs_b, zs_b, True)
    zr_b[z] = zs_b[z]
    send_z(0, zs_b, zr_b)
    ybr_b[y] = ybs_b[y]
    send_y(3, ybs_b, ybr_b)
    send_y(1, ys_f, yr_f)

    phase("hidden_x")
    wait_y(2, hid_p)
    for o in range(1, NX):
        send(hid_p, hid_x.at[x], h_sem.at[0], h_sem.at[1], x=peer_x(o))
    drain_later(hid_x.at[0 : NX - 1], h_sem.at[0])
    hid_x[x] = hid_p[...]

    phase("scan_z_b")
    wait_z(0, zr_b)
    scan_z(zr_b, zbs_b, True)
    zbr_b[z] = zbs_b[z]
    send_z(2, zbs_b, zbr_b)

    phase("wait_suffix")
    wait_y(3, ybr_b)
    phase("gv_plane")
    for pair in range(PAIRS):
        gv_s[pair] = gv_s[pair] + spread(to_end_t, pair) * dot_fine_right(k, ybr_b[pair])

    def share_slot(slot):
        for o in range(1, NY):
            send(gv_s.at[peer_y(o + slot)], gv_r.at[slot, y], ag_sem.at[0, slot], ag_sem.at[1, slot], y=peer_y(o))
        drain_later(gv_r.at[slot, 0 : NY - 1], ag_sem.at[0, slot])
        gv_r[slot, y] = gv_s[peer_y(slot)]

    share_slot(0)
    share_slot(1)

    phase("fade")
    wait_y(5, k_r)
    wait_y(6, cum_r)
    tail = jnp.zeros((8, 1), F32)
    tail_own = jnp.zeros((8, 1), F32)
    for block in range(NY - 1, -1, -1):
        here = cum_r[block]
        tail_own = jnp.where(y == block, tail, tail_own)
        tail = tail + here[:, 127:128]
        fade_t = jnp.exp(tail - here).T
        for pair in range(PAIRS):
            fade[block, pair] = spread(fade_t, pair)
    gain_own = jnp.exp(jnp.broadcast_to(tail_own, (8, 128)))
    k_all = k_r[...].reshape(512, 128).astype(BF16)

    phase("hidden_c")
    arrived(hid_x.at[0 : NX - 1], h_sem.at[1])
    send(hid_x, hid_c, d_sem.at[0, 1], d_sem.at[1, 1], c=1 - c)
    drain_later(hid_x, d_sem.at[0, 1])

    phase("wait_zg")
    wait_z(2, zbr_b)
    zg_s[...] = zbr_b[...].reshape(STATE, 128)
    zg_r[0] = zg_s[...]
    for o in range(1, NY):
        send(zg_s, zg_r.at[NY - o], zg_sem.at[0], zg_sem.at[1], y=peer_y(o))
    drain_later(zg_r.at[0 : NY - 1], zg_sem.at[0])
    share_slot(2)
    share_slot(3)

    phase("scan_y_f")
    wait_y(1, yr_f)
    scan_plane(yr_f, ybs_f, zs_f, False)
    zr_f[z] = zs_f[z]
    send_z(1, zs_f, zr_f)

    phase("hid_all")
    arrived(hid_c, d_sem.at[1, 1])
    for across_x in range(NX):
        for block in range(NY):
            hid_all[across_x, c, :, cols(block)] = hid_x[across_x, block].astype(BF16)
            hid_all[across_x, 1 - c, :, cols(block)] = hid_c[across_x, block].astype(BF16)

    def steps(slot, way):
        return 4 if (slot + way) % 2 == 0 else 3

    def ring_target(slot, way, step):
        n = steps(slot, way)
        return peer_z(n - step) if way == 0 else peer_z(NZ - n + step)

    def ring_send(src, slot, way, step):
        send(
            src, ring_r.at[way, slot, step], ring_sem.at[PAIRS, 0], ring_sem.at[slot, step],
            z=peer_z(1) if way == 0 else peer_z(NZ - 1),
        )

    def ring(slot, step):
        phase(f"ring{slot}_{step}")
        count = sum(step <= steps(slot, way) for way in range(2))
        arrived(ring_r.at[0:count, slot, step - 1], ring_sem.at[slot, step - 1])
        for way in range(2):
            if step < steps(slot, way):
                ring_s[way, slot, step] = ring_r[way, slot, step - 1] + part[slot, ring_target(slot, way, step)]
                ring_send(ring_s.at[way, slot, step], slot, way, step)
        if step == 4:
            last = [steps(slot, way) - 1 for way in range(2)]
            gw_out[slot] = part[slot, z] + ring_r[0, slot, last[0]] + ring_r[1, slot, last[1]]

    def weight(slot):
        phase(f"wait_ag{slot}")
        pair = peer_y(slot)
        arrived(gv_r.at[slot, 0 : NY - 1], ag_sem.at[1, slot])
        phase(f"weight{slot}")
        fresh = dot_fine_right(k_all, zg_r[slot])
        for block in range(NY):
            gv_r[slot, block] = gv_r[slot, block] + fade[block, pair] * fresh[128 * block : 128 * block + 128, :]
        gathered = gv_r[slot].reshape(512, 128).astype(BF16)
        part[slot] = dot(hid_all[...].reshape(512, 512), gathered).reshape(NZ, 64, 128)
        for way in range(2):
            ring_send(part.at[slot, ring_target(slot, way, 0)], slot, way, 0)

    weight(0)

    phase("scan_z_f")
    wait_z(1, zr_f)
    scan_z(zr_f, zbs_f, False)
    zbr_f[z] = zbs_f[z]
    send_z(3, zbs_f, zbr_f)
    ring(0, 1)

    phase("wait_zg_all")
    arrived(zg_r.at[0 : NY - 1], zg_sem.at[1])
    phase("grad_h")
    for slot in range(PAIRS):
        pair = peer_y(slot)
        gv_own[pair] = gv_s[pair] + fade[y, pair] * dot_fine_right(k, zg_r[slot])
    grad_v = jnp.concatenate([gv_own[pair].astype(BF16) for pair in range(PAIRS)], axis=1)
    for part_now in range(4):
        span = slice(512 * part_now, 512 * part_now + 512)
        gh_s[:, :, :, span] = dot(grad_v, w[span, :], ((1,), (1,))).reshape(NX, 2, 16, 512)
    send(gh_s.at[:, 1 - c], gh_r, d_sem.at[0, 0], d_sem.at[1, 0], c=1 - c)
    drain_later(gh_r, d_sem.at[0, 0])

    weight(1)
    ring(0, 2)
    weight(2)

    phase("chip_pair")
    arrived(gh_r, d_sem.at[1, 0])
    gx_s[...] = gh_s[:, c] + gh_r[...]
    for o in range(1, NX):
        send(gx_s.at[peer_x(o)], gx_r.at[x], x_sem.at[0], x_sem.at[1], x=peer_x(o))
    drain_later(gx_r.at[0 : NX - 1], x_sem.at[0])
    gx_r[x] = gx_s[x]

    weight(3)

    phase("back_y_f")
    wait_z(3, zbr_f)
    finish_plane(yr_f, ybs_f, zbr_f, False)
    ybr_f[y] = ybs_f[y]
    send_y(4, ybs_f, ybr_f)

    ring(1, 1)
    ring(0, 3)
    ring(2, 1)

    phase("grad_k")
    gk = dot_fine_left(blend, q)
    gq = dot_fine_left(blend.T, k)
    gap = row_sum[...]
    shared = jnp.zeros((8, 128), F32)
    head_row = lax.broadcasted_iota(jnp.int32, (8, 128), 0)
    choosers = [jnp.where(head_row == 2 * pair + (lane8 >= 64).astype(jnp.int32), 1.0, 0.0) for pair in range(PAIRS)]

    def gathered_rows(chooser, change):
        return lax.dot_general(
            chooser, change, (((1,), (1,)), ((), ())), precision=lax.Precision.HIGHEST, preferred_element_type=F32
        )

    for pair in range(PAIRS):
        pull = ybr_b[pair] + row_of(gain_own, pair) * zg_r[lax.rem(pair + NY - y, NY)]
        ybr_b[pair] = pull
        val_f = vals[:, cols(pair)].astype(F32)
        val_scaled = spread(to_end_t, pair) * val_f
        gk = gk + dot_fine(val_scaled, pull, ((1,), (1,)))
        whole = jnp.sum(val_scaled * dot_fine_right(k, pull), axis=0, keepdims=True)
        shared = shared + jnp.sum(choosers[pair] * whole, axis=1, keepdims=True)
        gv_own[pair] = val_f * gv_own[pair]
    gk_out[...] = gk.astype(BF16)

    ring(1, 2)
    ring(3, 1)
    ring(0, 4)
    ring(2, 2)

    phase("wait_carry")
    wait_y(4, ybr_f)
    phase("grad_q")
    for pair in range(PAIRS):
        carry = ybr_f[pair]
        cot_scaled = spread(from_start_t, pair) * cot[:, cols(pair)].astype(F32)
        gq = gq + dot_fine(cot_scaled, carry, ((1,), (1,)))
        change = cot_scaled * dot_fine_right(q, carry) - gv_own[pair]
        gap = gap + gathered_rows(choosers[pair], change)
        whole = row_of(factor, pair) * jnp.sum(carry * ybr_b[pair], axis=0, keepdims=True)
        shared = shared + jnp.sum(choosers[pair] * whole, axis=1, keepdims=True)
    for shift in (1, 2, 4, 8, 16, 32, 64):
        gap = gap + jnp.where(lane8 < 128 - shift, pltpu.roll(gap, 128 - shift, 1), 0.0)
    gd_out[...] = (gap + shared) * (-rate / (1.0 + jnp.exp(-pre_v)))
    gq_out[...] = gq.astype(BF16)

    ring(1, 3)
    ring(3, 2)
    ring(2, 3)
    ring(1, 4)
    ring(3, 3)

    phase("out_h")
    arrived(gx_r.at[0 : NX - 1], x_sem.at[1])
    gh_out[...] = (gx_r[0] + gx_r[1] + gx_r[2] + gx_r[3]).astype(BF16)

    ring(2, 4)
    ring(3, 4)
    drain_later(part.at[0:PAIRS, 0 : NZ - 1], ring_sem.at[PAIRS, 0])

    phase("drain")
    for made in sent:
        made.wait_send()
    stack.close()


def store_all(*refs):
    y = lax.axis_index("y")
    sems = refs[10]
    copies = [pltpu.make_async_copy(refs[i], refs[5 + i], sems.at[i]) for i in range(4)]
    for slot in range(PAIRS):
        pair = lax.rem(y + slot, PAIRS)
        place = refs[9].at[:, pl.ds(pl.multiple_of(128 * pair, 128), 128)]
        copies.append(pltpu.make_async_copy(refs[4].at[slot], place, sems.at[4 + slot]))
    for made in copies:
        made.start()
    for made in copies:
        made.wait()


def local(hidden, value_weight, key_vecs, queries, decay_pre, decay_rate, cotangent):
    dma = pltpu.SemaphoreType.DMA
    f32 = lambda *shape: pltpu.VMEM(shape, F32)
    y_box, z_box = (NY, STATE + 8, 128), (NZ, ROWS + 8, 128)
    z_back, y_back = (NZ, ROWS, 128), (NY, STATE, 128)
    outs = pl.pallas_call(
        kernel,
        out_shape=(
            jax.ShapeDtypeStruct((TOK, STATE), BF16),
            jax.ShapeDtypeStruct((TOK, STATE), BF16),
            jax.ShapeDtypeStruct((HEADS, TOK), F32),
            jax.ShapeDtypeStruct((16, 2048), BF16),
            jax.ShapeDtypeStruct((PAIRS, 64, 128), F32),
        ),
        in_specs=[pl.BlockSpec(memory_space=pltpu.HBM)] * 7,
        out_specs=[pl.BlockSpec(memory_space=pltpu.VMEM)] * 5,
        scratch_shapes=[
            *[f32(*y_box)] * 4,
            *[f32(*z_box)] * 4,
            *[f32(*z_back)] * 4,
            *[f32(*y_back)] * 4,
            f32(NZ, NY, 64, TOK),
            f32(NY, 64, TOK),
            f32(NX, NY, 64, TOK),
            f32(NX, NY, 64, TOK),
            pltpu.VMEM((NX, 2, 64, 512), BF16),
            f32(PAIRS, TOK, 128),
            f32(PAIRS, NY, TOK, 128),
            f32(PAIRS, NZ, 64, 128),
            f32(2, PAIRS, 4, 64, 128),
            f32(2, PAIRS, 4, 64, 128),
            f32(NX, 2, 16, 2048),
            f32(NX, 16, 2048),
            f32(NX, 16, 2048),
            f32(NX, 16, 2048),
            f32(STATE, 128),
            f32(NY, STATE, 128),
            f32(TOK, STATE),
            f32(NY, TOK, STATE),
            f32(HEADS, TOK),
            f32(NY, HEADS, TOK),
            f32(NY, PAIRS, TOK, 128),
            f32(PAIRS, TOK, 128),
            pltpu.VMEM((TOK, 512), BF16),
            f32(HEADS, TOK),
            pltpu.VMEM((TOK, 2048), BF16),
            pltpu.VMEM((2048, 512), BF16),
            pltpu.VMEM((TOK, STATE), BF16),
            pltpu.VMEM((TOK, STATE), BF16),
            f32(HEADS, TOK),
            f32(1, HEADS),
            pltpu.VMEM((512, TOK), BF16),
            pltpu.VMEM((TOK, 512), BF16),
            dma((2, 7)),
            dma((2, 4)),
            dma((2, PAIRS)),
            dma((PAIRS + 1, 4)),
            dma((2, 2)),
            dma((2,)),
            dma((7,)),
            dma((2,)),
            dma((2,)),
        ],
        compiler_params=pltpu.CompilerParams(
            collective_id=0, has_side_effects=True, vmem_limit_bytes=VMEM_LIMIT
        ),
        name="mixer_backward",
    )(
        *[
            pltpu.with_memory_space_constraint(a, pltpu.HBM)
            for a in (
                hidden,
                value_weight,
                key_vecs.reshape(TOK, STATE),
                queries.reshape(TOK, STATE),
                decay_pre.T,
                decay_rate[None, :],
                cotangent.reshape(TOK, 512).T,
            )
        ]
    )
    gk, gq, gd, gh, gw = pl.pallas_call(
        store_all,
        out_shape=(
            *[jax.ShapeDtypeStruct(o.shape, o.dtype) for o in outs[:4]],
            jax.ShapeDtypeStruct((64, 512), F32),
        ),
        in_specs=[pl.BlockSpec(memory_space=pltpu.VMEM)] * 5,
        out_specs=[pl.BlockSpec(memory_space=pltpu.HBM)] * 5,
        scratch_shapes=[dma((8,))],
        compiler_params=pltpu.CompilerParams(vmem_limit_bytes=2 * 1024 * 1024),
        name="store_all",
    )(*outs)
    return gk.reshape(TOK, 1, STATE), gq.reshape(TOK, 1, STATE), gd.T, gh, gw


def solution(mesh):
    split = Mesh(mesh.devices.reshape(NZ, NY, NX, 2), ("z", "y", "x", "c"))
    placed = (
        P(SP, None),
        P(None, TP),
        P(SP, TP, None),
        P(SP, TP, None),
        P(SP, TP),
        P(TP),
        P(SP, TP, None),
    )
    return jax.shard_map(
        local,
        mesh=split,
        in_specs=placed,
        out_specs=(P(SP, TP, None), P(SP, TP, None), P(SP, TP), P(SP + TP, None), P(SP, TP)),
        check_vma=False,
    )
```

```python
import contextlib

import jax
import jax.numpy as jnp
from jax import lax
from jax.experimental import pallas as pl
from jax.experimental.pallas import tpu as pltpu
from jax.sharding import Mesh
from jax.sharding import PartitionSpec as P

F32, BF16 = jnp.float32, jnp.bfloat16
MESH = pl.DeviceIdType.MESH
SP, TP = ("z", "y"), ("x", "c")
NZ, NY, NX = 8, 4, 4
TOK, STATE, PAIRS, HEADS = 128, 128, 4, 8
ROWS = STATE // NZ
VMEM_LIMIT = 48 * 1024 * 1024


def dot(a, b, dims=((1,), (0,))):
    return lax.dot_general(a, b, (dims, ((), ())), preferred_element_type=F32)


def halves(a):
    high = a.astype(BF16)
    return high, (a - high.astype(F32)).astype(BF16)


def dot_fine_right(a, b, dims=((1,), (0,))):
    high, low = halves(b)
    return dot(a, high, dims) + dot(a, low, dims)


def dot_fine_left(a, b, dims=((1,), (0,))):
    high, low = halves(a)
    return dot(high, b, dims) + dot(low, b, dims)


def dot_fine(a, b, dims=((1,), (0,))):
    a_high, a_low = halves(a)
    b_high, b_low = halves(b)
    return dot(a_high, b_high, dims) + dot(a_high, b_low, dims) + dot(a_low, b_high, dims)


def cols(pair):
    return slice(128 * pair, 128 * pair + 128)


def kernel(
    hid_at, w_at, k_at, q_at, pre_at, rate_at, cot_at,
    gk_out, gq_out, gd_out, gh_out, gw_out,
    ys_b, yr_b, ys_f, yr_f, zs_b, zr_b, zs_f, zr_f,
    zbs_b, zbr_b, zbs_f, zbr_f, ybs_b, ybr_b, ybs_f, ybr_f,
    hid_t, hid_p, hid_x, hid_c, hid_all, gv_s, gv_r, part, near_r, far_r, ring_s, ring_r,
    gh_s, gh_r, gx_s, gx_r, zg_s, zg_r, k_s, k_r, cum_s, cum_r, fade, gv_own, vals, row_sum,
    hid, w, k_in, q_in, pre, rate_in, cot_t, cot,
    y_sem, z_sem, ag_sem, ring_sem, d_sem, x_sem, in_sem, h_sem, zg_sem,
):
    z, y = lax.axis_index("z"), lax.axis_index("y")
    x, c = lax.axis_index("x"), lax.axis_index("c")
    lane = lax.broadcasted_iota(jnp.int32, (128, 128), 1)
    first_head = lane[0:1, :] < 64
    sent = []
    stack = contextlib.ExitStack()

    def phase(name):
        stack.close()
        stack.enter_context(jax.named_scope(name))

    def peer_y(o):
        return lax.rem(y + o, NY)

    def peer_z(o):
        return lax.rem(z + o, NZ)

    def peer_x(o):
        return lax.rem(x + o, NX)

    def copy(src, dst, s_sem, r_sem, **where):
        return pltpu.make_async_remote_copy(
            src_ref=src, dst_ref=dst, send_sem=s_sem, recv_sem=r_sem, device_id=where, device_id_type=MESH
        )

    def send(src, dst, s_sem, r_sem, **where):
        copy(src, dst, s_sem, r_sem, **where).start()

    def arrived(dst, r_sem):
        copy(dst, dst, r_sem, r_sem, c=1 - c).wait_recv()

    def drain_later(like, s_sem):
        sent.append(copy(like, like, s_sem, s_sem, c=1 - c))

    def send_y(kind, src, dst):
        for o in range(1, NY):
            send(src.at[peer_y(o)], dst.at[y], y_sem.at[0, kind], y_sem.at[1, kind], y=peer_y(o))
        drain_later(dst.at[0 : NY - 1], y_sem.at[0, kind])

    def share_y(kind, src, dst):
        for o in range(1, NY):
            send(src, dst.at[y], y_sem.at[0, kind], y_sem.at[1, kind], y=peer_y(o))
        drain_later(dst.at[0 : NY - 1], y_sem.at[0, kind])

    def wait_y(kind, dst):
        arrived(dst.at[0 : NY - 1], y_sem.at[1, kind])

    def send_z(kind, src, dst):
        for o in range(1, NZ):
            send(src.at[peer_z(o)], dst.at[z], z_sem.at[0, kind], z_sem.at[1, kind], z=peer_z(o))
        drain_later(dst.at[0 : NZ - 1], z_sem.at[0, kind])

    def wait_z(kind, dst):
        arrived(dst.at[0 : NZ - 1], z_sem.at[1, kind])

    phase("enter")
    loads = [
        pltpu.make_async_copy(src, dst, in_sem.at[i])
        for i, (src, dst) in enumerate(
            [(pre_at, pre), (rate_at, rate_in), (cot_at, cot_t), (q_at, q_in), (k_at, k_in), (hid_at, hid), (w_at, w)]
        )
    ]
    for made in loads:
        made.start()

    barrier = pltpu.get_barrier_semaphore()
    for o in range(1, NY):
        pl.semaphore_signal(barrier, inc=1, device_id={"y": peer_y(o)}, device_id_type=MESH)
    for o in range(1, NZ):
        pl.semaphore_signal(barrier, inc=1, device_id={"z": peer_z(o)}, device_id_type=MESH)
    for o in range(1, NX):
        pl.semaphore_signal(barrier, inc=1, device_id={"x": peer_x(o)}, device_id_type=MESH)
    pl.semaphore_signal(barrier, inc=1, device_id={"c": 1 - c}, device_id_type=MESH)

    phase("decay")
    loads[0].wait()
    loads[1].wait()
    pre_v = pre[...]
    square = lax.broadcasted_iota(jnp.int32, (8, 8), 0) == lax.broadcasted_iota(jnp.int32, (8, 8), 1)
    rate = jnp.sum(jnp.where(square, jnp.broadcast_to(rate_in[...], (8, 8)), 0.0), axis=1, keepdims=True)
    soft = jnp.maximum(pre_v, 0.0) + jnp.log1p(jnp.exp(-jnp.abs(pre_v)))
    cum = -rate * soft
    lane8 = lane[0:8, :]
    for shift in (1, 2, 4, 8, 16, 32, 64):
        cum = cum + jnp.where(lane8 >= shift, pltpu.roll(cum, shift, 1), 0.0)
    cum_s[...] = cum
    cum_r[y] = cum
    total = jnp.broadcast_to(cum[:, 127:128], (8, 128))
    factor = jnp.exp(total)
    cum_t = cum.T
    from_start = jnp.exp(cum)
    from_start_t = from_start.T
    to_end_t = jnp.exp(total - cum).T

    def spread(columns, pair):
        return jnp.where(first_head, columns[:, 2 * pair : 2 * pair + 1], columns[:, 2 * pair + 1 : 2 * pair + 2])

    def row_of(gains, pair):
        return jnp.where(first_head, gains[2 * pair : 2 * pair + 1, :], gains[2 * pair + 1 : 2 * pair + 2, :])

    phase("pull")
    loads[2].wait()
    loads[3].wait()
    q = q_in[...]
    q_t = q.astype(F32).T.astype(BF16)
    growth = jnp.concatenate(
        [jnp.broadcast_to(from_start[head : head + 1, :], (64, 128)) for head in range(HEADS)], axis=0
    )
    pulls = dot_fine_right(q_t, growth * cot_t[...].astype(F32), ((1,), (1,)))
    for pair in range(PAIRS):
        ys_b[pair, 0:128, :] = pulls[:, cols(pair)]
        ys_b[pair, 128:136, :] = jnp.broadcast_to(row_of(factor, pair), (8, 128))
    yr_b[y] = ys_b[y]
    loads[4].wait()
    k = k_in[...]
    k_s[...] = k.astype(F32)
    k_r[y] = k_s[...]

    phase("barrier")
    pl.semaphore_wait(barrier, NY + NZ + NX - 2)
    send_y(0, ys_b, yr_b)

    phase("hidden")
    loads[5].wait()
    for block in range(16):
        turned = hid[:, cols(block)].astype(F32).T
        hid_t[block // 2, 2 * (block % 2) : 2 * (block % 2) + 2] = turned.reshape(2, 64, 128)
    seat = 2 * x + c
    for o in range(1, NY):
        send(hid_t.at[seat, peer_y(o)], hid_p.at[y], y_sem.at[0, 2], y_sem.at[1, 2], y=peer_y(o))
    drain_later(hid_p.at[0 : NY - 1], y_sem.at[0, 2])
    hid_p[y] = hid_t[seat, y]
    share_y(5, k_s, k_r)
    share_y(6, cum_s, cum_r)

    phase("values")
    loads[6].wait()
    k_t = k_s[...].T.astype(BF16)
    for half in range(2):
        span = slice(256 * half, 256 * half + 256)
        vals[:, span] = dot(hid[...], w[:, span]).astype(BF16)
    scaled = jnp.concatenate([spread(to_end_t, pair) for pair in range(PAIRS)], axis=1) * vals[...].astype(F32)
    states = dot_fine_right(k_t, scaled)
    for pair in range(PAIRS):
        ys_f[pair, 0:128, :] = states[:, cols(pair)]
        ys_f[pair, 128:136, :] = jnp.broadcast_to(row_of(factor, pair), (8, 128))
    yr_f[y] = ys_f[y]

    phase("block")
    for pair in range(PAIRS):
        cot[:, cols(pair)] = cot_t[cols(pair), :].astype(F32).T.astype(BF16)
    score = dot(k, q, ((1,), (1,)))
    causal = lax.broadcasted_iota(jnp.int32, (128, 128), 0) <= lane
    blend = jnp.zeros((128, 128), F32)
    for pair in range(PAIRS):
        cot_pair, val_pair = cot[:, cols(pair)], vals[:, cols(pair)]
        inner = jnp.zeros((128, 128), F32)
        for side in range(2):
            head = 2 * pair + side
            mine = first_head if side == 0 else jnp.logical_not(first_head)
            across = jnp.where(causal, cum[head : head + 1, :] - cum_t[:, head : head + 1], 0.0)
            damping = jnp.where(causal, jnp.exp(across), 0.0)
            weight = score * damping
            cot_head = jnp.where(mine, cot_pair.astype(F32), 0.0).astype(BF16)
            inner = inner + dot_fine_left(weight, cot_head)
            moved = dot(val_pair, cot_head, ((1,), (1,)))
            blend = blend + moved * damping
            row_sum[head : head + 1, :] = jnp.sum(moved * weight, axis=0, keepdims=True)
        gv_s[pair] = inner

    def scan_plane(got, kept, z_send, reverse):
        state, gain = None, None
        order = range(NY - 1, -1, -1) if reverse else range(NY)
        for block in order:
            value, here = got[block, 0:128, :], got[block, 128:129, :]
            if state is None:
                kept[block] = jnp.zeros((128, 128), F32)
                state, gain = value, here
            else:
                kept[block] = state
                state, gain = here * state + value, gain * here
        for row in range(NZ):
            z_send[row, 0:ROWS, :] = state[row * ROWS : row * ROWS + ROWS, :]
            z_send[row, ROWS : ROWS + 8, :] = jnp.broadcast_to(gain, (8, 128))

    def scan_z(got, back, reverse):
        state = None
        for plane in range(NZ - 1, -1, -1) if reverse else range(NZ):
            value, here = got[plane, 0:ROWS, :], got[plane, ROWS : ROWS + 1, :]
            if state is None:
                back[plane] = jnp.zeros((ROWS, 128), F32)
                state = value
            else:
                back[plane] = state
                state = here * state + value

    def finish_plane(got, kept, plane_in, reverse):
        incoming = plane_in[...].reshape(STATE, 128)
        gain = None
        for block in range(NY - 1, -1, -1) if reverse else range(NY):
            kept[block] = kept[block] + (incoming if gain is None else gain * incoming)
            here = got[block, 128:129, :]
            gain = here if gain is None else gain * here

    phase("scan_y_b")
    wait_y(0, yr_b)
    scan_plane(yr_b, ybs_b, zs_b, True)
    zr_b[z] = zs_b[z]
    send_z(0, zs_b, zr_b)
    ybr_b[y] = ybs_b[y]
    send_y(3, ybs_b, ybr_b)
    send_y(1, ys_f, yr_f)

    phase("hidden_x")
    wait_y(2, hid_p)
    for o in range(1, NX):
        send(hid_p, hid_x.at[x], h_sem.at[0], h_sem.at[1], x=peer_x(o))
    drain_later(hid_x.at[0 : NX - 1], h_sem.at[0])
    hid_x[x] = hid_p[...]

    phase("scan_z_b")
    wait_z(0, zr_b)
    scan_z(zr_b, zbs_b, True)
    zbr_b[z] = zbs_b[z]
    send_z(2, zbs_b, zbr_b)

    phase("wait_suffix")
    wait_y(3, ybr_b)
    phase("gv_plane")
    for pair in range(PAIRS):
        gv_s[pair] = gv_s[pair] + spread(to_end_t, pair) * dot_fine_right(k, ybr_b[pair])

    def share_slot(slot):
        for o in range(1, NY):
            send(gv_s.at[peer_y(o + slot)], gv_r.at[slot, y], ag_sem.at[0, slot], ag_sem.at[1, slot], y=peer_y(o))
        drain_later(gv_r.at[slot, 0 : NY - 1], ag_sem.at[0, slot])
        gv_r[slot, y] = gv_s[peer_y(slot)]

    share_slot(0)
    share_slot(1)

    phase("fade")
    wait_y(5, k_r)
    wait_y(6, cum_r)
    tail = jnp.zeros((8, 1), F32)
    tail_own = jnp.zeros((8, 1), F32)
    for block in range(NY - 1, -1, -1):
        here = cum_r[block]
        tail_own = jnp.where(y == block, tail, tail_own)
        tail = tail + here[:, 127:128]
        fade_t = jnp.exp(tail - here).T
        for pair in range(PAIRS):
            fade[block, pair] = spread(fade_t, pair)
    gain_own = jnp.exp(jnp.broadcast_to(tail_own, (8, 128)))
    k_all = k_r[...].reshape(512, 128).astype(BF16)

    phase("hidden_c")
    arrived(hid_x.at[0 : NX - 1], h_sem.at[1])
    send(hid_x, hid_c, d_sem.at[0, 1], d_sem.at[1, 1], c=1 - c)
    drain_later(hid_x, d_sem.at[0, 1])

    phase("wait_zg")
    wait_z(2, zbr_b)
    zg_s[...] = zbr_b[...].reshape(STATE, 128)
    zg_r[0] = zg_s[...]
    for o in range(1, NY):
        send(zg_s, zg_r.at[NY - o], zg_sem.at[0], zg_sem.at[1], y=peer_y(o))
    drain_later(zg_r.at[0 : NY - 1], zg_sem.at[0])
    share_slot(2)
    share_slot(3)

    phase("scan_y_f")
    wait_y(1, yr_f)
    scan_plane(yr_f, ybs_f, zs_f, False)
    zr_f[z] = zs_f[z]
    send_z(1, zs_f, zr_f)

    phase("hid_all")
    arrived(hid_c, d_sem.at[1, 1])
    for across_x in range(NX):
        for block in range(NY):
            hid_all[across_x, c, :, cols(block)] = hid_x[across_x, block].astype(BF16)
            hid_all[across_x, 1 - c, :, cols(block)] = hid_c[across_x, block].astype(BF16)

    spans = (slice(0, 32), slice(32, 64))

    def ahead(way, o):
        return peer_z(o) if way == 0 else peer_z(NZ - o)

    def z_first(slot):
        for way in range(2):
            near, far = ahead(way, 1), ahead(way, 2)
            send(part.at[slot, ahead(way, 3)], near_r.at[way, slot], ring_sem.at[2, 0], ring_sem.at[0, slot], z=near)
            send(
                part.at[slot, ahead(way, 4), spans[way]], far_r.at[way, slot], ring_sem.at[2, 0], ring_sem.at[0, slot],
                z=far,
            )
        for way in range(2):
            near = ahead(way, 1)
            send(part.at[slot, near], ring_r.at[0, way, slot], ring_sem.at[2, 0], ring_sem.at[1, slot], z=near)

    def z_second(slot):
        phase(f"second{slot}")
        arrived(part.at[slot, 0:3], ring_sem.at[0, slot])
        for way in range(2):
            far = ahead(way, 2)
            mine = part[slot, far] + near_r[way, slot]
            extra = mine[spans[way]] + far_r[way, slot]
            ring_s[way, slot, spans[way]] = extra
            ring_s[way, slot, spans[1 - way]] = mine[spans[1 - way]]
            send(ring_s.at[way, slot], ring_r.at[1, way, slot], ring_sem.at[2, 0], ring_sem.at[1, slot], z=far)

    def z_last(slot):
        phase(f"last{slot}")
        arrived(part.at[slot, 0:4], ring_sem.at[1, slot])
        gw_out[slot] = (
            part[slot, z] + ring_r[0, 0, slot] + ring_r[0, 1, slot] + ring_r[1, 0, slot] + ring_r[1, 1, slot]
        )

    def weight(slot):
        phase(f"wait_ag{slot}")
        pair = peer_y(slot)
        arrived(gv_r.at[slot, 0 : NY - 1], ag_sem.at[1, slot])
        phase(f"weight{slot}")
        fresh = dot_fine_right(k_all, zg_r[slot])
        for block in range(NY):
            gv_r[slot, block] = gv_r[slot, block] + fade[block, pair] * fresh[128 * block : 128 * block + 128, :]
        gathered = gv_r[slot].reshape(512, 128).astype(BF16)
        part[slot] = dot(hid_all[...].reshape(512, 512), gathered).reshape(NZ, 64, 128)
        z_first(slot)

    weight(0)

    phase("scan_z_f")
    wait_z(1, zr_f)
    scan_z(zr_f, zbs_f, False)
    zbr_f[z] = zbs_f[z]
    send_z(3, zbs_f, zbr_f)
    z_second(0)

    phase("wait_zg_all")
    arrived(zg_r.at[0 : NY - 1], zg_sem.at[1])
    phase("grad_h")
    for slot in range(PAIRS):
        pair = peer_y(slot)
        gv_own[pair] = gv_s[pair] + fade[y, pair] * dot_fine_right(k, zg_r[slot])
    grad_v = jnp.concatenate([gv_own[pair].astype(BF16) for pair in range(PAIRS)], axis=1)
    for part_now in range(4):
        span = slice(512 * part_now, 512 * part_now + 512)
        gh_s[:, :, :, span] = dot(grad_v, w[span, :], ((1,), (1,))).reshape(NX, 2, 16, 512)
    send(gh_s.at[:, 1 - c], gh_r, d_sem.at[0, 0], d_sem.at[1, 0], c=1 - c)
    drain_later(gh_r, d_sem.at[0, 0])

    weight(1)

    phase("back_y_f")
    wait_z(3, zbr_f)
    finish_plane(yr_f, ybs_f, zbr_f, False)
    ybr_f[y] = ybs_f[y]
    send_y(4, ybs_f, ybr_f)

    weight(2)

    phase("chip_pair")
    arrived(gh_r, d_sem.at[1, 0])
    gx_s[...] = gh_s[:, c] + gh_r[...]
    for o in range(1, NX):
        send(gx_s.at[peer_x(o)], gx_r.at[x], x_sem.at[0], x_sem.at[1], x=peer_x(o))
    drain_later(gx_r.at[0 : NX - 1], x_sem.at[0])
    gx_r[x] = gx_s[x]

    weight(3)

    phase("grad_k")
    gk = dot_fine_left(blend, q)
    gq = dot_fine_left(blend.T, k)
    wide = lax.broadcasted_iota(jnp.int32, (8, 512), 1)
    chooser = jnp.where(lax.broadcasted_iota(jnp.int32, (8, 512), 0) == wide // 64, 1.0, 0.0)
    pull = jnp.concatenate(
        [ybr_b[pair] + row_of(gain_own, pair) * zg_r[lax.rem(pair + NY - y, NY)] for pair in range(PAIRS)], axis=1
    )
    val_f = vals[...].astype(F32)
    val_scaled = jnp.concatenate([spread(to_end_t, pair) for pair in range(PAIRS)], axis=1) * val_f
    gk = gk + dot_fine(val_scaled, pull, ((1,), (1,)))
    whole = jnp.sum(val_scaled * dot_fine_right(k, pull), axis=0, keepdims=True)
    used = val_f * jnp.concatenate([gv_own[pair] for pair in range(PAIRS)], axis=1)
    gk_out[...] = gk.astype(BF16)

    z_last(0)
    z_second(1)
    z_second(2)
    z_second(3)

    phase("wait_carry")
    wait_y(4, ybr_f)
    phase("grad_q")
    carry = jnp.concatenate([ybr_f[pair] for pair in range(PAIRS)], axis=1)
    cot_scaled = jnp.concatenate([spread(from_start_t, pair) for pair in range(PAIRS)], axis=1) * cot[...].astype(F32)
    gq = gq + dot_fine(cot_scaled, carry, ((1,), (1,)))
    change = cot_scaled * dot_fine_right(q, carry) - used
    high, low = halves(change)
    lowest = (change - high.astype(F32) - low.astype(F32)).astype(BF16)
    picked = chooser.astype(BF16)
    gap = row_sum[...]
    for level in (high, low, lowest):
        gap = gap + dot(picked, level, ((1,), (1,)))
    factors = jnp.concatenate([row_of(factor, pair) for pair in range(PAIRS)], axis=1)
    whole = whole + factors * jnp.sum(carry * pull, axis=0, keepdims=True)
    shared = jnp.sum(chooser * whole, axis=1, keepdims=True)
    for shift in (1, 2, 4, 8, 16, 32, 64):
        gap = gap + jnp.where(lane8 < 128 - shift, pltpu.roll(gap, 128 - shift, 1), 0.0)
    gd_out[...] = (gap + shared) * (-rate / (1.0 + jnp.exp(-pre_v)))
    gq_out[...] = gq.astype(BF16)

    phase("out_h")
    arrived(gx_r.at[0 : NX - 1], x_sem.at[1])
    gh_out[...] = (gx_r[0] + gx_r[1] + gx_r[2] + gx_r[3]).astype(BF16)

    z_last(1)
    z_last(2)
    z_last(3)
    drain_later(part.at[0:PAIRS, 0 : NZ - 1], ring_sem.at[2, 0])

    phase("drain")
    for made in sent:
        made.wait_send()
    stack.close()


def store_all(*refs):
    y = lax.axis_index("y")
    sems = refs[10]
    copies = [pltpu.make_async_copy(refs[i], refs[5 + i], sems.at[i]) for i in range(4)]
    for slot in range(PAIRS):
        pair = lax.rem(y + slot, PAIRS)
        place = refs[9].at[:, pl.ds(pl.multiple_of(128 * pair, 128), 128)]
        copies.append(pltpu.make_async_copy(refs[4].at[slot], place, sems.at[4 + slot]))
    for made in copies:
        made.start()
    for made in copies:
        made.wait()


def local(hidden, value_weight, key_vecs, queries, decay_pre, decay_rate, cotangent):
    dma = pltpu.SemaphoreType.DMA
    f32 = lambda *shape: pltpu.VMEM(shape, F32)
    y_box, z_box = (NY, STATE + 8, 128), (NZ, ROWS + 8, 128)
    z_back, y_back = (NZ, ROWS, 128), (NY, STATE, 128)
    outs = pl.pallas_call(
        kernel,
        out_shape=(
            jax.ShapeDtypeStruct((TOK, STATE), BF16),
            jax.ShapeDtypeStruct((TOK, STATE), BF16),
            jax.ShapeDtypeStruct((HEADS, TOK), F32),
            jax.ShapeDtypeStruct((16, 2048), BF16),
            jax.ShapeDtypeStruct((PAIRS, 64, 128), F32),
        ),
        in_specs=[pl.BlockSpec(memory_space=pltpu.HBM)] * 7,
        out_specs=[pl.BlockSpec(memory_space=pltpu.VMEM)] * 5,
        scratch_shapes=[
            *[f32(*y_box)] * 4,
            *[f32(*z_box)] * 4,
            *[f32(*z_back)] * 4,
            *[f32(*y_back)] * 4,
            f32(NZ, NY, 64, TOK),
            f32(NY, 64, TOK),
            f32(NX, NY, 64, TOK),
            f32(NX, NY, 64, TOK),
            pltpu.VMEM((NX, 2, 64, 512), BF16),
            f32(PAIRS, TOK, 128),
            f32(PAIRS, NY, TOK, 128),
            f32(PAIRS, NZ, 64, 128),
            f32(2, PAIRS, 64, 128),
            f32(2, PAIRS, 32, 128),
            f32(2, PAIRS, 64, 128),
            f32(2, 2, PAIRS, 64, 128),
            f32(NX, 2, 16, 2048),
            f32(NX, 16, 2048),
            f32(NX, 16, 2048),
            f32(NX, 16, 2048),
            f32(STATE, 128),
            f32(NY, STATE, 128),
            f32(TOK, STATE),
            f32(NY, TOK, STATE),
            f32(HEADS, TOK),
            f32(NY, HEADS, TOK),
            f32(NY, PAIRS, TOK, 128),
            f32(PAIRS, TOK, 128),
            pltpu.VMEM((TOK, 512), BF16),
            f32(HEADS, TOK),
            pltpu.VMEM((TOK, 2048), BF16),
            pltpu.VMEM((2048, 512), BF16),
            pltpu.VMEM((TOK, STATE), BF16),
            pltpu.VMEM((TOK, STATE), BF16),
            f32(HEADS, TOK),
            f32(1, HEADS),
            pltpu.VMEM((512, TOK), BF16),
            pltpu.VMEM((TOK, 512), BF16),
            dma((2, 7)),
            dma((2, 4)),
            dma((2, PAIRS)),
            dma((3, PAIRS)),
            dma((2, 2)),
            dma((2,)),
            dma((7,)),
            dma((2,)),
            dma((2,)),
        ],
        compiler_params=pltpu.CompilerParams(
            collective_id=0, has_side_effects=True, vmem_limit_bytes=VMEM_LIMIT
        ),
        name="mixer_backward",
    )(
        *[
            pltpu.with_memory_space_constraint(a, pltpu.HBM)
            for a in (
                hidden,
                value_weight,
                key_vecs.reshape(TOK, STATE),
                queries.reshape(TOK, STATE),
                decay_pre.T,
                decay_rate[None, :],
                cotangent.reshape(TOK, 512).T,
            )
        ]
    )
    gk, gq, gd, gh, gw = pl.pallas_call(
        store_all,
        out_shape=(
            *[jax.ShapeDtypeStruct(o.shape, o.dtype) for o in outs[:4]],
            jax.ShapeDtypeStruct((64, 512), F32),
        ),
        in_specs=[pl.BlockSpec(memory_space=pltpu.VMEM)] * 5,
        out_specs=[pl.BlockSpec(memory_space=pltpu.HBM)] * 5,
        scratch_shapes=[dma((8,))],
        compiler_params=pltpu.CompilerParams(vmem_limit_bytes=2 * 1024 * 1024),
        name="store_all",
    )(*outs)
    return gk.reshape(TOK, 1, STATE), gq.reshape(TOK, 1, STATE), gd.T, gh, gw


def solution(mesh):
    split = Mesh(mesh.devices.reshape(NZ, NY, NX, 2), ("z", "y", "x", "c"))
    placed = (
        P(SP, None),
        P(None, TP),
        P(SP, TP, None),
        P(SP, TP, None),
        P(SP, TP),
        P(TP),
        P(SP, TP, None),
    )
    return jax.shard_map(
        local,
        mesh=split,
        in_specs=placed,
        out_specs=(P(SP, TP, None), P(SP, TP, None), P(SP, TP), P(SP + TP, None), P(SP, TP)),
        check_vma=False,
    )
```

```python
import contextlib

import jax
import jax.numpy as jnp
from jax import lax
from jax.experimental import pallas as pl
from jax.experimental.pallas import tpu as pltpu
from jax.sharding import Mesh
from jax.sharding import PartitionSpec as P

F32, BF16 = jnp.float32, jnp.bfloat16
MESH = pl.DeviceIdType.MESH
SP, TP = ("z", "y"), ("x", "c")
NZ, NY, NX = 8, 4, 4
TOK, STATE, PAIRS, HEADS = 128, 128, 4, 8
ROWS = STATE // NZ
VMEM_LIMIT = 48 * 1024 * 1024


def dot(a, b, dims=((1,), (0,))):
    return lax.dot_general(a, b, (dims, ((), ())), preferred_element_type=F32)


def halves(a):
    high = a.astype(BF16)
    return high, (a - high.astype(F32)).astype(BF16)


def dot_fine_right(a, b, dims=((1,), (0,))):
    high, low = halves(b)
    return dot(a, high, dims) + dot(a, low, dims)


def dot_fine_left(a, b, dims=((1,), (0,))):
    high, low = halves(a)
    return dot(high, b, dims) + dot(low, b, dims)


def dot_fine(a, b, dims=((1,), (0,))):
    a_high, a_low = halves(a)
    b_high, b_low = halves(b)
    return dot(a_high, b_high, dims) + dot(a_high, b_low, dims) + dot(a_low, b_high, dims)


def cols(pair):
    return slice(128 * pair, 128 * pair + 128)


def kernel(
    hid_at, w_at, k_at, q_at, pre_at, rate_at, cot_at,
    gk_out, gq_out, gd_out, gh_out, gw_out,
    ys_f, yr_f, zs_b, zr_b, zs_f, zr_f,
    zbs_b, zbr_b, zbs_f, zbr_f, ybs_f, ybr_f,
    hid_t, hid_p, hid_x, hid_c, hid_all, gv_r, part, near_r, far_r, ring_s, ring_r,
    gh_s, gh_r, gx_s, gx_r, zg_s, zg_r, k_s, k_r, q_s, q_r, q_t, cot_s, cot_r, cum_s, cum_r,
    score, near_end, pulls, gains, suffix, reach, pull_own, gv_own, vals, row_sum,
    hid, w, k_in, q_in, pre, rate_in, cot_t, cot,
    y_sem, z_sem, rest_sem, ring_sem, d_sem, x_sem, in_sem, h_sem, zg_sem,
):
    z, y = lax.axis_index("z"), lax.axis_index("y")
    x, c = lax.axis_index("x"), lax.axis_index("c")
    lane = lax.broadcasted_iota(jnp.int32, (128, 128), 1)
    first_head = lane[0:1, :] < 64
    sent = []
    stack = contextlib.ExitStack()

    def phase(name):
        stack.close()
        stack.enter_context(jax.named_scope(name))

    def peer_y(o):
        return lax.rem(y + o, NY)

    def peer_z(o):
        return lax.rem(z + o, NZ)

    def peer_x(o):
        return lax.rem(x + o, NX)

    def copy(src, dst, s_sem, r_sem, **where):
        return pltpu.make_async_remote_copy(
            src_ref=src, dst_ref=dst, send_sem=s_sem, recv_sem=r_sem, device_id=where, device_id_type=MESH
        )

    def send(src, dst, s_sem, r_sem, **where):
        copy(src, dst, s_sem, r_sem, **where).start()

    def arrived(dst, r_sem):
        copy(dst, dst, r_sem, r_sem, c=1 - c).wait_recv()

    def drain_later(like, s_sem):
        sent.append(copy(like, like, s_sem, s_sem, c=1 - c))

    def send_y(kind, src, dst):
        for o in range(1, NY):
            send(src.at[peer_y(o)], dst.at[y], y_sem.at[0, kind], y_sem.at[1, kind], y=peer_y(o))
        drain_later(dst.at[0 : NY - 1], y_sem.at[0, kind])

    def share_y(kind, src, dst):
        for o in range(1, NY):
            send(src, dst.at[y], y_sem.at[0, kind], y_sem.at[1, kind], y=peer_y(o))
        drain_later(dst.at[0 : NY - 1], y_sem.at[0, kind])

    def wait_y(kind, dst):
        arrived(dst.at[0 : NY - 1], y_sem.at[1, kind])

    def send_z(kind, src, dst):
        for o in range(1, NZ):
            send(src.at[peer_z(o)], dst.at[z], z_sem.at[0, kind], z_sem.at[1, kind], z=peer_z(o))
        drain_later(dst.at[0 : NZ - 1], z_sem.at[0, kind])

    def wait_z(kind, dst):
        arrived(dst.at[0 : NZ - 1], z_sem.at[1, kind])

    phase("enter")
    loads = [
        pltpu.make_async_copy(src, dst, in_sem.at[i])
        for i, (src, dst) in enumerate(
            [(cot_at, cot_t), (q_at, q_in), (pre_at, pre), (rate_at, rate_in), (k_at, k_in), (hid_at, hid), (w_at, w)]
        )
    ]
    for made in loads:
        made.start()

    barrier = pltpu.get_barrier_semaphore()
    for o in range(1, NY):
        pl.semaphore_signal(barrier, inc=1, device_id={"y": peer_y(o)}, device_id_type=MESH)
    for o in range(1, NZ):
        pl.semaphore_signal(barrier, inc=1, device_id={"z": peer_z(o)}, device_id_type=MESH)
    for o in range(1, NX):
        pl.semaphore_signal(barrier, inc=1, device_id={"x": peer_x(o)}, device_id_type=MESH)
    pl.semaphore_signal(barrier, inc=1, device_id={"c": 1 - c}, device_id_type=MESH)

    phase("widen")
    loads[0].wait()
    for pair in range(PAIRS):
        cot_s[pair] = cot_t[cols(pair), :].astype(F32)
    cot_r[y] = cot_s[...]
    loads[1].wait()
    q = q_in[...]
    q_s[...] = q.astype(F32)
    q_r[y] = q_s[...]
    phase("barrier")
    pl.semaphore_wait(barrier, NY + NZ + NX - 2)
    share_y(3, q_s, q_r)
    for o in range(1, NY):
        send(cot_s.at[peer_y(o)], cot_r.at[y, peer_y(o)], y_sem.at[0, 0], y_sem.at[1, 0], y=peer_y(o))
    drain_later(cot_r.at[0, 0 : NY - 1], y_sem.at[0, 0])

    phase("decay")
    loads[2].wait()
    loads[3].wait()
    pre_v = pre[...]
    square = lax.broadcasted_iota(jnp.int32, (8, 8), 0) == lax.broadcasted_iota(jnp.int32, (8, 8), 1)
    rate = jnp.sum(jnp.where(square, jnp.broadcast_to(rate_in[...], (8, 8)), 0.0), axis=1, keepdims=True)
    soft = jnp.maximum(pre_v, 0.0) + jnp.log1p(jnp.exp(-jnp.abs(pre_v)))
    cum = -rate * soft
    lane8 = lane[0:8, :]
    for shift in (1, 2, 4, 8, 16, 32, 64):
        cum = cum + jnp.where(lane8 >= shift, pltpu.roll(cum, shift, 1), 0.0)
    cum_s[...] = cum
    cum_r[y] = cum
    total = jnp.broadcast_to(cum[:, 127:128], (8, 128))
    factor = jnp.exp(total)
    cum_t = cum.T
    from_start = jnp.exp(cum)
    from_start_t = from_start.T
    to_end_t = jnp.exp(total - cum).T

    def spread(columns, pair):
        return jnp.where(first_head, columns[:, 2 * pair : 2 * pair + 1], columns[:, 2 * pair + 1 : 2 * pair + 2])

    def row_of(gains, pair):
        return jnp.where(first_head, gains[2 * pair : 2 * pair + 1, :], gains[2 * pair + 1 : 2 * pair + 2, :])

    share_y(6, cum_s, cum_r)
    loads[4].wait()
    k = k_in[...]
    k_s[...] = k.astype(F32)
    k_r[y] = k_s[...]

    phase("hidden")
    loads[5].wait()
    for block in range(16):
        turned = hid[:, cols(block)].astype(F32).T
        hid_t[block // 2, 2 * (block % 2) : 2 * (block % 2) + 2] = turned.reshape(2, 64, 128)
    seat = 2 * x + c
    for o in range(1, NY):
        send(hid_t.at[seat, peer_y(o)], hid_p.at[y], y_sem.at[0, 2], y_sem.at[1, 2], y=peer_y(o))
    drain_later(hid_p.at[0 : NY - 1], y_sem.at[0, 2])
    hid_p[y] = hid_t[seat, y]
    phase("values")
    loads[6].wait()
    k_t = k_s[...].T.astype(BF16)
    for half in range(2):
        span = slice(256 * half, 256 * half + 256)
        vals[:, span] = dot(hid[...], w[:, span]).astype(BF16)
    scaled = jnp.concatenate([spread(to_end_t, pair) for pair in range(PAIRS)], axis=1) * vals[...].astype(F32)
    states = dot_fine_right(k_t, scaled)
    for pair in range(PAIRS):
        ys_f[pair, 0:128, :] = states[:, cols(pair)]
        ys_f[pair, 128:136, :] = jnp.broadcast_to(row_of(factor, pair), (8, 128))
    yr_f[y] = ys_f[y]
    send_y(1, ys_f, yr_f)

    share_y(5, k_s, k_r)

    for o in range(1, PAIRS):
        for way in range(2):
            side = peer_y(1 + 2 * way)
            pair = peer_y(1 + 2 * way + o)
            send(cot_s.at[pair], cot_r.at[y, pair], rest_sem.at[2, 0], rest_sem.at[way, o - 1], y=side)
    drain_later(cot_r.at[0:2, 0 : NY - 1], rest_sem.at[2, 0])
    halves_of = (slice(0, 64), slice(64, 128))

    def pass_on(way, o):
        origin, side = peer_y(3 - 2 * way), peer_y(1 + 2 * way)
        if o > 0:
            arrived(cot_r.at[origin, peer_y(o)], rest_sem.at[way, o - 1])
        if o != (1, 3)[way]:
            half = cot_r.at[origin, peer_y(o), halves_of[way]]
            send(half, half, y_sem.at[0, 7], y_sem.at[1, 7], y=side)

    phase("block")
    for pair in range(PAIRS):
        cot[:, cols(pair)] = cot_t[cols(pair), :].astype(F32).T.astype(BF16)
    causal = lax.broadcasted_iota(jnp.int32, (128, 128), 0) <= lane
    blend = jnp.zeros((128, 128), F32)
    score_own = dot(k, q, ((1,), (1,)))
    for pair in range(PAIRS):
        cot_pair, val_pair = cot[:, cols(pair)], vals[:, cols(pair)]
        for side in range(2):
            head = 2 * pair + side
            mine = first_head if side == 0 else jnp.logical_not(first_head)
            across = jnp.where(causal, cum[head : head + 1, :] - cum_t[:, head : head + 1], 0.0)
            damping = jnp.where(causal, jnp.exp(across), 0.0)
            cot_head = jnp.where(mine, cot_pair.astype(F32), 0.0).astype(BF16)
            moved = dot(val_pair, cot_head, ((1,), (1,))) * damping
            blend = blend + moved
            row_sum[head : head + 1, :] = jnp.sum(moved * score_own, axis=0, keepdims=True)

    upper = lax.broadcasted_iota(jnp.int32, (128, 128), 0) < 64

    def rows_of(slot, block):
        pair = peer_y(slot)
        return [cum_r[block, pl.ds(2 * pair + side, 1), :] for side in range(2)]

    def block_pull(slot, block):
        first, second = rows_of(slot, block)
        growth = jnp.where(upper, jnp.exp(first), jnp.exp(second))
        pulls[slot, block] = dot_fine_right(q_t[block], growth * cot_r[block, peer_y(slot)], ((1,), (1,)))
        gain = jnp.where(first_head, jnp.exp(first[:, 127:128]), jnp.exp(second[:, 127:128]))
        gains[slot, block] = jnp.broadcast_to(gain, (8, 128))

    def plane_chain(slot):
        after = gain = None
        for block in range(NY - 1, -1, -1):
            suffix[slot, block] = jnp.zeros((128, 128), F32) if after is None else after
            reach[slot, block] = jnp.ones((8, 128), F32) if gain is None else gain
            here = gains[slot, block]
            after = pulls[slot, block] if after is None else pulls[slot, block] + here[0:1, :] * after
            gain = here if gain is None else gain * here
        return after, gain

    def block_values(slot, block):
        rows = rows_of(slot, block)
        tall = [jnp.broadcast_to(row, (128, 128)).T for row in rows]
        near_end[slot, block] = jnp.exp(
            jnp.where(first_head, rows[0][:, 127:128] - tall[0], rows[1][:, 127:128] - tall[1])
        )
        weights = []
        for side in range(2):
            across = jnp.where(causal, rows[side] - tall[side], 0.0)
            weights.append(score[block] * jnp.where(causal, jnp.exp(across), 0.0))
        cot_pair = cot_r[block, peer_y(slot)]
        cots = jnp.concatenate([jnp.where(upper, cot_pair, 0.0), jnp.where(upper, 0.0, cot_pair)], axis=1)
        gv_r[slot, block] = dot_fine_left(jnp.concatenate(weights, axis=1), cots.astype(BF16), ((1,), (1,)))

    def scan_plane(got, kept, z_send, reverse):
        state, gain = None, None
        order = range(NY - 1, -1, -1) if reverse else range(NY)
        for block in order:
            value, here = got[block, 0:128, :], got[block, 128:129, :]
            if state is None:
                kept[block] = jnp.zeros((128, 128), F32)
                state, gain = value, here
            else:
                kept[block] = state
                state, gain = here * state + value, gain * here
        for row in range(NZ):
            z_send[row, 0:ROWS, :] = state[row * ROWS : row * ROWS + ROWS, :]
            z_send[row, ROWS : ROWS + 8, :] = jnp.broadcast_to(gain, (8, 128))

    def scan_z(got, back, reverse):
        state = None
        for plane in range(NZ - 1, -1, -1) if reverse else range(NZ):
            value, here = got[plane, 0:ROWS, :], got[plane, ROWS : ROWS + 1, :]
            if state is None:
                back[plane] = jnp.zeros((ROWS, 128), F32)
                state = value
            else:
                back[plane] = state
                state = here * state + value

    def finish_plane(got, kept, plane_in, reverse):
        incoming = plane_in[...].reshape(STATE, 128)
        gain = None
        for block in range(NY - 1, -1, -1) if reverse else range(NY):
            kept[block] = kept[block] + (incoming if gain is None else gain * incoming)
            here = got[block, 128:129, :]
            gain = here if gain is None else gain * here

    phase("first")
    wait_y(6, cum_r)
    wait_y(3, q_r)
    arrived(cot_r.at[0, 0 : NY - 1], y_sem.at[1, 0])
    phase("pulls0")
    for block in range(NY):
        q_t[block] = q_r[block].T.astype(BF16)
    for block in range(NY):
        block_pull(0, block)
    state, gain = plane_chain(0)
    for row in range(NZ):
        zs_b[row, 0:ROWS, :] = state[row * ROWS : row * ROWS + ROWS, :]
        zs_b[row, ROWS : ROWS + 8, :] = gain
    zr_b[z] = zs_b[z]
    send_z(0, zs_b, zr_b)
    pass_on(0, 0)
    pass_on(1, 0)
    for slot in range(1, PAIRS):
        block_pull(slot, y)

    phase("hidden_x")
    wait_y(2, hid_p)
    for o in range(1, NX):
        send(hid_p, hid_x.at[x], h_sem.at[0], h_sem.at[1], x=peer_x(o))
    drain_later(hid_x.at[0 : NX - 1], h_sem.at[0])
    hid_x[x] = hid_p[...]

    phase("scan_y_f")
    wait_y(1, yr_f)
    scan_plane(yr_f, ybs_f, zs_f, False)
    zr_f[z] = zs_f[z]
    send_z(1, zs_f, zr_f)

    phase("scan_z_b")
    wait_z(0, zr_b)
    scan_z(zr_b, zbs_b, True)
    zbr_b[z] = zbs_b[z]
    send_z(2, zbs_b, zbr_b)

    phase("hidden_c")
    arrived(hid_x.at[0 : NX - 1], h_sem.at[1])
    send(hid_x, hid_c, d_sem.at[0, 1], d_sem.at[1, 1], c=1 - c)
    drain_later(hid_x, d_sem.at[0, 1])

    phase("keys_far")
    wait_y(5, k_r)
    phase("values0")
    for block in range(NY):
        score[block] = dot(k_r[block].astype(BF16), q_r[block].astype(BF16), ((1,), (1,)))
    for block in range(NY):
        block_values(0, block)
    for slot in range(1, PAIRS):
        block_values(slot, y)

    phase("pass1")
    pass_on(0, 1)
    pass_on(1, 1)
    phase("scan_z_f")
    wait_z(1, zr_f)
    scan_z(zr_f, zbs_f, False)
    zbr_f[z] = zbs_f[z]
    send_z(3, zbs_f, zbr_f)

    phase("pass2")
    pass_on(0, 2)
    pass_on(1, 2)

    phase("wait_zg")
    wait_z(2, zbr_b)
    zg_s[...] = zbr_b[...].reshape(STATE, 128)
    zg_r[0] = zg_s[...]
    for o in range(1, NY):
        send(zg_s, zg_r.at[NY - o], zg_sem.at[0], zg_sem.at[1], y=peer_y(o))
    drain_later(zg_r.at[0 : NY - 1], zg_sem.at[0])

    phase("hid_all")
    arrived(hid_c, d_sem.at[1, 1])
    for across_x in range(NX):
        for block in range(NY):
            hid_all[across_x, c, :, cols(block)] = hid_x[across_x, block].astype(BF16)
            hid_all[across_x, 1 - c, :, cols(block)] = hid_c[across_x, block].astype(BF16)

    spans = (slice(0, 32), slice(32, 64))

    def ahead(way, o):
        return peer_z(o) if way == 0 else peer_z(NZ - o)

    def z_first(slot):
        sems = (ring_sem.at[2, 0], ring_sem.at[0, slot])
        for way in range(2):
            src = part.at[slot, ahead(way, 4), spans[way]]
            send(src, far_r.at[way, slot], *sems, z=ahead(way, 2))
        for way in range(2):
            send(part.at[slot, ahead(way, 3)], near_r.at[way, slot], *sems, z=ahead(way, 1))

    def z_direct(slot):
        for way in range(2):
            near = ahead(way, 1)
            send(part.at[slot, near], ring_r.at[0, way, slot], ring_sem.at[2, 0], ring_sem.at[1, slot], z=near)

    def z_second(slot):
        phase(f"second{slot}")
        arrived(part.at[slot, 0:3], ring_sem.at[0, slot])
        for way in range(2):
            far = ahead(way, 2)
            mine = part[slot, far] + near_r[way, slot]
            extra = mine[spans[way]] + far_r[way, slot]
            ring_s[way, slot, spans[way]] = extra
            ring_s[way, slot, spans[1 - way]] = mine[spans[1 - way]]
            send(ring_s.at[way, slot], ring_r.at[1, way, slot], ring_sem.at[2, 0], ring_sem.at[1, slot], z=far)

    def z_last(slot):
        phase(f"last{slot}")
        arrived(part.at[slot, 0:4], ring_sem.at[1, slot])
        gw_out[slot] = (
            part[slot, z] + ring_r[0, 0, slot] + ring_r[0, 1, slot] + ring_r[1, 0, slot] + ring_r[1, 1, slot]
        )

    def own_values(slot):
        pair = peer_y(slot)
        pull_now = suffix[slot, y] + reach[slot, y, 0:1, :] * zg_r[slot]
        pull_own[pair] = pull_now
        gv_own[pair] = gv_r[slot, y] + near_end[slot, y] * dot_fine_right(k, pull_now)

    def weight(slot):
        phase(f"weight{slot}")
        incoming = zg_r[slot]
        for block in range(NY):
            pull_now = suffix[slot, block] + reach[slot, block, 0:1, :] * incoming
            from_state = dot_fine_right(k_r[block].astype(BF16), pull_now)
            gv_r[slot, block] = gv_r[slot, block] + near_end[slot, block] * from_state
        gathered = gv_r[slot].reshape(512, 128).astype(BF16)
        part[slot] = dot(hid_all[...].reshape(512, 512), gathered).reshape(NZ, 64, 128)
        z_first(slot)

    own_values(0)
    weight(0)
    z_direct(0)

    phase("pass3")
    pass_on(0, 3)
    pass_on(1, 3)
    drain_later(cot_r.at[0, 0 : NY - 1], y_sem.at[0, 7])
    phase("values_near")
    for slot in range(1, PAIRS):
        for o in (1, 3):
            block_pull(slot, peer_y(o))
            block_values(slot, peer_y(o))

    phase("wait_opposite")
    arrived(cot_r.at[0, 0 : NY - 1], y_sem.at[1, 7])
    phase("values_far")
    for slot in range(1, PAIRS):
        block_pull(slot, peer_y(2))
        block_values(slot, peer_y(2))
        plane_chain(slot)
    phase("back_y_f")
    wait_z(3, zbr_f)
    finish_plane(yr_f, ybs_f, zbr_f, False)
    ybr_f[y] = ybs_f[y]
    send_y(4, ybs_f, ybr_f)

    phase("wait_zg_all")
    arrived(zg_r.at[0 : NY - 1], zg_sem.at[1])
    phase("own_values")
    for slot in range(1, PAIRS):
        own_values(slot)
    phase("grad_h")
    grad_v = jnp.concatenate([gv_own[pair].astype(BF16) for pair in range(PAIRS)], axis=1)
    for part_now in range(4):
        span = slice(512 * part_now, 512 * part_now + 512)
        gh_s[:, :, :, span] = dot(grad_v, w[span, :], ((1,), (1,))).reshape(NX, 2, 16, 512)
    send(gh_s.at[:, 1 - c], gh_r, d_sem.at[0, 0], d_sem.at[1, 0], c=1 - c)
    drain_later(gh_r, d_sem.at[0, 0])

    weight(1)
    z_second(0)
    weight(2)
    weight(3)
    for slot in range(1, PAIRS):
        z_direct(slot)

    phase("chip_pair")
    arrived(gh_r, d_sem.at[1, 0])
    gx_s[...] = gh_s[:, c] + gh_r[...]
    for o in range(1, NX):
        send(gx_s.at[peer_x(o)], gx_r.at[x], x_sem.at[0], x_sem.at[1], x=peer_x(o))
    drain_later(gx_r.at[0 : NX - 1], x_sem.at[0])
    gx_r[x] = gx_s[x]

    z_second(1)
    phase("grad_k")
    gk = dot_fine_left(blend, q)
    gq = dot_fine_left(blend.T, k)
    wide = lax.broadcasted_iota(jnp.int32, (8, 512), 1)
    chooser = jnp.where(lax.broadcasted_iota(jnp.int32, (8, 512), 0) == wide // 64, 1.0, 0.0)
    pull = jnp.concatenate([pull_own[pair] for pair in range(PAIRS)], axis=1)
    val_f = vals[...].astype(F32)
    val_scaled = jnp.concatenate([spread(to_end_t, pair) for pair in range(PAIRS)], axis=1) * val_f
    gk = gk + dot_fine(val_scaled, pull, ((1,), (1,)))
    whole = jnp.sum(val_scaled * dot_fine_right(k, pull), axis=0, keepdims=True)
    used = val_f * jnp.concatenate([gv_own[pair] for pair in range(PAIRS)], axis=1)
    gk_out[...] = gk.astype(BF16)

    z_second(2)
    z_second(3)
    z_last(0)

    phase("wait_carry")
    wait_y(4, ybr_f)
    phase("grad_q")
    carry = jnp.concatenate([ybr_f[pair] for pair in range(PAIRS)], axis=1)
    cot_scaled = jnp.concatenate([spread(from_start_t, pair) for pair in range(PAIRS)], axis=1) * cot[...].astype(F32)
    gq = gq + dot_fine(cot_scaled, carry, ((1,), (1,)))
    change = cot_scaled * dot_fine_right(q, carry) - used
    high, low = halves(change)
    lowest = (change - high.astype(F32) - low.astype(F32)).astype(BF16)
    picked = chooser.astype(BF16)
    gap = row_sum[...]
    for level in (high, low, lowest):
        gap = gap + dot(picked, level, ((1,), (1,)))
    factors = jnp.concatenate([row_of(factor, pair) for pair in range(PAIRS)], axis=1)
    whole = whole + factors * jnp.sum(carry * pull, axis=0, keepdims=True)
    shared = jnp.sum(chooser * whole, axis=1, keepdims=True)
    for shift in (1, 2, 4, 8, 16, 32, 64):
        gap = gap + jnp.where(lane8 < 128 - shift, pltpu.roll(gap, 128 - shift, 1), 0.0)
    gd_out[...] = (gap + shared) * (-rate / (1.0 + jnp.exp(-pre_v)))
    gq_out[...] = gq.astype(BF16)

    phase("out_h")
    arrived(gx_r.at[0 : NX - 1], x_sem.at[1])
    gh_out[...] = (gx_r[0] + gx_r[1] + gx_r[2] + gx_r[3]).astype(BF16)

    z_last(1)
    z_last(2)
    z_last(3)
    drain_later(part.at[0:PAIRS, 0 : NZ - 1], ring_sem.at[2, 0])

    phase("drain")
    for made in sent:
        made.wait_send()
    stack.close()


def store_all(*refs):
    y = lax.axis_index("y")
    sems = refs[10]
    copies = [pltpu.make_async_copy(refs[i], refs[5 + i], sems.at[i]) for i in range(4)]
    for slot in range(PAIRS):
        pair = lax.rem(y + slot, PAIRS)
        place = refs[9].at[:, pl.ds(pl.multiple_of(128 * pair, 128), 128)]
        copies.append(pltpu.make_async_copy(refs[4].at[slot], place, sems.at[4 + slot]))
    for made in copies:
        made.start()
    for made in copies:
        made.wait()


def local(hidden, value_weight, key_vecs, queries, decay_pre, decay_rate, cotangent):
    dma = pltpu.SemaphoreType.DMA
    f32 = lambda *shape: pltpu.VMEM(shape, F32)
    y_box, z_box = (NY, STATE + 8, 128), (NZ, ROWS + 8, 128)
    z_back, y_back = (NZ, ROWS, 128), (NY, STATE, 128)
    outs = pl.pallas_call(
        kernel,
        out_shape=(
            jax.ShapeDtypeStruct((TOK, STATE), BF16),
            jax.ShapeDtypeStruct((TOK, STATE), BF16),
            jax.ShapeDtypeStruct((HEADS, TOK), F32),
            jax.ShapeDtypeStruct((16, 2048), BF16),
            jax.ShapeDtypeStruct((PAIRS, 64, 128), F32),
        ),
        in_specs=[pl.BlockSpec(memory_space=pltpu.HBM)] * 7,
        out_specs=[pl.BlockSpec(memory_space=pltpu.VMEM)] * 5,
        scratch_shapes=[
            *[f32(*y_box)] * 2,
            *[f32(*z_box)] * 4,
            *[f32(*z_back)] * 4,
            *[f32(*y_back)] * 2,
            f32(NZ, NY, 64, TOK),
            f32(NY, 64, TOK),
            f32(NX, NY, 64, TOK),
            f32(NX, NY, 64, TOK),
            pltpu.VMEM((NX, 2, 64, 512), BF16),
            f32(PAIRS, NY, TOK, 128),
            f32(PAIRS, NZ, 64, 128),
            f32(2, PAIRS, 64, 128),
            f32(2, PAIRS, 32, 128),
            f32(2, PAIRS, 64, 128),
            f32(2, 2, PAIRS, 64, 128),
            f32(NX, 2, 16, 2048),
            f32(NX, 16, 2048),
            f32(NX, 16, 2048),
            f32(NX, 16, 2048),
            f32(STATE, 128),
            f32(NY, STATE, 128),
            f32(TOK, STATE),
            f32(NY, TOK, STATE),
            f32(TOK, STATE),
            f32(NY, TOK, STATE),
            pltpu.VMEM((NY, STATE, TOK), BF16),
            f32(PAIRS, 128, TOK),
            f32(NY, PAIRS, 128, TOK),
            f32(HEADS, TOK),
            f32(NY, HEADS, TOK),
            f32(NY, TOK, TOK),
            f32(PAIRS, NY, TOK, 128),
            f32(PAIRS, NY, STATE, 128),
            f32(PAIRS, NY, 8, 128),
            f32(PAIRS, NY, STATE, 128),
            f32(PAIRS, NY, 8, 128),
            f32(PAIRS, STATE, 128),
            f32(PAIRS, TOK, 128),
            pltpu.VMEM((TOK, 512), BF16),
            f32(HEADS, TOK),
            pltpu.VMEM((TOK, 2048), BF16),
            pltpu.VMEM((2048, 512), BF16),
            pltpu.VMEM((TOK, STATE), BF16),
            pltpu.VMEM((TOK, STATE), BF16),
            f32(HEADS, TOK),
            f32(1, HEADS),
            pltpu.VMEM((512, TOK), BF16),
            pltpu.VMEM((TOK, 512), BF16),
            dma((2, 8)),
            dma((2, 4)),
            dma((3, 3)),
            dma((3, PAIRS)),
            dma((2, 2)),
            dma((2,)),
            dma((7,)),
            dma((2,)),
            dma((2,)),
        ],
        compiler_params=pltpu.CompilerParams(
            collective_id=0, has_side_effects=True, vmem_limit_bytes=VMEM_LIMIT
        ),
        name="mixer_backward",
    )(
        *[
            pltpu.with_memory_space_constraint(a, pltpu.HBM)
            for a in (
                hidden,
                value_weight,
                key_vecs.reshape(TOK, STATE),
                queries.reshape(TOK, STATE),
                decay_pre.T,
                decay_rate[None, :],
                cotangent.reshape(TOK, 512).T,
            )
        ]
    )
    gk, gq, gd, gh, gw = pl.pallas_call(
        store_all,
        out_shape=(
            *[jax.ShapeDtypeStruct(o.shape, o.dtype) for o in outs[:4]],
            jax.ShapeDtypeStruct((64, 512), F32),
        ),
        in_specs=[pl.BlockSpec(memory_space=pltpu.VMEM)] * 5,
        out_specs=[pl.BlockSpec(memory_space=pltpu.HBM)] * 5,
        scratch_shapes=[dma((8,))],
        compiler_params=pltpu.CompilerParams(vmem_limit_bytes=2 * 1024 * 1024),
        name="store_all",
    )(*outs)
    return gk.reshape(TOK, 1, STATE), gq.reshape(TOK, 1, STATE), gd.T, gh, gw


def solution(mesh):
    split = Mesh(mesh.devices.reshape(NZ, NY, NX, 2), ("z", "y", "x", "c"))
    placed = (
        P(SP, None),
        P(None, TP),
        P(SP, TP, None),
        P(SP, TP, None),
        P(SP, TP),
        P(TP),
        P(SP, TP, None),
    )
    return jax.shard_map(
        local,
        mesh=split,
        in_specs=placed,
        out_specs=(P(SP, TP, None), P(SP, TP, None), P(SP, TP), P(SP + TP, None), P(SP, TP)),
        check_vma=False,
    )
```

```python
import contextlib

import jax
import jax.numpy as jnp
from jax import lax
from jax.experimental import pallas as pl
from jax.experimental.pallas import tpu as pltpu
from jax.sharding import Mesh
from jax.sharding import PartitionSpec as P

F32, BF16 = jnp.float32, jnp.bfloat16
MESH = pl.DeviceIdType.MESH
SP, TP = ("z", "y"), ("x", "c")
NZ, NY, NX = 8, 4, 4
TOK, STATE, PAIRS, HEADS = 128, 128, 4, 8
ROWS = STATE // NZ
VMEM_LIMIT = 48 * 1024 * 1024


def dot(a, b, dims=((1,), (0,))):
    return lax.dot_general(a, b, (dims, ((), ())), preferred_element_type=F32)


def halves(a):
    high = a.astype(BF16)
    return high, (a - high.astype(F32)).astype(BF16)


def dot_fine_right(a, b, dims=((1,), (0,))):
    high, low = halves(b)
    return dot(a, high, dims) + dot(a, low, dims)


def dot_fine_left(a, b, dims=((1,), (0,))):
    high, low = halves(a)
    return dot(high, b, dims) + dot(low, b, dims)


def dot_fine(a, b, dims=((1,), (0,))):
    a_high, a_low = halves(a)
    b_high, b_low = halves(b)
    return dot(a_high, b_high, dims) + dot(a_high, b_low, dims) + dot(a_low, b_high, dims)


def cols(pair):
    return slice(128 * pair, 128 * pair + 128)


def kernel(
    hid_at, w_at, k_at, q_at, pre_at, rate_at, cot_at,
    gk_out, gq_out, gd_out, gh_out, gw_out,
    ys_f, yr_f, zs_b, zr_b, zs_f, zr_f,
    zbs_b, zbr_b, zbs_f, zbr_f, ybs_f, ybr_f,
    hid_t, hid_p, hid_x, hid_c, hid_all, gv_r, part, near_r, far_r, ring_s, ring_r,
    gh_s, gh_r, gx_s, gx_r, zg_s, zg_r, k_s, k_r, q_s, q_r, q_t, cot_s, cot_r, cum_s, cum_r,
    score, near_end, pulls, gains, suffix, reach, pull_own, gv_own, vals, row_sum,
    hid, w, k_in, q_in, pre, rate_in, cot_t, cot,
    y_sem, z_sem, rest_sem, ring_sem, d_sem, x_sem, in_sem, h_sem, zg_sem, near_sem,
):
    z, y = lax.axis_index("z"), lax.axis_index("y")
    x, c = lax.axis_index("x"), lax.axis_index("c")
    lane = lax.broadcasted_iota(jnp.int32, (128, 128), 1)
    first_head = lane[0:1, :] < 64
    sent = []
    stack = contextlib.ExitStack()

    def phase(name):
        stack.close()
        stack.enter_context(jax.named_scope(name))

    def peer_y(o):
        return lax.rem(y + o, NY)

    def peer_z(o):
        return lax.rem(z + o, NZ)

    def peer_x(o):
        return lax.rem(x + o, NX)

    def copy(src, dst, s_sem, r_sem, **where):
        return pltpu.make_async_remote_copy(
            src_ref=src, dst_ref=dst, send_sem=s_sem, recv_sem=r_sem, device_id=where, device_id_type=MESH
        )

    def send(src, dst, s_sem, r_sem, **where):
        copy(src, dst, s_sem, r_sem, **where).start()

    def arrived(dst, r_sem):
        copy(dst, dst, r_sem, r_sem, c=1 - c).wait_recv()

    def drain_later(like, s_sem):
        sent.append(copy(like, like, s_sem, s_sem, c=1 - c))

    def send_y(kind, src, dst):
        for o in range(1, NY):
            send(src.at[peer_y(o)], dst.at[y], y_sem.at[0, kind], y_sem.at[1, kind], y=peer_y(o))
        drain_later(dst.at[0 : NY - 1], y_sem.at[0, kind])

    def share_y(kind, src, dst):
        for o in range(1, NY):
            send(src, dst.at[y], y_sem.at[0, kind], y_sem.at[1, kind], y=peer_y(o))
        drain_later(dst.at[0 : NY - 1], y_sem.at[0, kind])

    def wait_y(kind, dst):
        arrived(dst.at[0 : NY - 1], y_sem.at[1, kind])

    def send_z(kind, src, dst):
        for o in range(1, NZ):
            send(src.at[peer_z(o)], dst.at[z], z_sem.at[0, kind], z_sem.at[1, kind], z=peer_z(o))
        drain_later(dst.at[0 : NZ - 1], z_sem.at[0, kind])

    def wait_z(kind, dst):
        arrived(dst.at[0 : NZ - 1], z_sem.at[1, kind])

    phase("enter")
    loads = [
        pltpu.make_async_copy(src, dst, in_sem.at[i])
        for i, (src, dst) in enumerate(
            [(cot_at, cot_t), (q_at, q_in), (pre_at, pre), (rate_at, rate_in), (k_at, k_in), (hid_at, hid), (w_at, w)]
        )
    ]
    for made in loads:
        made.start()

    barrier = pltpu.get_barrier_semaphore()
    for o in range(1, NY):
        pl.semaphore_signal(barrier, inc=1, device_id={"y": peer_y(o)}, device_id_type=MESH)
    for o in (1, NZ - 1):
        pl.semaphore_signal(barrier, inc=1, device_id={"z": peer_z(o)}, device_id_type=MESH)
    for o in range(1, NX):
        pl.semaphore_signal(barrier, inc=1, device_id={"x": peer_x(o)}, device_id_type=MESH)
    pl.semaphore_signal(barrier, inc=1, device_id={"c": 1 - c}, device_id_type=MESH)

    phase("widen")
    loads[0].wait()
    for pair in range(PAIRS):
        cot_s[pair] = cot_t[cols(pair), :].astype(F32)
    cot_r[y] = cot_s[...]
    loads[1].wait()
    q = q_in[...]
    q_s[...] = q.astype(F32)
    q_r[y] = q_s[...]
    phase("barrier")
    pl.semaphore_wait(barrier, NY + NX + 1)

    def tell_z(turn):
        for o in (1, NZ - 1):
            pl.semaphore_signal(near_sem.at[turn], inc=1, device_id={"z": peer_z(o)}, device_id_type=MESH)

    def heard_z(turn):
        pl.semaphore_wait(near_sem.at[turn], 2)

    tell_z(0)
    share_y(3, q_s, q_r)
    for o in range(1, NY):
        send(cot_s.at[peer_y(o)], cot_r.at[y, peer_y(o)], y_sem.at[0, 0], y_sem.at[1, 0], y=peer_y(o))
    drain_later(cot_r.at[0, 0 : NY - 1], y_sem.at[0, 0])

    phase("decay")
    loads[2].wait()
    loads[3].wait()
    pre_v = pre[...]
    square = lax.broadcasted_iota(jnp.int32, (8, 8), 0) == lax.broadcasted_iota(jnp.int32, (8, 8), 1)
    rate = jnp.sum(jnp.where(square, jnp.broadcast_to(rate_in[...], (8, 8)), 0.0), axis=1, keepdims=True)
    soft = jnp.maximum(pre_v, 0.0) + jnp.log1p(jnp.exp(-jnp.abs(pre_v)))
    cum = -rate * soft
    lane8 = lane[0:8, :]
    for shift in (1, 2, 4, 8, 16, 32, 64):
        cum = cum + jnp.where(lane8 >= shift, pltpu.roll(cum, shift, 1), 0.0)
    cum_s[...] = cum
    cum_r[y] = cum
    total = jnp.broadcast_to(cum[:, 127:128], (8, 128))
    factor = jnp.exp(total)
    cum_t = cum.T
    from_start = jnp.exp(cum)
    from_start_t = from_start.T
    to_end_t = jnp.exp(total - cum).T

    def spread(columns, pair):
        return jnp.where(first_head, columns[:, 2 * pair : 2 * pair + 1], columns[:, 2 * pair + 1 : 2 * pair + 2])

    def row_of(gains, pair):
        return jnp.where(first_head, gains[2 * pair : 2 * pair + 1, :], gains[2 * pair + 1 : 2 * pair + 2, :])

    share_y(6, cum_s, cum_r)
    loads[4].wait()
    k = k_in[...]
    k_s[...] = k.astype(F32)
    k_r[y] = k_s[...]

    heard_z(0)
    tell_z(1)
    phase("hidden")
    loads[5].wait()
    for block in range(16):
        turned = hid[:, cols(block)].astype(F32).T
        hid_t[block // 2, 2 * (block % 2) : 2 * (block % 2) + 2] = turned.reshape(2, 64, 128)
    seat = 2 * x + c
    for o in range(1, NY):
        send(hid_t.at[seat, peer_y(o)], hid_p.at[y], y_sem.at[0, 2], y_sem.at[1, 2], y=peer_y(o))
    drain_later(hid_p.at[0 : NY - 1], y_sem.at[0, 2])
    hid_p[y] = hid_t[seat, y]
    phase("values")
    loads[6].wait()
    k_t = k_s[...].T.astype(BF16)
    for half in range(2):
        span = slice(256 * half, 256 * half + 256)
        vals[:, span] = dot(hid[...], w[:, span]).astype(BF16)
    scaled = jnp.concatenate([spread(to_end_t, pair) for pair in range(PAIRS)], axis=1) * vals[...].astype(F32)
    states = dot_fine_right(k_t, scaled)
    for pair in range(PAIRS):
        ys_f[pair, 0:128, :] = states[:, cols(pair)]
        ys_f[pair, 128:136, :] = jnp.broadcast_to(row_of(factor, pair), (8, 128))
    yr_f[y] = ys_f[y]
    send_y(1, ys_f, yr_f)

    share_y(5, k_s, k_r)

    for o in range(1, PAIRS):
        for way in range(2):
            side = peer_y(1 + 2 * way)
            pair = peer_y(1 + 2 * way + o)
            send(cot_s.at[pair], cot_r.at[y, pair], rest_sem.at[2, 0], rest_sem.at[way, o - 1], y=side)
    drain_later(cot_r.at[0:2, 0 : NY - 1], rest_sem.at[2, 0])
    halves_of = (slice(0, 64), slice(64, 128))

    def pass_on(way, o):
        origin, side = peer_y(3 - 2 * way), peer_y(1 + 2 * way)
        if o > 0:
            arrived(cot_r.at[origin, peer_y(o)], rest_sem.at[way, o - 1])
        if o != (1, 3)[way]:
            half = cot_r.at[origin, peer_y(o), halves_of[way]]
            send(half, half, y_sem.at[0, 7], y_sem.at[1, 7], y=side)

    heard_z(1)
    tell_z(2)
    phase("block")
    for pair in range(PAIRS):
        cot[:, cols(pair)] = cot_t[cols(pair), :].astype(F32).T.astype(BF16)
    causal = lax.broadcasted_iota(jnp.int32, (128, 128), 0) <= lane
    blend = jnp.zeros((128, 128), F32)
    score_own = dot(k, q, ((1,), (1,)))
    for pair in range(PAIRS):
        cot_pair, val_pair = cot[:, cols(pair)], vals[:, cols(pair)]
        for side in range(2):
            head = 2 * pair + side
            mine = first_head if side == 0 else jnp.logical_not(first_head)
            across = jnp.where(causal, cum[head : head + 1, :] - cum_t[:, head : head + 1], 0.0)
            damping = jnp.where(causal, jnp.exp(across), 0.0)
            cot_head = jnp.where(mine, cot_pair.astype(F32), 0.0).astype(BF16)
            moved = dot(val_pair, cot_head, ((1,), (1,))) * damping
            blend = blend + moved
            row_sum[head : head + 1, :] = jnp.sum(moved * score_own, axis=0, keepdims=True)

    upper = lax.broadcasted_iota(jnp.int32, (128, 128), 0) < 64

    def rows_of(slot, block):
        pair = peer_y(slot)
        return [cum_r[block, pl.ds(2 * pair + side, 1), :] for side in range(2)]

    def block_pull(slot, block):
        first, second = rows_of(slot, block)
        growth = jnp.where(upper, jnp.exp(first), jnp.exp(second))
        pulls[slot, block] = dot_fine_right(q_t[block], growth * cot_r[block, peer_y(slot)], ((1,), (1,)))
        gain = jnp.where(first_head, jnp.exp(first[:, 127:128]), jnp.exp(second[:, 127:128]))
        gains[slot, block] = jnp.broadcast_to(gain, (8, 128))

    def plane_chain(slot):
        after = gain = None
        for block in range(NY - 1, -1, -1):
            suffix[slot, block] = jnp.zeros((128, 128), F32) if after is None else after
            reach[slot, block] = jnp.ones((8, 128), F32) if gain is None else gain
            here = gains[slot, block]
            after = pulls[slot, block] if after is None else pulls[slot, block] + here[0:1, :] * after
            gain = here if gain is None else gain * here
        return after, gain

    def block_values(slot, block):
        rows = rows_of(slot, block)
        tall = [jnp.broadcast_to(row, (128, 128)).T for row in rows]
        near_end[slot, block] = jnp.exp(
            jnp.where(first_head, rows[0][:, 127:128] - tall[0], rows[1][:, 127:128] - tall[1])
        )
        weights = []
        for side in range(2):
            across = jnp.where(causal, rows[side] - tall[side], 0.0)
            weights.append(score[block] * jnp.where(causal, jnp.exp(across), 0.0))
        cot_pair = cot_r[block, peer_y(slot)]
        cots = jnp.concatenate([jnp.where(upper, cot_pair, 0.0), jnp.where(upper, 0.0, cot_pair)], axis=1)
        gv_r[slot, block] = dot_fine_left(jnp.concatenate(weights, axis=1), cots.astype(BF16), ((1,), (1,)))

    def scan_plane(got, kept, z_send, reverse):
        state, gain = None, None
        order = range(NY - 1, -1, -1) if reverse else range(NY)
        for block in order:
            value, here = got[block, 0:128, :], got[block, 128:129, :]
            if state is None:
                kept[block] = jnp.zeros((128, 128), F32)
                state, gain = value, here
            else:
                kept[block] = state
                state, gain = here * state + value, gain * here
        for row in range(NZ):
            z_send[row, 0:ROWS, :] = state[row * ROWS : row * ROWS + ROWS, :]
            z_send[row, ROWS : ROWS + 8, :] = jnp.broadcast_to(gain, (8, 128))

    def scan_z(got, back, reverse):
        state = None
        for plane in range(NZ - 1, -1, -1) if reverse else range(NZ):
            value, here = got[plane, 0:ROWS, :], got[plane, ROWS : ROWS + 1, :]
            if state is None:
                back[plane] = jnp.zeros((ROWS, 128), F32)
                state = value
            else:
                back[plane] = state
                state = here * state + value

    def finish_plane(got, kept, plane_in, reverse):
        incoming = plane_in[...].reshape(STATE, 128)
        gain = None
        for block in range(NY - 1, -1, -1) if reverse else range(NY):
            kept[block] = kept[block] + (incoming if gain is None else gain * incoming)
            here = got[block, 128:129, :]
            gain = here if gain is None else gain * here

    phase("first")
    wait_y(6, cum_r)
    wait_y(3, q_r)
    arrived(cot_r.at[0, 0 : NY - 1], y_sem.at[1, 0])
    phase("pulls0")
    for block in range(NY):
        q_t[block] = q_r[block].T.astype(BF16)
    for block in range(NY):
        block_pull(0, block)
    state, gain = plane_chain(0)
    for row in range(NZ):
        zs_b[row, 0:ROWS, :] = state[row * ROWS : row * ROWS + ROWS, :]
        zs_b[row, ROWS : ROWS + 8, :] = gain
    zr_b[z] = zs_b[z]
    heard_z(2)
    send_z(0, zs_b, zr_b)
    pass_on(0, 0)
    pass_on(1, 0)
    for slot in range(1, PAIRS):
        block_pull(slot, y)

    phase("hidden_x")
    wait_y(2, hid_p)
    for o in range(1, NX):
        send(hid_p, hid_x.at[x], h_sem.at[0], h_sem.at[1], x=peer_x(o))
    drain_later(hid_x.at[0 : NX - 1], h_sem.at[0])
    hid_x[x] = hid_p[...]

    phase("scan_y_f")
    wait_y(1, yr_f)
    scan_plane(yr_f, ybs_f, zs_f, False)
    zr_f[z] = zs_f[z]
    send_z(1, zs_f, zr_f)

    phase("scan_z_b")
    wait_z(0, zr_b)
    scan_z(zr_b, zbs_b, True)
    zbr_b[z] = zbs_b[z]
    send_z(2, zbs_b, zbr_b)

    phase("hidden_c")
    arrived(hid_x.at[0 : NX - 1], h_sem.at[1])
    send(hid_x, hid_c, d_sem.at[0, 1], d_sem.at[1, 1], c=1 - c)
    drain_later(hid_x, d_sem.at[0, 1])

    phase("keys_far")
    wait_y(5, k_r)
    phase("values0")
    for block in range(NY):
        score[block] = dot(k_r[block].astype(BF16), q_r[block].astype(BF16), ((1,), (1,)))
    for block in range(NY):
        block_values(0, block)
    for slot in range(1, PAIRS):
        block_values(slot, y)

    phase("pass1")
    pass_on(0, 1)
    pass_on(1, 1)
    phase("scan_z_f")
    wait_z(1, zr_f)
    scan_z(zr_f, zbs_f, False)
    zbr_f[z] = zbs_f[z]
    send_z(3, zbs_f, zbr_f)

    phase("pass2")
    pass_on(0, 2)
    pass_on(1, 2)

    phase("wait_zg")
    wait_z(2, zbr_b)
    zg_s[...] = zbr_b[...].reshape(STATE, 128)
    zg_r[0] = zg_s[...]
    for o in range(1, NY):
        send(zg_s, zg_r.at[NY - o], zg_sem.at[0], zg_sem.at[1], y=peer_y(o))
    drain_later(zg_r.at[0 : NY - 1], zg_sem.at[0])

    phase("hid_all")
    arrived(hid_c, d_sem.at[1, 1])
    for across_x in range(NX):
        for block in range(NY):
            hid_all[across_x, c, :, cols(block)] = hid_x[across_x, block].astype(BF16)
            hid_all[across_x, 1 - c, :, cols(block)] = hid_c[across_x, block].astype(BF16)

    spans = (slice(0, 32), slice(32, 64))

    def ahead(way, o):
        return peer_z(o) if way == 0 else peer_z(NZ - o)

    def z_first(slot):
        sems = (ring_sem.at[2, 0], ring_sem.at[0, slot])
        for way in range(2):
            src = part.at[slot, ahead(way, 4), spans[way]]
            send(src, far_r.at[way, slot], *sems, z=ahead(way, 2))
        for way in range(2):
            send(part.at[slot, ahead(way, 3)], near_r.at[way, slot], *sems, z=ahead(way, 1))

    def z_direct(slot):
        for way in range(2):
            near = ahead(way, 1)
            send(part.at[slot, near], ring_r.at[0, way, slot], ring_sem.at[2, 0], ring_sem.at[1, slot], z=near)

    def z_second(slot):
        phase(f"second{slot}")
        arrived(part.at[slot, 0:3], ring_sem.at[0, slot])
        for way in range(2):
            far = ahead(way, 2)
            mine = part[slot, far] + near_r[way, slot]
            extra = mine[spans[way]] + far_r[way, slot]
            ring_s[way, slot, spans[way]] = extra
            ring_s[way, slot, spans[1 - way]] = mine[spans[1 - way]]
            send(ring_s.at[way, slot], ring_r.at[1, way, slot], ring_sem.at[2, 0], ring_sem.at[1, slot], z=far)

    def z_last(slot):
        phase(f"last{slot}")
        arrived(part.at[slot, 0:4], ring_sem.at[1, slot])
        gw_out[slot] = (
            part[slot, z] + ring_r[0, 0, slot] + ring_r[0, 1, slot] + ring_r[1, 0, slot] + ring_r[1, 1, slot]
        )

    def own_values(slot):
        pair = peer_y(slot)
        pull_now = suffix[slot, y] + reach[slot, y, 0:1, :] * zg_r[slot]
        pull_own[pair] = pull_now
        gv_own[pair] = gv_r[slot, y] + near_end[slot, y] * dot_fine_right(k, pull_now)

    def weight(slot):
        phase(f"weight{slot}")
        incoming = zg_r[slot]
        for block in range(NY):
            pull_now = suffix[slot, block] + reach[slot, block, 0:1, :] * incoming
            from_state = dot_fine_right(k_r[block].astype(BF16), pull_now)
            gv_r[slot, block] = gv_r[slot, block] + near_end[slot, block] * from_state
        gathered = gv_r[slot].reshape(512, 128).astype(BF16)
        part[slot] = dot(hid_all[...].reshape(512, 512), gathered).reshape(NZ, 64, 128)
        z_first(slot)

    own_values(0)
    weight(0)
    z_direct(0)

    phase("pass3")
    pass_on(0, 3)
    pass_on(1, 3)
    drain_later(cot_r.at[0, 0 : NY - 1], y_sem.at[0, 7])
    phase("values_near")
    for slot in range(1, PAIRS):
        for o in (1, 3):
            block_pull(slot, peer_y(o))
            block_values(slot, peer_y(o))

    phase("wait_opposite")
    arrived(cot_r.at[0, 0 : NY - 1], y_sem.at[1, 7])
    phase("values_far")
    for slot in range(1, PAIRS):
        block_pull(slot, peer_y(2))
        block_values(slot, peer_y(2))
        plane_chain(slot)
    phase("back_y_f")
    wait_z(3, zbr_f)
    finish_plane(yr_f, ybs_f, zbr_f, False)
    ybr_f[y] = ybs_f[y]
    send_y(4, ybs_f, ybr_f)

    phase("wait_zg_all")
    arrived(zg_r.at[0 : NY - 1], zg_sem.at[1])
    phase("own_values")
    for slot in range(1, PAIRS):
        own_values(slot)
    weight(1)
    z_second(0)
    weight(2)
    phase("grad_h")
    grad_v = jnp.concatenate([gv_own[pair].astype(BF16) for pair in range(PAIRS)], axis=1)
    for part_now in range(4):
        span = slice(512 * part_now, 512 * part_now + 512)
        gh_s[:, :, :, span] = dot(grad_v, w[span, :], ((1,), (1,))).reshape(NX, 2, 16, 512)
    send(gh_s.at[:, 1 - c], gh_r, d_sem.at[0, 0], d_sem.at[1, 0], c=1 - c)
    drain_later(gh_r, d_sem.at[0, 0])

    weight(3)
    for slot in range(1, PAIRS):
        z_direct(slot)

    phase("chip_pair")
    arrived(gh_r, d_sem.at[1, 0])
    gx_s[...] = gh_s[:, c] + gh_r[...]
    for o in (2, 1, 3):
        send(gx_s.at[peer_x(o)], gx_r.at[x], x_sem.at[0], x_sem.at[1], x=peer_x(o))
    drain_later(gx_r.at[0 : NX - 1], x_sem.at[0])
    gx_r[x] = gx_s[x]

    z_second(1)
    phase("grad_k")
    gk = dot_fine_left(blend, q)
    gq = dot_fine_left(blend.T, k)
    wide = lax.broadcasted_iota(jnp.int32, (8, 512), 1)
    chooser = jnp.where(lax.broadcasted_iota(jnp.int32, (8, 512), 0) == wide // 64, 1.0, 0.0)
    pull = jnp.concatenate([pull_own[pair] for pair in range(PAIRS)], axis=1)
    val_f = vals[...].astype(F32)
    val_scaled = jnp.concatenate([spread(to_end_t, pair) for pair in range(PAIRS)], axis=1) * val_f
    gk = gk + dot_fine(val_scaled, pull, ((1,), (1,)))
    whole = jnp.sum(val_scaled * dot_fine_right(k, pull), axis=0, keepdims=True)
    used = val_f * jnp.concatenate([gv_own[pair] for pair in range(PAIRS)], axis=1)
    gk_out[...] = gk.astype(BF16)

    z_second(2)
    z_second(3)
    z_last(0)

    phase("wait_carry")
    wait_y(4, ybr_f)
    phase("grad_q")
    carry = jnp.concatenate([ybr_f[pair] for pair in range(PAIRS)], axis=1)
    cot_scaled = jnp.concatenate([spread(from_start_t, pair) for pair in range(PAIRS)], axis=1) * cot[...].astype(F32)
    gq = gq + dot_fine(cot_scaled, carry, ((1,), (1,)))
    change = cot_scaled * dot_fine_right(q, carry) - used
    high, low = halves(change)
    lowest = (change - high.astype(F32) - low.astype(F32)).astype(BF16)
    picked = chooser.astype(BF16)
    gap = row_sum[...]
    for level in (high, low, lowest):
        gap = gap + dot(picked, level, ((1,), (1,)))
    factors = jnp.concatenate([row_of(factor, pair) for pair in range(PAIRS)], axis=1)
    whole = whole + factors * jnp.sum(carry * pull, axis=0, keepdims=True)
    shared = jnp.sum(chooser * whole, axis=1, keepdims=True)
    for shift in (1, 2, 4, 8, 16, 32, 64):
        gap = gap + jnp.where(lane8 < 128 - shift, pltpu.roll(gap, 128 - shift, 1), 0.0)
    gd_out[...] = (gap + shared) * (-rate / (1.0 + jnp.exp(-pre_v)))
    gq_out[...] = gq.astype(BF16)

    phase("out_h")
    arrived(gx_r.at[0 : NX - 1], x_sem.at[1])
    gh_out[...] = (gx_r[0] + gx_r[1] + gx_r[2] + gx_r[3]).astype(BF16)

    z_last(1)
    z_last(2)
    z_last(3)
    drain_later(part.at[0:PAIRS, 0 : NZ - 1], ring_sem.at[2, 0])

    phase("drain")
    for made in sent:
        made.wait_send()
    stack.close()


def store_all(*refs):
    y = lax.axis_index("y")
    sems = refs[10]
    copies = [pltpu.make_async_copy(refs[i], refs[5 + i], sems.at[i]) for i in range(4)]
    for slot in range(PAIRS):
        pair = lax.rem(y + slot, PAIRS)
        place = refs[9].at[:, pl.ds(pl.multiple_of(128 * pair, 128), 128)]
        copies.append(pltpu.make_async_copy(refs[4].at[slot], place, sems.at[4 + slot]))
    for made in copies:
        made.start()
    for made in copies:
        made.wait()


def local(hidden, value_weight, key_vecs, queries, decay_pre, decay_rate, cotangent):
    dma = pltpu.SemaphoreType.DMA
    f32 = lambda *shape: pltpu.VMEM(shape, F32)
    y_box, z_box = (NY, STATE + 8, 128), (NZ, ROWS + 8, 128)
    z_back, y_back = (NZ, ROWS, 128), (NY, STATE, 128)
    outs = pl.pallas_call(
        kernel,
        out_shape=(
            jax.ShapeDtypeStruct((TOK, STATE), BF16),
            jax.ShapeDtypeStruct((TOK, STATE), BF16),
            jax.ShapeDtypeStruct((HEADS, TOK), F32),
            jax.ShapeDtypeStruct((16, 2048), BF16),
            jax.ShapeDtypeStruct((PAIRS, 64, 128), F32),
        ),
        in_specs=[pl.BlockSpec(memory_space=pltpu.HBM)] * 7,
        out_specs=[pl.BlockSpec(memory_space=pltpu.VMEM)] * 5,
        scratch_shapes=[
            *[f32(*y_box)] * 2,
            *[f32(*z_box)] * 4,
            *[f32(*z_back)] * 4,
            *[f32(*y_back)] * 2,
            f32(NZ, NY, 64, TOK),
            f32(NY, 64, TOK),
            f32(NX, NY, 64, TOK),
            f32(NX, NY, 64, TOK),
            pltpu.VMEM((NX, 2, 64, 512), BF16),
            f32(PAIRS, NY, TOK, 128),
            f32(PAIRS, NZ, 64, 128),
            f32(2, PAIRS, 64, 128),
            f32(2, PAIRS, 32, 128),
            f32(2, PAIRS, 64, 128),
            f32(2, 2, PAIRS, 64, 128),
            f32(NX, 2, 16, 2048),
            f32(NX, 16, 2048),
            f32(NX, 16, 2048),
            f32(NX, 16, 2048),
            f32(STATE, 128),
            f32(NY, STATE, 128),
            f32(TOK, STATE),
            f32(NY, TOK, STATE),
            f32(TOK, STATE),
            f32(NY, TOK, STATE),
            pltpu.VMEM((NY, STATE, TOK), BF16),
            f32(PAIRS, 128, TOK),
            f32(NY, PAIRS, 128, TOK),
            f32(HEADS, TOK),
            f32(NY, HEADS, TOK),
            f32(NY, TOK, TOK),
            f32(PAIRS, NY, TOK, 128),
            f32(PAIRS, NY, STATE, 128),
            f32(PAIRS, NY, 8, 128),
            f32(PAIRS, NY, STATE, 128),
            f32(PAIRS, NY, 8, 128),
            f32(PAIRS, STATE, 128),
            f32(PAIRS, TOK, 128),
            pltpu.VMEM((TOK, 512), BF16),
            f32(HEADS, TOK),
            pltpu.VMEM((TOK, 2048), BF16),
            pltpu.VMEM((2048, 512), BF16),
            pltpu.VMEM((TOK, STATE), BF16),
            pltpu.VMEM((TOK, STATE), BF16),
            f32(HEADS, TOK),
            f32(1, HEADS),
            pltpu.VMEM((512, TOK), BF16),
            pltpu.VMEM((TOK, 512), BF16),
            dma((2, 8)),
            dma((2, 4)),
            dma((3, 3)),
            dma((3, PAIRS)),
            dma((2, 2)),
            dma((2,)),
            dma((7,)),
            dma((2,)),
            dma((2,)),
            pltpu.SemaphoreType.REGULAR((3,)),
        ],
        compiler_params=pltpu.CompilerParams(
            collective_id=0, has_side_effects=True, vmem_limit_bytes=VMEM_LIMIT
        ),
        name="mixer_backward",
    )(
        *[
            pltpu.with_memory_space_constraint(a, pltpu.HBM)
            for a in (
                hidden,
                value_weight,
                key_vecs.reshape(TOK, STATE),
                queries.reshape(TOK, STATE),
                decay_pre.T,
                decay_rate[None, :],
                cotangent.reshape(TOK, 512).T,
            )
        ]
    )
    gk, gq, gd, gh, gw = pl.pallas_call(
        store_all,
        out_shape=(
            *[jax.ShapeDtypeStruct(o.shape, o.dtype) for o in outs[:4]],
            jax.ShapeDtypeStruct((64, 512), F32),
        ),
        in_specs=[pl.BlockSpec(memory_space=pltpu.VMEM)] * 5,
        out_specs=[pl.BlockSpec(memory_space=pltpu.HBM)] * 5,
        scratch_shapes=[dma((8,))],
        compiler_params=pltpu.CompilerParams(vmem_limit_bytes=2 * 1024 * 1024),
        name="store_all",
    )(*outs)
    return gk.reshape(TOK, 1, STATE), gq.reshape(TOK, 1, STATE), gd.T, gh, gw


def solution(mesh):
    split = Mesh(mesh.devices.reshape(NZ, NY, NX, 2), ("z", "y", "x", "c"))
    placed = (
        P(SP, None),
        P(None, TP),
        P(SP, TP, None),
        P(SP, TP, None),
        P(SP, TP),
        P(TP),
        P(SP, TP, None),
    )
    return jax.shard_map(
        local,
        mesh=split,
        in_specs=placed,
        out_specs=(P(SP, TP, None), P(SP, TP, None), P(SP, TP), P(SP + TP, None), P(SP, TP)),
        check_vma=False,
    )
```

```python
import contextlib

import jax
import jax.numpy as jnp
from jax import lax
from jax.experimental import pallas as pl
from jax.experimental.pallas import tpu as pltpu
from jax.sharding import Mesh
from jax.sharding import PartitionSpec as P

F32, BF16 = jnp.float32, jnp.bfloat16
MESH = pl.DeviceIdType.MESH
SP, TP = ("z", "y"), ("x", "c")
NZ, NY, NX = 8, 4, 4
TOK, STATE, PAIRS, HEADS = 128, 128, 4, 8
ROWS = STATE // NZ
VMEM_LIMIT = 48 * 1024 * 1024


def dot(a, b, dims=((1,), (0,))):
    return lax.dot_general(a, b, (dims, ((), ())), preferred_element_type=F32)


def halves(a):
    high = a.astype(BF16)
    return high, (a - high.astype(F32)).astype(BF16)


def dot_fine_right(a, b, dims=((1,), (0,))):
    high, low = halves(b)
    return dot(a, high, dims) + dot(a, low, dims)


def dot_fine_left(a, b, dims=((1,), (0,))):
    high, low = halves(a)
    return dot(high, b, dims) + dot(low, b, dims)


def dot_fine(a, b, dims=((1,), (0,))):
    a_high, a_low = halves(a)
    b_high, b_low = halves(b)
    return dot(a_high, b_high, dims) + dot(a_high, b_low, dims) + dot(a_low, b_high, dims)


def cols(pair):
    return slice(128 * pair, 128 * pair + 128)


def kernel(
    hid_at, w_at, k_at, q_at, pre_at, rate_at, cot_at,
    gk_out, gq_out, gd_out, gh_out, gw_out,
    ys_f, yr_f, zs_b, zr_b, zs_f, zr_f,
    zbs_b, zbr_b, zbs_f, zbr_f, ybs_f, ybr_f,
    hid_t, hid_p, hid_x, hid_c, hid_all, gv_r, part, near_r, far_r, ring_s, ring_r,
    gh_s, gh_r, gx_s, gx_r, zg_s, zg_r, k_s, k_r, q_s, q_r, q_t, cot_s, cot_r, cum_s, cum_r,
    score, near_end, pulls, gains, suffix, reach, pull_own, gv_own, vals, row_sum,
    hid, w, k_in, q_in, pre, rate_in, cot_t, cot,
    y_sem, z_sem, rest_sem, ring_sem, d_sem, x_sem, in_sem, h_sem, zg_sem, near_sem,
):
    z, y = lax.axis_index("z"), lax.axis_index("y")
    x, c = lax.axis_index("x"), lax.axis_index("c")
    lane = lax.broadcasted_iota(jnp.int32, (128, 128), 1)
    first_head = lane[0:1, :] < 64
    sent = []
    stack = contextlib.ExitStack()

    def phase(name):
        stack.close()
        stack.enter_context(jax.named_scope(name))

    def peer_y(o):
        return lax.rem(y + o, NY)

    def peer_z(o):
        return lax.rem(z + o, NZ)

    def peer_x(o):
        return lax.rem(x + o, NX)

    def copy(src, dst, s_sem, r_sem, **where):
        return pltpu.make_async_remote_copy(
            src_ref=src, dst_ref=dst, send_sem=s_sem, recv_sem=r_sem, device_id=where, device_id_type=MESH
        )

    def send(src, dst, s_sem, r_sem, **where):
        copy(src, dst, s_sem, r_sem, **where).start()

    def arrived(dst, r_sem):
        copy(dst, dst, r_sem, r_sem, c=1 - c).wait_recv()

    def drain_later(like, s_sem):
        sent.append(copy(like, like, s_sem, s_sem, c=1 - c))

    def send_y(kind, src, dst):
        for o in range(1, NY):
            send(src.at[peer_y(o)], dst.at[y], y_sem.at[0, kind], y_sem.at[1, kind], y=peer_y(o))
        drain_later(dst.at[0 : NY - 1], y_sem.at[0, kind])

    def share_y(kind, src, dst):
        for o in range(1, NY):
            send(src, dst.at[y], y_sem.at[0, kind], y_sem.at[1, kind], y=peer_y(o))
        drain_later(dst.at[0 : NY - 1], y_sem.at[0, kind])

    def wait_y(kind, dst):
        arrived(dst.at[0 : NY - 1], y_sem.at[1, kind])

    def send_z(kind, src, dst):
        for o in range(1, NZ):
            send(src.at[peer_z(o)], dst.at[z], z_sem.at[0, kind], z_sem.at[1, kind], z=peer_z(o))
        drain_later(dst.at[0 : NZ - 1], z_sem.at[0, kind])

    def wait_z(kind, dst):
        arrived(dst.at[0 : NZ - 1], z_sem.at[1, kind])

    phase("enter")
    loads = [
        pltpu.make_async_copy(src, dst, in_sem.at[i])
        for i, (src, dst) in enumerate(
            [(cot_at, cot_t), (q_at, q_in), (pre_at, pre), (rate_at, rate_in), (k_at, k_in), (hid_at, hid), (w_at, w)]
        )
    ]
    for made in loads:
        made.start()

    barrier = pltpu.get_barrier_semaphore()
    for o in range(1, NY):
        pl.semaphore_signal(barrier, inc=1, device_id={"y": peer_y(o)}, device_id_type=MESH)
    for o in (1, NZ - 1):
        pl.semaphore_signal(barrier, inc=1, device_id={"z": peer_z(o)}, device_id_type=MESH)
    for o in range(1, NX):
        pl.semaphore_signal(barrier, inc=1, device_id={"x": peer_x(o)}, device_id_type=MESH)
    pl.semaphore_signal(barrier, inc=1, device_id={"c": 1 - c}, device_id_type=MESH)

    phase("widen")
    loads[0].wait()
    for pair in range(PAIRS):
        cot_s[pair] = cot_t[cols(pair), :].astype(F32)
    cot_r[y] = cot_s[...]
    loads[1].wait()
    q = q_in[...]
    q_s[...] = q.astype(F32)
    q_r[y] = q_s[...]
    phase("barrier")
    pl.semaphore_wait(barrier, NY + NX + 1)

    def tell_z(turn):
        for o in (1, NZ - 1):
            pl.semaphore_signal(near_sem.at[turn], inc=1, device_id={"z": peer_z(o)}, device_id_type=MESH)

    def heard_z(turn):
        pl.semaphore_wait(near_sem.at[turn], 2)

    tell_z(0)
    share_y(3, q_s, q_r)
    for o in range(1, NY):
        send(cot_s.at[peer_y(o)], cot_r.at[y, peer_y(o)], y_sem.at[0, 0], y_sem.at[1, 0], y=peer_y(o))
    drain_later(cot_r.at[0, 0 : NY - 1], y_sem.at[0, 0])

    phase("decay")
    loads[2].wait()
    loads[3].wait()
    pre_v = pre[...]
    square = lax.broadcasted_iota(jnp.int32, (8, 8), 0) == lax.broadcasted_iota(jnp.int32, (8, 8), 1)
    rate = jnp.sum(jnp.where(square, jnp.broadcast_to(rate_in[...], (8, 8)), 0.0), axis=1, keepdims=True)
    soft = jnp.maximum(pre_v, 0.0) + jnp.log1p(jnp.exp(-jnp.abs(pre_v)))
    cum = -rate * soft
    lane8 = lane[0:8, :]
    for shift in (1, 2, 4, 8, 16, 32, 64):
        cum = cum + jnp.where(lane8 >= shift, pltpu.roll(cum, shift, 1), 0.0)
    cum_s[...] = cum
    cum_r[y] = cum
    total = jnp.broadcast_to(cum[:, 127:128], (8, 128))
    factor = jnp.exp(total)
    cum_t = cum.T
    from_start = jnp.exp(cum)
    from_start_t = from_start.T
    to_end_t = jnp.exp(total - cum).T

    def spread(columns, pair):
        return jnp.where(first_head, columns[:, 2 * pair : 2 * pair + 1], columns[:, 2 * pair + 1 : 2 * pair + 2])

    def row_of(gains, pair):
        return jnp.where(first_head, gains[2 * pair : 2 * pair + 1, :], gains[2 * pair + 1 : 2 * pair + 2, :])

    share_y(6, cum_s, cum_r)
    loads[4].wait()
    k = k_in[...]
    k_s[...] = k.astype(F32)
    k_r[y] = k_s[...]

    heard_z(0)
    tell_z(1)
    phase("hidden")
    loads[5].wait()
    for block in range(16):
        turned = hid[:, cols(block)].astype(F32).T
        hid_t[block // 2, 2 * (block % 2) : 2 * (block % 2) + 2] = turned.reshape(2, 64, 128)
    seat = 2 * x + c
    for o in range(1, NY):
        send(hid_t.at[seat, peer_y(o)], hid_p.at[y], y_sem.at[0, 2], y_sem.at[1, 2], y=peer_y(o))
    drain_later(hid_p.at[0 : NY - 1], y_sem.at[0, 2])
    hid_p[y] = hid_t[seat, y]
    phase("values")
    loads[6].wait()
    k_t = k_s[...].T.astype(BF16)
    for half in range(2):
        span = slice(256 * half, 256 * half + 256)
        vals[:, span] = dot(hid[...], w[:, span]).astype(BF16)
    scaled = jnp.concatenate([spread(to_end_t, pair) for pair in range(PAIRS)], axis=1) * vals[...].astype(F32)
    states = dot_fine_right(k_t, scaled)
    for pair in range(PAIRS):
        ys_f[pair] = states[:, cols(pair)]
    yr_f[y] = ys_f[y]
    send_y(1, ys_f, yr_f)

    share_y(5, k_s, k_r)

    for o in range(1, PAIRS):
        for way in range(2):
            side = peer_y(1 + 2 * way)
            pair = peer_y(1 + 2 * way + o)
            send(cot_s.at[pair], cot_r.at[y, pair], rest_sem.at[2, 0], rest_sem.at[way, o - 1], y=side)
    drain_later(cot_r.at[0:2, 0 : NY - 1], rest_sem.at[2, 0])
    halves_of = (slice(0, 64), slice(64, 128))

    def pass_on(way, o):
        origin, side = peer_y(3 - 2 * way), peer_y(1 + 2 * way)
        if o > 0:
            arrived(cot_r.at[origin, peer_y(o)], rest_sem.at[way, o - 1])
        if o != (1, 3)[way]:
            half = cot_r.at[origin, peer_y(o), halves_of[way]]
            send(half, half, y_sem.at[0, 7], y_sem.at[1, 7], y=side)

    heard_z(1)
    tell_z(2)
    phase("block")
    for pair in range(PAIRS):
        cot[:, cols(pair)] = cot_t[cols(pair), :].astype(F32).T.astype(BF16)
    causal = lax.broadcasted_iota(jnp.int32, (128, 128), 0) <= lane
    blend = jnp.zeros((128, 128), F32)
    score_own = dot(k, q, ((1,), (1,)))
    for pair in range(PAIRS):
        cot_pair, val_pair = cot[:, cols(pair)], vals[:, cols(pair)]
        for side in range(2):
            head = 2 * pair + side
            mine = first_head if side == 0 else jnp.logical_not(first_head)
            across = jnp.where(causal, cum[head : head + 1, :] - cum_t[:, head : head + 1], 0.0)
            damping = jnp.where(causal, jnp.exp(across), 0.0)
            cot_head = jnp.where(mine, cot_pair.astype(F32), 0.0).astype(BF16)
            moved = dot(val_pair, cot_head, ((1,), (1,))) * damping
            blend = blend + moved
            row_sum[head : head + 1, :] = jnp.sum(moved * score_own, axis=0, keepdims=True)

    upper = lax.broadcasted_iota(jnp.int32, (128, 128), 0) < 64

    def rows_of(slot, block):
        pair = peer_y(slot)
        return [cum_r[block, pl.ds(2 * pair + side, 1), :] for side in range(2)]

    def block_pull(slot, block):
        first, second = rows_of(slot, block)
        growth = jnp.where(upper, jnp.exp(first), jnp.exp(second))
        pulls[slot, block] = dot_fine_right(q_t[block], growth * cot_r[block, peer_y(slot)], ((1,), (1,)))
        gain = jnp.where(first_head, jnp.exp(first[:, 127:128]), jnp.exp(second[:, 127:128]))
        gains[slot, block] = jnp.broadcast_to(gain, (8, 128))

    def plane_chain(slot):
        after = gain = None
        for block in range(NY - 1, -1, -1):
            suffix[slot, block] = jnp.zeros((128, 128), F32) if after is None else after
            reach[slot, block] = jnp.ones((8, 128), F32) if gain is None else gain
            here = gains[slot, block]
            after = pulls[slot, block] if after is None else pulls[slot, block] + here[0:1, :] * after
            gain = here if gain is None else gain * here
        return after, gain

    def block_values(slot, block):
        rows = rows_of(slot, block)
        tall = [jnp.broadcast_to(row, (128, 128)).T for row in rows]
        near_end[slot, block] = jnp.exp(
            jnp.where(first_head, rows[0][:, 127:128] - tall[0], rows[1][:, 127:128] - tall[1])
        )
        weights = []
        for side in range(2):
            across = jnp.where(causal, rows[side] - tall[side], 0.0)
            weights.append(score[block] * jnp.where(causal, jnp.exp(across), 0.0))
        cot_pair = cot_r[block, peer_y(slot)]
        cots = jnp.concatenate([jnp.where(upper, cot_pair, 0.0), jnp.where(upper, 0.0, cot_pair)], axis=1)
        gv_r[slot, block] = dot_fine_left(jnp.concatenate(weights, axis=1), cots.astype(BF16), ((1,), (1,)))

    def scan_plane(got, kept, z_send, reverse):
        state, gain = None, None
        order = range(NY - 1, -1, -1) if reverse else range(NY)
        for block in order:
            value, here = got[block], gains[0, block, 0:1, :]
            if state is None:
                kept[block] = jnp.zeros((128, 128), F32)
                state, gain = value, here
            else:
                kept[block] = state
                state, gain = here * state + value, gain * here
        for row in range(NZ):
            z_send[row, 0:ROWS, :] = state[row * ROWS : row * ROWS + ROWS, :]
            z_send[row, ROWS : ROWS + 8, :] = jnp.broadcast_to(gain, (8, 128))

    def scan_z(got, back, reverse):
        state = None
        for plane in range(NZ - 1, -1, -1) if reverse else range(NZ):
            value, here = got[plane, 0:ROWS, :], got[plane, ROWS : ROWS + 1, :]
            if state is None:
                back[plane] = jnp.zeros((ROWS, 128), F32)
                state = value
            else:
                back[plane] = state
                state = here * state + value

    def finish_plane(got, kept, plane_in, reverse):
        incoming = plane_in[...].reshape(STATE, 128)
        gain = None
        for block in range(NY - 1, -1, -1) if reverse else range(NY):
            kept[block] = kept[block] + (incoming if gain is None else gain * incoming)
            here = gains[0, block, 0:1, :]
            gain = here if gain is None else gain * here

    phase("first")
    wait_y(6, cum_r)
    wait_y(3, q_r)
    arrived(cot_r.at[0, 0 : NY - 1], y_sem.at[1, 0])
    phase("pulls0")
    for block in range(NY):
        q_t[block] = q_r[block].T.astype(BF16)
    for block in range(NY):
        block_pull(0, block)
    state, gain = plane_chain(0)
    for row in range(NZ):
        zs_b[row, 0:ROWS, :] = state[row * ROWS : row * ROWS + ROWS, :]
        zs_b[row, ROWS : ROWS + 8, :] = gain
    zr_b[z] = zs_b[z]
    heard_z(2)
    send_z(0, zs_b, zr_b)
    pass_on(0, 0)
    pass_on(1, 0)
    for slot in range(1, PAIRS):
        block_pull(slot, y)

    phase("hidden_x")
    wait_y(2, hid_p)
    for o in range(1, NX):
        send(hid_p, hid_x.at[x], h_sem.at[0], h_sem.at[1], x=peer_x(o))
    drain_later(hid_x.at[0 : NX - 1], h_sem.at[0])
    hid_x[x] = hid_p[...]

    phase("scan_y_f")
    wait_y(1, yr_f)
    scan_plane(yr_f, ybs_f, zs_f, False)
    zr_f[z] = zs_f[z]
    send_z(1, zs_f, zr_f)

    phase("scan_z_b")
    wait_z(0, zr_b)
    scan_z(zr_b, zbs_b, True)
    zbr_b[z] = zbs_b[z]
    send_z(2, zbs_b, zbr_b)

    phase("hidden_c")
    arrived(hid_x.at[0 : NX - 1], h_sem.at[1])
    send(hid_x, hid_c, d_sem.at[0, 1], d_sem.at[1, 1], c=1 - c)
    drain_later(hid_x, d_sem.at[0, 1])

    phase("keys_far")
    wait_y(5, k_r)
    phase("values0")
    for block in range(NY):
        score[block] = dot(k_r[block].astype(BF16), q_r[block].astype(BF16), ((1,), (1,)))
    for block in range(NY):
        block_values(0, block)
    for slot in range(1, PAIRS):
        block_values(slot, y)

    phase("pass1")
    pass_on(0, 1)
    pass_on(1, 1)
    phase("scan_z_f")
    wait_z(1, zr_f)
    scan_z(zr_f, zbs_f, False)
    zbr_f[z] = zbs_f[z]
    send_z(3, zbs_f, zbr_f)

    phase("pass2")
    pass_on(0, 2)
    pass_on(1, 2)

    phase("wait_zg")
    wait_z(2, zbr_b)
    zg_s[...] = zbr_b[...].reshape(STATE, 128)
    zg_r[0] = zg_s[...]
    for o in range(1, NY):
        send(zg_s, zg_r.at[NY - o], zg_sem.at[0], zg_sem.at[1], y=peer_y(o))
    drain_later(zg_r.at[0 : NY - 1], zg_sem.at[0])

    phase("hid_all")
    arrived(hid_c, d_sem.at[1, 1])
    for across_x in range(NX):
        for block in range(NY):
            hid_all[across_x, c, :, cols(block)] = hid_x[across_x, block].astype(BF16)
            hid_all[across_x, 1 - c, :, cols(block)] = hid_c[across_x, block].astype(BF16)

    spans = (slice(0, 32), slice(32, 64))

    def ahead(way, o):
        return peer_z(o) if way == 0 else peer_z(NZ - o)

    def z_first(slot):
        sems = (ring_sem.at[2, 0], ring_sem.at[0, slot])
        for way in range(2):
            src = part.at[slot, ahead(way, 4), spans[way]]
            send(src, far_r.at[way, slot], *sems, z=ahead(way, 2))
        for way in range(2):
            send(part.at[slot, ahead(way, 3)], near_r.at[way, slot], *sems, z=ahead(way, 1))

    def z_direct(slot):
        for way in range(2):
            near = ahead(way, 1)
            send(part.at[slot, near], ring_r.at[0, way, slot], ring_sem.at[2, 0], ring_sem.at[1, slot], z=near)

    def z_second(slot):
        phase(f"second{slot}")
        arrived(part.at[slot, 0:3], ring_sem.at[0, slot])
        for way in range(2):
            far = ahead(way, 2)
            mine = part[slot, far] + near_r[way, slot]
            extra = mine[spans[way]] + far_r[way, slot]
            ring_s[way, slot, spans[way]] = extra
            ring_s[way, slot, spans[1 - way]] = mine[spans[1 - way]]
            send(ring_s.at[way, slot], ring_r.at[1, way, slot], ring_sem.at[2, 0], ring_sem.at[1, slot], z=far)

    def z_last(slot):
        phase(f"last{slot}")
        arrived(part.at[slot, 0:4], ring_sem.at[1, slot])
        gw_out[slot] = (
            part[slot, z] + ring_r[0, 0, slot] + ring_r[0, 1, slot] + ring_r[1, 0, slot] + ring_r[1, 1, slot]
        )

    def own_values(slot):
        pair = peer_y(slot)
        pull_now = suffix[slot, y] + reach[slot, y, 0:1, :] * zg_r[slot]
        pull_own[pair] = pull_now
        gv_own[pair] = gv_r[slot, y] + near_end[slot, y] * dot_fine_right(k, pull_now)

    def weight(slot):
        phase(f"weight{slot}")
        incoming = zg_r[slot]
        for block in range(NY):
            pull_now = suffix[slot, block] + reach[slot, block, 0:1, :] * incoming
            from_state = dot_fine_right(k_r[block].astype(BF16), pull_now)
            gv_r[slot, block] = gv_r[slot, block] + near_end[slot, block] * from_state
        gathered = gv_r[slot].reshape(512, 128).astype(BF16)
        part[slot] = dot(hid_all[...].reshape(512, 512), gathered).reshape(NZ, 64, 128)
        z_first(slot)

    own_values(0)
    weight(0)
    z_direct(0)

    phase("pass3")
    pass_on(0, 3)
    pass_on(1, 3)
    drain_later(cot_r.at[0, 0 : NY - 1], y_sem.at[0, 7])
    phase("values_near")
    for slot in range(1, PAIRS):
        for o in (1, 3):
            block_pull(slot, peer_y(o))
            block_values(slot, peer_y(o))

    phase("wait_opposite")
    arrived(cot_r.at[0, 0 : NY - 1], y_sem.at[1, 7])
    phase("values_far")
    for slot in range(1, PAIRS):
        block_pull(slot, peer_y(2))
        block_values(slot, peer_y(2))
        plane_chain(slot)
    phase("back_y_f")
    wait_z(3, zbr_f)
    finish_plane(yr_f, ybs_f, zbr_f, False)
    ybr_f[y] = ybs_f[y]
    send_y(4, ybs_f, ybr_f)

    phase("wait_zg_all")
    arrived(zg_r.at[0 : NY - 1], zg_sem.at[1])
    phase("own_values")
    for slot in range(1, PAIRS):
        own_values(slot)
    weight(1)
    z_second(0)
    weight(2)
    phase("grad_h")
    grad_v = jnp.concatenate([gv_own[pair].astype(BF16) for pair in range(PAIRS)], axis=1)
    for part_now in range(4):
        span = slice(512 * part_now, 512 * part_now + 512)
        gh_s[:, :, :, span] = dot(grad_v, w[span, :], ((1,), (1,))).reshape(NX, 2, 16, 512)
    send(gh_s.at[:, 1 - c], gh_r, d_sem.at[0, 0], d_sem.at[1, 0], c=1 - c)
    drain_later(gh_r, d_sem.at[0, 0])

    weight(3)
    for slot in range(1, PAIRS):
        z_direct(slot)

    phase("chip_pair")
    arrived(gh_r, d_sem.at[1, 0])
    gx_s[...] = gh_s[:, c] + gh_r[...]
    for o in (2, 1, 3):
        send(gx_s.at[peer_x(o)], gx_r.at[x], x_sem.at[0], x_sem.at[1], x=peer_x(o))
    drain_later(gx_r.at[0 : NX - 1], x_sem.at[0])
    gx_r[x] = gx_s[x]

    z_second(1)
    phase("grad_k")
    gk = dot_fine_left(blend, q)
    gq = dot_fine_left(blend.T, k)
    wide = lax.broadcasted_iota(jnp.int32, (8, 512), 1)
    chooser = jnp.where(lax.broadcasted_iota(jnp.int32, (8, 512), 0) == wide // 64, 1.0, 0.0)
    pull = jnp.concatenate([pull_own[pair] for pair in range(PAIRS)], axis=1)
    val_f = vals[...].astype(F32)
    val_scaled = jnp.concatenate([spread(to_end_t, pair) for pair in range(PAIRS)], axis=1) * val_f
    gk = gk + dot_fine(val_scaled, pull, ((1,), (1,)))
    whole = jnp.sum(val_scaled * dot_fine_right(k, pull), axis=0, keepdims=True)
    used = val_f * jnp.concatenate([gv_own[pair] for pair in range(PAIRS)], axis=1)
    gk_out[...] = gk.astype(BF16)

    z_second(2)
    z_second(3)
    z_last(0)

    phase("wait_carry")
    wait_y(4, ybr_f)
    phase("grad_q")
    carry = jnp.concatenate([ybr_f[pair] for pair in range(PAIRS)], axis=1)
    cot_scaled = jnp.concatenate([spread(from_start_t, pair) for pair in range(PAIRS)], axis=1) * cot[...].astype(F32)
    gq = gq + dot_fine(cot_scaled, carry, ((1,), (1,)))
    change = cot_scaled * dot_fine_right(q, carry) - used
    high, low = halves(change)
    lowest = (change - high.astype(F32) - low.astype(F32)).astype(BF16)
    picked = chooser.astype(BF16)
    gap = row_sum[...]
    for level in (high, low, lowest):
        gap = gap + dot(picked, level, ((1,), (1,)))
    factors = jnp.concatenate([row_of(factor, pair) for pair in range(PAIRS)], axis=1)
    whole = whole + factors * jnp.sum(carry * pull, axis=0, keepdims=True)
    shared = jnp.sum(chooser * whole, axis=1, keepdims=True)
    for shift in (1, 2, 4, 8, 16, 32, 64):
        gap = gap + jnp.where(lane8 < 128 - shift, pltpu.roll(gap, 128 - shift, 1), 0.0)
    gd_out[...] = (gap + shared) * (-rate / (1.0 + jnp.exp(-pre_v)))
    gq_out[...] = gq.astype(BF16)

    phase("out_h")
    arrived(gx_r.at[0 : NX - 1], x_sem.at[1])
    gh_out[...] = (gx_r[0] + gx_r[1] + gx_r[2] + gx_r[3]).astype(BF16)

    z_last(1)
    z_last(2)
    z_last(3)
    drain_later(part.at[0:PAIRS, 0 : NZ - 1], ring_sem.at[2, 0])

    phase("drain")
    for made in sent:
        made.wait_send()
    stack.close()


def store_all(*refs):
    y = lax.axis_index("y")
    sems = refs[10]
    copies = [pltpu.make_async_copy(refs[i], refs[5 + i], sems.at[i]) for i in range(4)]
    for slot in range(PAIRS):
        pair = lax.rem(y + slot, PAIRS)
        place = refs[9].at[:, pl.ds(pl.multiple_of(128 * pair, 128), 128)]
        copies.append(pltpu.make_async_copy(refs[4].at[slot], place, sems.at[4 + slot]))
    for made in copies:
        made.start()
    for made in copies:
        made.wait()


def local(hidden, value_weight, key_vecs, queries, decay_pre, decay_rate, cotangent):
    dma = pltpu.SemaphoreType.DMA
    f32 = lambda *shape: pltpu.VMEM(shape, F32)
    y_box, z_box = (NY, STATE, 128), (NZ, ROWS + 8, 128)
    z_back, y_back = (NZ, ROWS, 128), (NY, STATE, 128)
    outs = pl.pallas_call(
        kernel,
        out_shape=(
            jax.ShapeDtypeStruct((TOK, STATE), BF16),
            jax.ShapeDtypeStruct((TOK, STATE), BF16),
            jax.ShapeDtypeStruct((HEADS, TOK), F32),
            jax.ShapeDtypeStruct((16, 2048), BF16),
            jax.ShapeDtypeStruct((PAIRS, 64, 128), F32),
        ),
        in_specs=[pl.BlockSpec(memory_space=pltpu.HBM)] * 7,
        out_specs=[pl.BlockSpec(memory_space=pltpu.VMEM)] * 5,
        scratch_shapes=[
            *[f32(*y_box)] * 2,
            *[f32(*z_box)] * 4,
            *[f32(*z_back)] * 4,
            *[f32(*y_back)] * 2,
            f32(NZ, NY, 64, TOK),
            f32(NY, 64, TOK),
            f32(NX, NY, 64, TOK),
            f32(NX, NY, 64, TOK),
            pltpu.VMEM((NX, 2, 64, 512), BF16),
            f32(PAIRS, NY, TOK, 128),
            f32(PAIRS, NZ, 64, 128),
            f32(2, PAIRS, 64, 128),
            f32(2, PAIRS, 32, 128),
            f32(2, PAIRS, 64, 128),
            f32(2, 2, PAIRS, 64, 128),
            f32(NX, 2, 16, 2048),
            f32(NX, 16, 2048),
            f32(NX, 16, 2048),
            f32(NX, 16, 2048),
            f32(STATE, 128),
            f32(NY, STATE, 128),
            f32(TOK, STATE),
            f32(NY, TOK, STATE),
            f32(TOK, STATE),
            f32(NY, TOK, STATE),
            pltpu.VMEM((NY, STATE, TOK), BF16),
            f32(PAIRS, 128, TOK),
            f32(NY, PAIRS, 128, TOK),
            f32(HEADS, TOK),
            f32(NY, HEADS, TOK),
            f32(NY, TOK, TOK),
            f32(PAIRS, NY, TOK, 128),
            f32(PAIRS, NY, STATE, 128),
            f32(PAIRS, NY, 8, 128),
            f32(PAIRS, NY, STATE, 128),
            f32(PAIRS, NY, 8, 128),
            f32(PAIRS, STATE, 128),
            f32(PAIRS, TOK, 128),
            pltpu.VMEM((TOK, 512), BF16),
            f32(HEADS, TOK),
            pltpu.VMEM((TOK, 2048), BF16),
            pltpu.VMEM((2048, 512), BF16),
            pltpu.VMEM((TOK, STATE), BF16),
            pltpu.VMEM((TOK, STATE), BF16),
            f32(HEADS, TOK),
            f32(1, HEADS),
            pltpu.VMEM((512, TOK), BF16),
            pltpu.VMEM((TOK, 512), BF16),
            dma((2, 8)),
            dma((2, 4)),
            dma((3, 3)),
            dma((3, PAIRS)),
            dma((2, 2)),
            dma((2,)),
            dma((7,)),
            dma((2,)),
            dma((2,)),
            pltpu.SemaphoreType.REGULAR((3,)),
        ],
        compiler_params=pltpu.CompilerParams(
            collective_id=0, has_side_effects=True, vmem_limit_bytes=VMEM_LIMIT
        ),
        name="mixer_backward",
    )(
        *[
            pltpu.with_memory_space_constraint(a, pltpu.HBM)
            for a in (
                hidden,
                value_weight,
                key_vecs.reshape(TOK, STATE),
                queries.reshape(TOK, STATE),
                decay_pre.T,
                decay_rate[None, :],
                cotangent.reshape(TOK, 512).T,
            )
        ]
    )
    gk, gq, gd, gh, gw = pl.pallas_call(
        store_all,
        out_shape=(
            *[jax.ShapeDtypeStruct(o.shape, o.dtype) for o in outs[:4]],
            jax.ShapeDtypeStruct((64, 512), F32),
        ),
        in_specs=[pl.BlockSpec(memory_space=pltpu.VMEM)] * 5,
        out_specs=[pl.BlockSpec(memory_space=pltpu.HBM)] * 5,
        scratch_shapes=[dma((8,))],
        compiler_params=pltpu.CompilerParams(vmem_limit_bytes=2 * 1024 * 1024),
        name="store_all",
    )(*outs)
    return gk.reshape(TOK, 1, STATE), gq.reshape(TOK, 1, STATE), gd.T, gh, gw


def solution(mesh):
    split = Mesh(mesh.devices.reshape(NZ, NY, NX, 2), ("z", "y", "x", "c"))
    placed = (
        P(SP, None),
        P(None, TP),
        P(SP, TP, None),
        P(SP, TP, None),
        P(SP, TP),
        P(TP),
        P(SP, TP, None),
    )
    return jax.shard_map(
        local,
        mesh=split,
        in_specs=placed,
        out_specs=(P(SP, TP, None), P(SP, TP, None), P(SP, TP), P(SP + TP, None), P(SP, TP)),
        check_vma=False,
    )
```

```python
import contextlib

import jax
import jax.numpy as jnp
from jax import lax
from jax.experimental import pallas as pl
from jax.experimental.pallas import tpu as pltpu
from jax.sharding import Mesh
from jax.sharding import PartitionSpec as P

F32, BF16 = jnp.float32, jnp.bfloat16
MESH = pl.DeviceIdType.MESH
SP, TP = ("z", "y"), ("x", "c")
NZ, NY, NX = 8, 4, 4
TOK, STATE, PAIRS, HEADS = 128, 128, 4, 8
ROWS = STATE // NZ
VMEM_LIMIT = 48 * 1024 * 1024


def dot(a, b, dims=((1,), (0,))):
    return lax.dot_general(a, b, (dims, ((), ())), preferred_element_type=F32)


def halves(a):
    high = a.astype(BF16)
    return high, (a - high.astype(F32)).astype(BF16)


def dot_fine_right(a, b, dims=((1,), (0,))):
    high, low = halves(b)
    return dot(a, high, dims) + dot(a, low, dims)


def dot_fine_left(a, b, dims=((1,), (0,))):
    high, low = halves(a)
    return dot(high, b, dims) + dot(low, b, dims)


def dot_fine(a, b, dims=((1,), (0,))):
    a_high, a_low = halves(a)
    b_high, b_low = halves(b)
    return dot(a_high, b_high, dims) + dot(a_high, b_low, dims) + dot(a_low, b_high, dims)


def cols(pair):
    return slice(128 * pair, 128 * pair + 128)


def kernel(
    hid_at, w_at, k_at, q_at, pre_at, rate_at, cot_at,
    gk_out, gq_out, gd_out, gh_out, gw_out,
    ys_f, yr_f, zs_b, zr_b, zs_f, zr_f,
    zbs_b, zbr_b, zbs_f, zbr_f, ybs_f, ybr_f,
    hid_t, hid_p, hid_x, hid_c, hid_all, gv_r, part, near_r, far_r, ring_s, ring_r,
    gh_s, gh_r, gx_s, gx_r, zg_s, zg_r, k_s, k_r, q_s, q_r, q_t, cot_s, cot_r, cum_s, cum_r,
    score, near_end, pulls, gains, suffix, reach, pull_own, gv_own, vals, row_sum,
    hid, w, k_in, q_in, pre, rate_in, cot_t, cot,
    y_sem, z_sem, rest_sem, ring_sem, d_sem, x_sem, in_sem, h_sem, zg_sem, near_sem,
):
    z, y = lax.axis_index("z"), lax.axis_index("y")
    x, c = lax.axis_index("x"), lax.axis_index("c")
    lane = lax.broadcasted_iota(jnp.int32, (128, 128), 1)
    first_head = lane[0:1, :] < 64
    sent = []
    stack = contextlib.ExitStack()

    def phase(name):
        stack.close()
        stack.enter_context(jax.named_scope(name))

    def peer_y(o):
        return lax.rem(y + o, NY)

    def peer_z(o):
        return lax.rem(z + o, NZ)

    def peer_x(o):
        return lax.rem(x + o, NX)

    def copy(src, dst, s_sem, r_sem, **where):
        return pltpu.make_async_remote_copy(
            src_ref=src, dst_ref=dst, send_sem=s_sem, recv_sem=r_sem, device_id=where, device_id_type=MESH
        )

    def send(src, dst, s_sem, r_sem, **where):
        copy(src, dst, s_sem, r_sem, **where).start()

    def arrived(dst, r_sem):
        copy(dst, dst, r_sem, r_sem, c=1 - c).wait_recv()

    def drain_later(like, s_sem):
        sent.append(copy(like, like, s_sem, s_sem, c=1 - c))

    def send_y(kind, src, dst):
        for o in range(1, NY):
            send(src.at[peer_y(o)], dst.at[y], y_sem.at[0, kind], y_sem.at[1, kind], y=peer_y(o))
        drain_later(dst.at[0 : NY - 1], y_sem.at[0, kind])

    def share_y(kind, src, dst):
        for o in range(1, NY):
            send(src, dst.at[y], y_sem.at[0, kind], y_sem.at[1, kind], y=peer_y(o))
        drain_later(dst.at[0 : NY - 1], y_sem.at[0, kind])

    def wait_y(kind, dst):
        arrived(dst.at[0 : NY - 1], y_sem.at[1, kind])

    def send_z(kind, src, dst):
        for o in range(1, NZ):
            send(src.at[peer_z(o)], dst.at[z], z_sem.at[0, kind], z_sem.at[1, kind], z=peer_z(o))
        drain_later(dst.at[0 : NZ - 1], z_sem.at[0, kind])

    def wait_z(kind, dst):
        arrived(dst.at[0 : NZ - 1], z_sem.at[1, kind])

    phase("enter")
    loads = [
        pltpu.make_async_copy(src, dst, in_sem.at[i])
        for i, (src, dst) in enumerate(
            [(cot_at, cot_t), (q_at, q_in), (pre_at, pre), (rate_at, rate_in), (k_at, k_in), (hid_at, hid), (w_at, w)]
        )
    ]
    for made in loads:
        made.start()

    barrier = pltpu.get_barrier_semaphore()
    for o in range(1, NY):
        pl.semaphore_signal(barrier, inc=1, device_id={"y": peer_y(o)}, device_id_type=MESH)
    for o in (1, NZ - 1):
        pl.semaphore_signal(barrier, inc=1, device_id={"z": peer_z(o)}, device_id_type=MESH)
    for o in range(1, NX):
        pl.semaphore_signal(barrier, inc=1, device_id={"x": peer_x(o)}, device_id_type=MESH)
    pl.semaphore_signal(barrier, inc=1, device_id={"c": 1 - c}, device_id_type=MESH)

    phase("widen")
    loads[0].wait()
    for pair in range(PAIRS):
        cot_s[pair] = cot_t[cols(pair), :].astype(F32)
    cot_r[y] = cot_s[...]
    loads[1].wait()
    q = q_in[...]
    q_s[...] = q.astype(F32)
    q_r[y] = q_s[...]
    phase("barrier")
    pl.semaphore_wait(barrier, NY + NX + 1)

    def tell_z(turn):
        for o in (1, NZ - 1):
            pl.semaphore_signal(near_sem.at[turn], inc=1, device_id={"z": peer_z(o)}, device_id_type=MESH)

    def heard_z(turn):
        pl.semaphore_wait(near_sem.at[turn], 2)

    tell_z(0)
    share_y(3, q_s, q_r)
    for o in range(1, NY):
        send(cot_s.at[peer_y(o)], cot_r.at[y, peer_y(o)], y_sem.at[0, 0], y_sem.at[1, 0], y=peer_y(o))
    drain_later(cot_r.at[0, 0 : NY - 1], y_sem.at[0, 0])

    phase("decay")
    loads[2].wait()
    loads[3].wait()
    pre_v = pre[...]
    square = lax.broadcasted_iota(jnp.int32, (8, 8), 0) == lax.broadcasted_iota(jnp.int32, (8, 8), 1)
    rate = jnp.sum(jnp.where(square, jnp.broadcast_to(rate_in[...], (8, 8)), 0.0), axis=1, keepdims=True)
    soft = jnp.maximum(pre_v, 0.0) + jnp.log1p(jnp.exp(-jnp.abs(pre_v)))
    cum = -rate * soft
    lane8 = lane[0:8, :]
    for shift in (1, 2, 4, 8, 16, 32, 64):
        cum = cum + jnp.where(lane8 >= shift, pltpu.roll(cum, shift, 1), 0.0)
    cum_s[...] = cum
    cum_r[y] = cum
    total = jnp.broadcast_to(cum[:, 127:128], (8, 128))
    factor = jnp.exp(total)
    cum_t = cum.T
    from_start = jnp.exp(cum)
    from_start_t = from_start.T
    to_end_t = jnp.exp(total - cum).T

    def spread(columns, pair):
        return jnp.where(first_head, columns[:, 2 * pair : 2 * pair + 1], columns[:, 2 * pair + 1 : 2 * pair + 2])

    def row_of(gains, pair):
        return jnp.where(first_head, gains[2 * pair : 2 * pair + 1, :], gains[2 * pair + 1 : 2 * pair + 2, :])

    share_y(6, cum_s, cum_r)
    loads[4].wait()
    k = k_in[...]
    k_s[...] = k.astype(F32)
    k_r[y] = k_s[...]

    heard_z(0)
    tell_z(1)
    phase("hidden")
    loads[5].wait()
    for block in range(16):
        turned = hid[:, cols(block)].astype(F32).T
        hid_t[block // 2, 2 * (block % 2) : 2 * (block % 2) + 2] = turned.reshape(2, 64, 128)
    seat = 2 * x + c
    for o in range(1, NY):
        send(hid_t.at[seat, peer_y(o)], hid_p.at[y], y_sem.at[0, 2], y_sem.at[1, 2], y=peer_y(o))
    drain_later(hid_p.at[0 : NY - 1], y_sem.at[0, 2])
    hid_p[y] = hid_t[seat, y]
    phase("values")
    loads[6].wait()
    k_t = k_s[...].T.astype(BF16)
    for half in range(2):
        span = slice(256 * half, 256 * half + 256)
        vals[:, span] = dot(hid[...], w[:, span]).astype(BF16)
    scaled = jnp.concatenate([spread(to_end_t, pair) for pair in range(PAIRS)], axis=1) * vals[...].astype(F32)
    states = dot_fine_right(k_t, scaled)
    for pair in range(PAIRS):
        ys_f[pair, 0:128, :] = states[:, cols(pair)]
        ys_f[pair, 128:136, :] = jnp.broadcast_to(row_of(factor, pair), (8, 128))
    yr_f[y] = ys_f[y]
    send_y(1, ys_f, yr_f)

    share_y(5, k_s, k_r)

    for o in range(1, PAIRS):
        for way in range(2):
            side = peer_y(1 + 2 * way)
            pair = peer_y(1 + 2 * way + o)
            send(cot_s.at[pair], cot_r.at[y, pair], rest_sem.at[2, 0], rest_sem.at[way, o - 1], y=side)
    drain_later(cot_r.at[0:2, 0 : NY - 1], rest_sem.at[2, 0])
    halves_of = (slice(0, 64), slice(64, 128))

    def pass_on(way, o):
        origin, side = peer_y(3 - 2 * way), peer_y(1 + 2 * way)
        if o > 0:
            arrived(cot_r.at[origin, peer_y(o)], rest_sem.at[way, o - 1])
        if o != (1, 3)[way]:
            half = cot_r.at[origin, peer_y(o), halves_of[way]]
            send(half, half, y_sem.at[0, 7], y_sem.at[1, 7], y=side)

    heard_z(1)
    tell_z(2)
    phase("block")
    for pair in range(PAIRS):
        cot[:, cols(pair)] = cot_t[cols(pair), :].astype(F32).T.astype(BF16)
    causal = lax.broadcasted_iota(jnp.int32, (128, 128), 0) <= lane
    blend = jnp.zeros((128, 128), F32)
    score_own = dot(k, q, ((1,), (1,)))
    for pair in range(PAIRS):
        cot_pair, val_pair = cot[:, cols(pair)], vals[:, cols(pair)]
        for side in range(2):
            head = 2 * pair + side
            mine = first_head if side == 0 else jnp.logical_not(first_head)
            across = jnp.where(causal, cum[head : head + 1, :] - cum_t[:, head : head + 1], 0.0)
            damping = jnp.where(causal, jnp.exp(across), 0.0)
            cot_head = jnp.where(mine, cot_pair.astype(F32), 0.0).astype(BF16)
            moved = dot(val_pair, cot_head, ((1,), (1,))) * damping
            blend = blend + moved
            row_sum[head : head + 1, :] = jnp.sum(moved * score_own, axis=0, keepdims=True)

    upper = lax.broadcasted_iota(jnp.int32, (128, 128), 0) < 64

    def rows_of(slot, block):
        pair = peer_y(slot)
        return [cum_r[block, pl.ds(2 * pair + side, 1), :] for side in range(2)]

    def block_pull(slot, block):
        first, second = rows_of(slot, block)
        growth = jnp.where(upper, jnp.exp(first), jnp.exp(second))
        pulls[slot, block] = dot_fine_right(q_t[block], growth * cot_r[block, peer_y(slot)], ((1,), (1,)))
        gain = jnp.where(first_head, jnp.exp(first[:, 127:128]), jnp.exp(second[:, 127:128]))
        gains[slot, block] = jnp.broadcast_to(gain, (8, 128))

    def plane_chain(slot):
        after = gain = None
        for block in range(NY - 1, -1, -1):
            suffix[slot, block] = jnp.zeros((128, 128), F32) if after is None else after
            reach[slot, block] = jnp.ones((8, 128), F32) if gain is None else gain
            here = gains[slot, block]
            after = pulls[slot, block] if after is None else pulls[slot, block] + here[0:1, :] * after
            gain = here if gain is None else gain * here
        return after, gain

    def block_values(slot, block):
        rows = rows_of(slot, block)
        tall = [jnp.broadcast_to(row, (128, 128)).T for row in rows]
        near_end[slot, block] = jnp.exp(
            jnp.where(first_head, rows[0][:, 127:128] - tall[0], rows[1][:, 127:128] - tall[1])
        )
        weights = []
        for side in range(2):
            across = jnp.where(causal, rows[side] - tall[side], 0.0)
            weights.append(score[block] * jnp.where(causal, jnp.exp(across), 0.0))
        cot_pair = cot_r[block, peer_y(slot)]
        cots = jnp.concatenate([jnp.where(upper, cot_pair, 0.0), jnp.where(upper, 0.0, cot_pair)], axis=1)
        gv_r[slot, block] = dot_fine_left(jnp.concatenate(weights, axis=1), cots.astype(BF16), ((1,), (1,)))

    def scan_plane(got, kept, z_send, reverse):
        state, gain = None, None
        order = range(NY - 1, -1, -1) if reverse else range(NY)
        for block in order:
            value, here = got[block, 0:128, :], got[block, 128:129, :]
            if state is None:
                kept[block] = jnp.zeros((128, 128), F32)
                state, gain = value, here
            else:
                kept[block] = state
                state, gain = here * state + value, gain * here
        for row in range(NZ):
            z_send[row, 0:ROWS, :] = state[row * ROWS : row * ROWS + ROWS, :]
            z_send[row, ROWS : ROWS + 8, :] = jnp.broadcast_to(gain, (8, 128))

    def scan_z(got, back, reverse):
        state = None
        for plane in range(NZ - 1, -1, -1) if reverse else range(NZ):
            value, here = got[plane, 0:ROWS, :], got[plane, ROWS : ROWS + 1, :]
            if state is None:
                back[plane] = jnp.zeros((ROWS, 128), F32)
                state = value
            else:
                back[plane] = state
                state = here * state + value

    def finish_plane(got, kept, plane_in, reverse):
        incoming = plane_in[...].reshape(STATE, 128)
        gain = None
        for block in range(NY - 1, -1, -1) if reverse else range(NY):
            kept[block] = kept[block] + (incoming if gain is None else gain * incoming)
            here = got[block, 128:129, :]
            gain = here if gain is None else gain * here

    phase("first")
    wait_y(6, cum_r)
    wait_y(3, q_r)
    arrived(cot_r.at[0, 0 : NY - 1], y_sem.at[1, 0])
    phase("pulls0")
    for block in range(NY):
        q_t[block] = q_r[block].T.astype(BF16)
    for block in range(NY):
        block_pull(0, block)
    state, gain = plane_chain(0)
    for row in range(NZ):
        zs_b[row, 0:ROWS, :] = state[row * ROWS : row * ROWS + ROWS, :]
        zs_b[row, ROWS : ROWS + 8, :] = gain
    zr_b[z] = zs_b[z]
    heard_z(2)
    send_z(0, zs_b, zr_b)
    pass_on(0, 0)
    pass_on(1, 0)
    for slot in range(1, PAIRS):
        block_pull(slot, y)

    phase("hidden_x")
    wait_y(2, hid_p)
    for o in range(1, NX):
        send(hid_p, hid_x.at[x], h_sem.at[0], h_sem.at[1], x=peer_x(o))
    drain_later(hid_x.at[0 : NX - 1], h_sem.at[0])
    hid_x[x] = hid_p[...]

    phase("scan_y_f")
    wait_y(1, yr_f)
    scan_plane(yr_f, ybs_f, zs_f, False)
    zr_f[z] = zs_f[z]
    send_z(1, zs_f, zr_f)

    phase("scan_z_b")
    wait_z(0, zr_b)
    scan_z(zr_b, zbs_b, True)
    zbr_b[z] = zbs_b[z]
    send_z(2, zbs_b, zbr_b)

    phase("hidden_c")
    arrived(hid_x.at[0 : NX - 1], h_sem.at[1])
    send(hid_x, hid_c, d_sem.at[0, 1], d_sem.at[1, 1], c=1 - c)
    drain_later(hid_x, d_sem.at[0, 1])

    phase("keys_far")
    wait_y(5, k_r)
    phase("values0")
    for block in range(NY):
        score[block] = dot(k_r[block].astype(BF16), q_r[block].astype(BF16), ((1,), (1,)))
    for block in range(NY):
        block_values(0, block)
    for slot in range(1, PAIRS):
        block_values(slot, y)

    phase("pass1")
    pass_on(0, 1)
    pass_on(1, 1)
    phase("scan_z_f")
    wait_z(1, zr_f)
    scan_z(zr_f, zbs_f, False)
    zbr_f[z] = zbs_f[z]
    send_z(3, zbs_f, zbr_f)

    phase("pass2")
    pass_on(0, 2)
    pass_on(1, 2)

    phase("wait_zg")
    wait_z(2, zbr_b)
    zg_s[...] = zbr_b[...].reshape(STATE, 128)
    zg_r[0] = zg_s[...]
    for o in range(1, NY):
        send(zg_s, zg_r.at[NY - o], zg_sem.at[0], zg_sem.at[1], y=peer_y(o))
    drain_later(zg_r.at[0 : NY - 1], zg_sem.at[0])

    phase("hid_all")
    arrived(hid_c, d_sem.at[1, 1])
    for across_x in range(NX):
        for block in range(NY):
            hid_all[across_x, c, :, cols(block)] = hid_x[across_x, block].astype(BF16)
            hid_all[across_x, 1 - c, :, cols(block)] = hid_c[across_x, block].astype(BF16)

    spans = (slice(0, 32), slice(32, 64))

    def ahead(way, o):
        return peer_z(o) if way == 0 else peer_z(NZ - o)

    def z_first(slot):
        sems = (ring_sem.at[2, 0], ring_sem.at[0, slot])
        for way in range(2):
            src = part.at[slot, ahead(way, 4), spans[way]]
            send(src, far_r.at[way, slot], *sems, z=ahead(way, 2))
        for way in range(2):
            send(part.at[slot, ahead(way, 3)], near_r.at[way, slot], *sems, z=ahead(way, 1))

    def z_direct(slot):
        for way in range(2):
            near = ahead(way, 1)
            send(part.at[slot, near], ring_r.at[0, way, slot], ring_sem.at[2, 0], ring_sem.at[1, slot], z=near)

    def z_second(slot):
        phase(f"second{slot}")
        arrived(part.at[slot, 0:3], ring_sem.at[0, slot])
        for way in range(2):
            far = ahead(way, 2)
            mine = part[slot, far] + near_r[way, slot]
            extra = mine[spans[way]] + far_r[way, slot]
            ring_s[way, slot, spans[way]] = extra
            ring_s[way, slot, spans[1 - way]] = mine[spans[1 - way]]
            send(ring_s.at[way, slot], ring_r.at[1, way, slot], ring_sem.at[2, 0], ring_sem.at[1, slot], z=far)

    def z_last(slot):
        phase(f"last{slot}")
        arrived(part.at[slot, 0:4], ring_sem.at[1, slot])
        gw_out[slot] = (
            part[slot, z] + ring_r[0, 0, slot] + ring_r[0, 1, slot] + ring_r[1, 0, slot] + ring_r[1, 1, slot]
        )

    def own_values(slot):
        pair = peer_y(slot)
        pull_now = suffix[slot, y] + reach[slot, y, 0:1, :] * zg_r[slot]
        pull_own[pair] = pull_now
        gv_own[pair] = gv_r[slot, y] + near_end[slot, y] * dot_fine_right(k, pull_now)

    def weight(slot):
        phase(f"weight{slot}")
        incoming = zg_r[slot]
        for block in range(NY):
            pull_now = suffix[slot, block] + reach[slot, block, 0:1, :] * incoming
            from_state = dot_fine_right(k_r[block].astype(BF16), pull_now)
            gv_r[slot, block] = gv_r[slot, block] + near_end[slot, block] * from_state
        gathered = gv_r[slot].reshape(512, 128).astype(BF16)
        part[slot] = dot(hid_all[...].reshape(512, 512), gathered).reshape(NZ, 64, 128)
        z_first(slot)

    own_values(0)
    weight(0)
    z_direct(0)

    phase("pass3")
    pass_on(0, 3)
    pass_on(1, 3)
    drain_later(cot_r.at[0, 0 : NY - 1], y_sem.at[0, 7])
    phase("values_near")
    for slot in range(1, PAIRS):
        for o in (1, 3):
            block_pull(slot, peer_y(o))
            block_values(slot, peer_y(o))

    phase("wait_opposite")
    arrived(cot_r.at[0, 0 : NY - 1], y_sem.at[1, 7])
    phase("values_far")
    for slot in range(1, PAIRS):
        block_pull(slot, peer_y(2))
        block_values(slot, peer_y(2))
        plane_chain(slot)
    phase("back_y_f")
    wait_z(3, zbr_f)
    finish_plane(yr_f, ybs_f, zbr_f, False)
    ybr_f[y] = ybs_f[y]
    send_y(4, ybs_f, ybr_f)

    phase("wait_zg_all")
    arrived(zg_r.at[0 : NY - 1], zg_sem.at[1])
    phase("own_values")
    for slot in range(1, PAIRS):
        own_values(slot)
    z_second(0)
    weight(1)
    weight(2)
    phase("grad_h")
    grad_v = jnp.concatenate([gv_own[pair].astype(BF16) for pair in range(PAIRS)], axis=1)
    for part_now in range(4):
        span = slice(512 * part_now, 512 * part_now + 512)
        gh_s[:, :, :, span] = dot(grad_v, w[span, :], ((1,), (1,))).reshape(NX, 2, 16, 512)
    send(gh_s.at[:, 1 - c], gh_r, d_sem.at[0, 0], d_sem.at[1, 0], c=1 - c)
    drain_later(gh_r, d_sem.at[0, 0])

    weight(3)
    for slot in range(1, PAIRS):
        z_direct(slot)

    phase("chip_pair")
    arrived(gh_r, d_sem.at[1, 0])
    gx_s[...] = gh_s[:, c] + gh_r[...]
    for o in (2, 1, 3):
        send(gx_s.at[peer_x(o)], gx_r.at[x], x_sem.at[0], x_sem.at[1], x=peer_x(o))
    drain_later(gx_r.at[0 : NX - 1], x_sem.at[0])
    gx_r[x] = gx_s[x]

    z_second(1)
    phase("grad_k")
    gk = dot_fine_left(blend, q)
    gq = dot_fine_left(blend.T, k)
    wide = lax.broadcasted_iota(jnp.int32, (8, 512), 1)
    chooser = jnp.where(lax.broadcasted_iota(jnp.int32, (8, 512), 0) == wide // 64, 1.0, 0.0)
    pull = jnp.concatenate([pull_own[pair] for pair in range(PAIRS)], axis=1)
    val_f = vals[...].astype(F32)
    val_scaled = jnp.concatenate([spread(to_end_t, pair) for pair in range(PAIRS)], axis=1) * val_f
    gk = gk + dot_fine(val_scaled, pull, ((1,), (1,)))
    whole = jnp.sum(val_scaled * dot_fine_right(k, pull), axis=0, keepdims=True)
    used = val_f * jnp.concatenate([gv_own[pair] for pair in range(PAIRS)], axis=1)
    gk_out[...] = gk.astype(BF16)

    z_second(2)
    z_second(3)
    z_last(0)

    phase("wait_carry")
    wait_y(4, ybr_f)
    phase("grad_q")
    carry = jnp.concatenate([ybr_f[pair] for pair in range(PAIRS)], axis=1)
    cot_scaled = jnp.concatenate([spread(from_start_t, pair) for pair in range(PAIRS)], axis=1) * cot[...].astype(F32)
    gq = gq + dot_fine(cot_scaled, carry, ((1,), (1,)))
    change = cot_scaled * dot_fine_right(q, carry) - used
    high, low = halves(change)
    lowest = (change - high.astype(F32) - low.astype(F32)).astype(BF16)
    picked = chooser.astype(BF16)
    gap = row_sum[...]
    for level in (high, low, lowest):
        gap = gap + dot(picked, level, ((1,), (1,)))
    factors = jnp.concatenate([row_of(factor, pair) for pair in range(PAIRS)], axis=1)
    whole = whole + factors * jnp.sum(carry * pull, axis=0, keepdims=True)
    shared = jnp.sum(chooser * whole, axis=1, keepdims=True)
    for shift in (1, 2, 4, 8, 16, 32, 64):
        gap = gap + jnp.where(lane8 < 128 - shift, pltpu.roll(gap, 128 - shift, 1), 0.0)
    gd_out[...] = (gap + shared) * (-rate / (1.0 + jnp.exp(-pre_v)))
    gq_out[...] = gq.astype(BF16)

    phase("out_h")
    arrived(gx_r.at[0 : NX - 1], x_sem.at[1])
    gh_out[...] = (gx_r[0] + gx_r[1] + gx_r[2] + gx_r[3]).astype(BF16)

    z_last(1)
    z_last(2)
    z_last(3)
    drain_later(part.at[0:PAIRS, 0 : NZ - 1], ring_sem.at[2, 0])

    phase("drain")
    for made in sent:
        made.wait_send()
    stack.close()


def store_all(*refs):
    y = lax.axis_index("y")
    sems = refs[10]
    copies = [pltpu.make_async_copy(refs[i], refs[5 + i], sems.at[i]) for i in range(4)]
    for slot in range(PAIRS):
        pair = lax.rem(y + slot, PAIRS)
        place = refs[9].at[:, pl.ds(pl.multiple_of(128 * pair, 128), 128)]
        copies.append(pltpu.make_async_copy(refs[4].at[slot], place, sems.at[4 + slot]))
    for made in copies:
        made.start()
    for made in copies:
        made.wait()


def local(hidden, value_weight, key_vecs, queries, decay_pre, decay_rate, cotangent):
    dma = pltpu.SemaphoreType.DMA
    f32 = lambda *shape: pltpu.VMEM(shape, F32)
    y_box, z_box = (NY, STATE + 8, 128), (NZ, ROWS + 8, 128)
    z_back, y_back = (NZ, ROWS, 128), (NY, STATE, 128)
    outs = pl.pallas_call(
        kernel,
        out_shape=(
            jax.ShapeDtypeStruct((TOK, STATE), BF16),
            jax.ShapeDtypeStruct((TOK, STATE), BF16),
            jax.ShapeDtypeStruct((HEADS, TOK), F32),
            jax.ShapeDtypeStruct((16, 2048), BF16),
            jax.ShapeDtypeStruct((PAIRS, 64, 128), F32),
        ),
        in_specs=[pl.BlockSpec(memory_space=pltpu.HBM)] * 7,
        out_specs=[pl.BlockSpec(memory_space=pltpu.VMEM)] * 5,
        scratch_shapes=[
            *[f32(*y_box)] * 2,
            *[f32(*z_box)] * 4,
            *[f32(*z_back)] * 4,
            *[f32(*y_back)] * 2,
            f32(NZ, NY, 64, TOK),
            f32(NY, 64, TOK),
            f32(NX, NY, 64, TOK),
            f32(NX, NY, 64, TOK),
            pltpu.VMEM((NX, 2, 64, 512), BF16),
            f32(PAIRS, NY, TOK, 128),
            f32(PAIRS, NZ, 64, 128),
            f32(2, PAIRS, 64, 128),
            f32(2, PAIRS, 32, 128),
            f32(2, PAIRS, 64, 128),
            f32(2, 2, PAIRS, 64, 128),
            f32(NX, 2, 16, 2048),
            f32(NX, 16, 2048),
            f32(NX, 16, 2048),
            f32(NX, 16, 2048),
            f32(STATE, 128),
            f32(NY, STATE, 128),
            f32(TOK, STATE),
            f32(NY, TOK, STATE),
            f32(TOK, STATE),
            f32(NY, TOK, STATE),
            pltpu.VMEM((NY, STATE, TOK), BF16),
            f32(PAIRS, 128, TOK),
            f32(NY, PAIRS, 128, TOK),
            f32(HEADS, TOK),
            f32(NY, HEADS, TOK),
            f32(NY, TOK, TOK),
            f32(PAIRS, NY, TOK, 128),
            f32(PAIRS, NY, STATE, 128),
            f32(PAIRS, NY, 8, 128),
            f32(PAIRS, NY, STATE, 128),
            f32(PAIRS, NY, 8, 128),
            f32(PAIRS, STATE, 128),
            f32(PAIRS, TOK, 128),
            pltpu.VMEM((TOK, 512), BF16),
            f32(HEADS, TOK),
            pltpu.VMEM((TOK, 2048), BF16),
            pltpu.VMEM((2048, 512), BF16),
            pltpu.VMEM((TOK, STATE), BF16),
            pltpu.VMEM((TOK, STATE), BF16),
            f32(HEADS, TOK),
            f32(1, HEADS),
            pltpu.VMEM((512, TOK), BF16),
            pltpu.VMEM((TOK, 512), BF16),
            dma((2, 8)),
            dma((2, 4)),
            dma((3, 3)),
            dma((3, PAIRS)),
            dma((2, 2)),
            dma((2,)),
            dma((7,)),
            dma((2,)),
            dma((2,)),
            pltpu.SemaphoreType.REGULAR((3,)),
        ],
        compiler_params=pltpu.CompilerParams(
            collective_id=0, has_side_effects=True, vmem_limit_bytes=VMEM_LIMIT
        ),
        name="mixer_backward",
    )(
        *[
            pltpu.with_memory_space_constraint(a, pltpu.HBM)
            for a in (
                hidden,
                value_weight,
                key_vecs.reshape(TOK, STATE),
                queries.reshape(TOK, STATE),
                decay_pre.T,
                decay_rate[None, :],
                cotangent.reshape(TOK, 512).T,
            )
        ]
    )
    gk, gq, gd, gh, gw = pl.pallas_call(
        store_all,
        out_shape=(
            *[jax.ShapeDtypeStruct(o.shape, o.dtype) for o in outs[:4]],
            jax.ShapeDtypeStruct((64, 512), F32),
        ),
        in_specs=[pl.BlockSpec(memory_space=pltpu.VMEM)] * 5,
        out_specs=[pl.BlockSpec(memory_space=pltpu.HBM)] * 5,
        scratch_shapes=[dma((8,))],
        compiler_params=pltpu.CompilerParams(vmem_limit_bytes=2 * 1024 * 1024),
        name="store_all",
    )(*outs)
    return gk.reshape(TOK, 1, STATE), gq.reshape(TOK, 1, STATE), gd.T, gh, gw


def solution(mesh):
    split = Mesh(mesh.devices.reshape(NZ, NY, NX, 2), ("z", "y", "x", "c"))
    placed = (
        P(SP, None),
        P(None, TP),
        P(SP, TP, None),
        P(SP, TP, None),
        P(SP, TP),
        P(TP),
        P(SP, TP, None),
    )
    return jax.shard_map(
        local,
        mesh=split,
        in_specs=placed,
        out_specs=(P(SP, TP, None), P(SP, TP, None), P(SP, TP), P(SP + TP, None), P(SP, TP)),
        check_vma=False,
    )
```
